32 devices in a mesh: sp: 8 (over z, x), tp: 4 (over y, core).
Axes of the slice: x: 2, y: 2, z: 4, core: 2. Of those that a mesh axis runs over, the one named last changes fastest.
Arguments:
- tokens: bfloat16 [4096, 2048], P(('sp', 'tp')), may hold values from -6 to 6
- norm_gain: float32 [2048], replicated, may hold values from 0.1 to 1.9
- rec_query: bfloat16 [2048, 1024], P(None, 'tp'), may hold values from -0.125 to 0.125
- fwd_gate: bfloat16 [2048, 1024], P(None, 'tp'), may hold values from -0.125 to 0.125
- bwd_gate: bfloat16 [2048, 1024], P(None, 'tp'), may hold values from -0.125 to 0.125
- rec_value: bfloat16 [2048, 1024], P(None, 'tp'), may hold values from -0.125 to 0.125
- gate_leak: float32 [2, 1024], P(None, 'tp'), may hold values from 0 to 0.08, as said below
- log_decay: float32 [2, 4096, 8], P(None, 'sp', 'tp'), may hold values from -2.2 to 0, as said below
- rec_gain: float32 [128], replicated, may hold values from 0.1 to 1.9
- att_query: bfloat16 [2048, 1024], P(None, 'tp'), as said below
- att_key: bfloat16 [2048, 1024], P(None, 'tp')
- att_value: bfloat16 [2048, 1024], P(None, 'tp'), may hold values from -0.125 to 0.125
- lambdas: float32 [8], P('tp'), may hold values from 0.3 to 0.8
- att_gain: float32 [128], replicated, may hold values from 0.1 to 1.9
- out_rec: bfloat16 [1024, 2048], replicated, may hold values from -0.125 to 0.125
- out_att: bfloat16 [1024, 2048], replicated, may hold values from -0.125 to 0.125
Outputs:
- layer_out: bfloat16 [4096, 2048], P(('sp', 'tp'))
The draws below stay inside these ranges and needn't reach their ends.
Inputs may be any that keep to these rules, and one draw needn't show every extreme that they name: `gate_leak`: positive, by direction and channel. `log_decay`: never positive. `att_query`: entries of order 2048 to the power -1/2.
All inputs are finite; a program needn't handle non-finite values.
Results may differ from the reference program's by a relative error of at most 0.011.
Values may be sent and summed in bfloat16 or wider, within the bound.
A program may use at most 128 MiB of HBM per device.

```python
import jax
import jax.numpy as jnp
from jax import lax

D = 2048
HR = 8
HK = 128
HV = 128
HA = 8
AK = 64
AV = 128
BLOCK = 64
TOK_DEV = 512
SEQ = 4096


def draw_gate_leak(key, part):
    pick_key, slow_key, fast_key = jax.random.split(jax.random.fold_in(key, 3), 3)
    slow_share = 0.5
    slow_heads = jax.random.uniform(pick_key, (2, HR, 1), jnp.float32) < slow_share
    slow_rates = jnp.exp(jax.random.uniform(slow_key, (2, HR, HK), jnp.float32, jnp.log(0.3), jnp.log(1.0))) / SEQ
    fast_rates = jnp.exp(jax.random.uniform(fast_key, (2, HR, HK), jnp.float32, jnp.log(0.03), jnp.log(0.08)))
    return jnp.where(slow_heads, slow_rates, fast_rates).reshape(2, HR * HK)


def draw_log_decay(key, part):
    rate_key, spot_key, depth_key = jax.random.split(jax.random.fold_in(key, 5), 3)
    low_rate = 0.3
    high_rate = 1.2
    block_count = SEQ // TOK_DEV
    rates = jnp.exp(jax.random.uniform(rate_key, (2, block_count, 1, HR), jnp.float32, jnp.log(low_rate), jnp.log(high_rate)))
    stable_baseline = jnp.broadcast_to(-rates / SEQ, (2, block_count, TOK_DEV, HR)).reshape(2, SEQ, HR)
    marked_locations = jax.random.randint(spot_key, (2, 3, 1, HR), 0, SEQ)
    layer_depth_list = jax.random.uniform(depth_key, (2, 3, 1, HR), jnp.float32, jnp.log(0.5), jnp.log(0.8))
    token_locations = jnp.arange(SEQ, dtype=jnp.int32)[None, None, :, None]
    spike_events = jnp.sum(jnp.where(token_locations == marked_locations, layer_depth_list, 0.0), axis=1)
    return stable_baseline + spike_events


def attention_pair(key):
    base_key, own_key = jax.random.split(jax.random.fold_in(key, 7), 2)
    columns = HA * 2 * AK
    query_table = jax.random.normal(base_key, (D, columns), jnp.float32) * (3.0 / D) ** 0.5
    key_table = jax.random.normal(own_key, (D, columns), jnp.float32) / D ** 0.5
    return (query_table, key_table)


def draw_att_query(key, part):
    return attention_pair(key)[0].astype(jnp.bfloat16)


def draw_att_key(key, part):
    return attention_pair(key)[1].astype(jnp.bfloat16)


def shard_levels(key, extent, pieces, low, largest):
    factor_of, own = 1.0, jax.random.fold_in(key, 6)
    for dim, blocks in pieces:
        draws = jnp.exp(jax.random.uniform(jax.random.fold_in(own, dim), (blocks,), jnp.float32, low / len(pieces), largest / len(pieces)))
        factor_of = factor_of * jnp.repeat(draws, extent[dim] // blocks).reshape([-1 if axis == dim else 1 for axis in range(len(extent))])
    return factor_of


def bell_draw(rng, extent, deviation, limit, pieces=(), kind=jnp.bfloat16):
    level = shard_levels(rng, extent, pieces, -0.22, 0.18) if pieces else 1.0
    result = jax.random.normal(rng, extent, jnp.float32) * deviation * level
    return jnp.minimum(jnp.maximum(result, -limit), limit).astype(kind)


def setup_inputs(seed: int = 0) -> dict:
    arg_keys = jax.random.split(jax.random.key(seed), 17)
    return {
        "tokens": bell_draw(arg_keys[0], (SEQ, D), 1.0, 6.0, ((0, 32),)),
        "norm_gain": jnp.clip(1.0 + 0.18 * jax.random.normal(arg_keys[1], (D,), jnp.float32), 0.1, 1.9),
        "rec_query": bell_draw(arg_keys[2], (D, HR * HK), D ** -0.5, 0.125, ((1, 4),)),
        "fwd_gate": bell_draw(arg_keys[3], (D, HR * HK), D ** -0.5, 0.125, ((1, 4),)),
        "bwd_gate": bell_draw(arg_keys[4], (D, HR * HK), D ** -0.5, 0.125, ((1, 4),)),
        "rec_value": bell_draw(arg_keys[5], (D, HR * HV), D ** -0.5, 0.125, ((1, 4),)),
        "gate_leak": draw_gate_leak(jax.random.fold_in(arg_keys[16], 71), 0),
        "log_decay": draw_log_decay(jax.random.fold_in(arg_keys[16], 71), 0),
        "rec_gain": jnp.clip(1.0 + 0.18 * jax.random.normal(arg_keys[8], (HV,), jnp.float32), 0.1, 1.9),
        "att_query": draw_att_query(jax.random.fold_in(arg_keys[16], 71), 0),
        "att_key": draw_att_key(jax.random.fold_in(arg_keys[16], 71), 0),
        "att_value": bell_draw(arg_keys[11], (D, HA * AV), D ** -0.5, 0.125, ((1, 4),)),
        "lambdas": jnp.clip(0.3 + 0.5 * jax.random.uniform(arg_keys[12], (HA,), jnp.float32) ** shard_levels(arg_keys[12], (HA,), ((0, 4),), -0.2, 0.2), 0.3, 0.8),
        "att_gain": jnp.clip(1.0 + 0.18 * jax.random.normal(arg_keys[13], (AV,), jnp.float32), 0.1, 1.9),
        "out_rec": bell_draw(arg_keys[14], (HR * HV, D), (HR * HV + HA * AV) ** -0.5, 0.125),
        "out_att": bell_draw(arg_keys[15], (HA * AV, D), (HR * HV + HA * AV) ** -0.5, 0.125),
    }


EPS = 1e-06
THETA = 500000.0
HIGHEST = lax.Precision.HIGHEST

def rms_scale(values, gain):
    return values * lax.rsqrt(lax.optimization_barrier(jnp.mean(values * values, axis=-1, keepdims=True)) + EPS) * gain

def block_recurrence(queries, keys_in, values, log_forget):
    head_count, length, key_width = queries.shape
    value_width = values.shape[-1]
    block_count = length // BLOCK
    block_shape = (head_count, block_count, BLOCK, key_width)
    query_blocks = queries.reshape(block_shape)
    key_blocks = keys_in.reshape(block_shape)
    value_blocks = values.reshape(head_count, block_count, BLOCK, value_width)
    cumulative = jnp.cumsum(log_forget.reshape(block_shape), axis=2)
    middle = cumulative[:, :, BLOCK // 2 - 1:BLOCK // 2]
    block_last = cumulative[:, :, BLOCK - 1:]
    scores = jnp.einsum('hntd,hnsd->hnts', query_blocks * jnp.exp(cumulative - middle), key_blocks * jnp.exp(middle - cumulative), precision=HIGHEST)
    causal_mask = jnp.arange(BLOCK)[:, None] >= jnp.arange(BLOCK)[None, :]
    scores = jnp.where(causal_mask, scores, 0.0)
    within_out = jnp.einsum('hnts,hnsv->hntv', scores, value_blocks, precision=HIGHEST)
    per_block_state = jnp.einsum('hnsd,hnsv->hndv', key_blocks * jnp.exp(block_last - cumulative), value_blocks, precision=HIGHEST)
    block_decay = jnp.exp(block_last[:, :, 0])

    def advance(running, inputs_now):
        factor, added_state = inputs_now
        return (factor[..., None] * running + added_state, running)
    initial = jnp.zeros((head_count, key_width, value_width), jnp.float32)
    end_state, before = lax.scan(advance, initial, (jnp.moveaxis(block_decay, 1, 0), jnp.moveaxis(per_block_state, 1, 0)))
    before = jnp.moveaxis(before, 0, 1)
    carried = jnp.einsum('hntd,hndv->hntv', query_blocks * jnp.exp(cumulative), before, precision=HIGHEST)
    return ((within_out + carried).reshape(head_count, length, value_width), end_state, cumulative)

def rotate(vectors, positions):
    half_width = AK // 2
    frequency = THETA ** (-(jnp.arange(half_width, dtype=jnp.float32) * 2.0 / AK))
    angles = positions[:, None] * frequency[None, :]
    cosine = jnp.cos(angles)[:, None, None, :]
    sines = jnp.sin(angles)[:, None, None, :]
    first_half = vectors[..., :half_width]
    second = vectors[..., half_width:]
    return jnp.concatenate([first_half * cosine - second * sines, second * cosine + first_half * sines], axis=-1)

def reference(tokens, norm_gain, rec_query, fwd_gate, bwd_gate, rec_value, gate_leak, log_decay, rec_gain, att_query, att_key, att_value, lambdas, att_gain, out_rec, out_att):
    normed = rms_scale(tokens.astype(jnp.float32), norm_gain).astype(jnp.bfloat16)

    def project(weight):
        return jnp.dot(normed, weight, preferred_element_type=jnp.float32).astype(jnp.bfloat16)

    def split_heads(table, width):
        return table.astype(jnp.float32).reshape(SEQ, -1, width).transpose(1, 0, 2)
    queries = jax.nn.silu(split_heads(project(rec_query), HK))
    values = split_heads(project(rec_value), HV)
    key_fwd = gate_leak[0].reshape(HR, 1, HK) * jax.nn.sigmoid(-split_heads(project(fwd_gate), HK))
    key_bwd = gate_leak[1].reshape(HR, 1, HK) * jax.nn.sigmoid(-split_heads(project(bwd_gate), HK))
    log_fwd = jnp.log1p(-key_fwd) + log_decay[0].T[:, :, None]
    log_bwd = jnp.log1p(-key_bwd) + log_decay[1].T[:, :, None]
    out_fwd = block_recurrence(queries, key_fwd, values, log_fwd)[0]
    flipped = block_recurrence(jnp.flip(queries, 1), jnp.flip(key_bwd, 1), jnp.flip(values, 1), jnp.flip(log_bwd, 1))[0]
    rec_rows = rms_scale(out_fwd + jnp.flip(flipped, 1), rec_gain)
    rec_rows = rec_rows.transpose(1, 0, 2).reshape(SEQ, HR * HV).astype(jnp.bfloat16)
    positions = jnp.arange(SEQ, dtype=jnp.int32).astype(jnp.float32)
    att_queries = (rotate(project(att_query).astype(jnp.float32).reshape(SEQ, HA, 2, AK), positions) * AK ** (-0.5)).astype(jnp.bfloat16)
    att_keys = rotate(project(att_key).astype(jnp.float32).reshape(SEQ, HA, 2, AK), positions).astype(jnp.bfloat16)
    att_values = project(att_value).reshape(SEQ, HA, AV)

    def attend_head(inputs_now):
        head_queries, head_keys, head_values, weight = inputs_now
        keys_wide = head_keys.astype(jnp.float32)
        values_wide = head_values.astype(jnp.float32)

        def attend_rows(query_block):
            scores = jnp.einsum('qmd,kmd->mqk', query_block.astype(jnp.float32), keys_wide, precision=HIGHEST)
            weights_raw = jnp.exp(scores - lax.optimization_barrier(jnp.max(scores, axis=-1, keepdims=True)))
            totals = lax.optimization_barrier(jnp.sum(weights_raw, axis=-1))
            rounded = lax.optimization_barrier(weights_raw.astype(jnp.bfloat16)).astype(jnp.float32)
            summed = jnp.einsum('mqk,kv->mqv', rounded, values_wide, precision=HIGHEST)
            return summed[0] / totals[0][:, None] - weight * summed[1] / totals[1][:, None]
        blocks = head_queries.reshape(SEQ // TOK_DEV, TOK_DEV, 2, AK)
        return lax.map(attend_rows, blocks).reshape(SEQ, AV)
    mixed_heads = lax.map(attend_head, (jnp.moveaxis(att_queries, 1, 0), jnp.moveaxis(att_keys, 1, 0), jnp.moveaxis(att_values, 1, 0), lambdas))
    att_rows = rms_scale(mixed_heads, att_gain).transpose(1, 0, 2).reshape(SEQ, HA * AV).astype(jnp.bfloat16)
    projected = jnp.dot(rec_rows, out_rec, preferred_element_type=jnp.float32) + jnp.dot(att_rows, out_att, preferred_element_type=jnp.float32)
    return projected.astype(jnp.bfloat16)
```

```python
import functools

import jax
import jax.numpy as jnp
import numpy as np
from jax import lax
from jax.experimental import pallas as pl
from jax.experimental.pallas import tpu as pltpu
from jax.sharding import PartitionSpec as P

HK = 128
AK = 64
BLOCK = 64
LANES = 128
EPS = 1e-06
THETA = 500000.0
HIGHEST = lax.Precision.HIGHEST
F32 = jnp.float32
BF16 = jnp.bfloat16
PAD = 16


def rms_scale(values, gain):
    return values * lax.rsqrt(jnp.mean(values * values, axis=-1, keepdims=True) + EPS) * gain


def dot_t(a, b):
    return lax.dot_general(a, b, (((1,), (1,)), ((), ())), preferred_element_type=F32)


def dot_0(a, b):
    return lax.dot_general(a, b, (((0,), (0,)), ((), ())), preferred_element_type=F32)


def gather_kernel(tp, tokens, gain, *refs):
    weights, outs = refs[:7], refs[7:14]
    held, across, along, landed = refs[14:]
    me = lax.axis_index("tp")
    core = lax.rem(me, 2)
    pair = lax.div(me, 2)
    pairs = tp // 2
    count = tokens.shape[0]
    partner = pair * 2 + 1 - core
    others = [lax.rem(pair + k, pairs) for k in range(1, pairs)]
    barrier = pltpu.get_barrier_semaphore()
    pl.semaphore_signal(barrier, inc=1, device_id={"tp": partner})
    for q in others:
        pl.semaphore_signal(barrier, inc=1, device_id={"tp": q * 2 + core})

    def rows_at(block):
        return held.at[pl.ds(pl.multiple_of(block * count, count), count)]

    def to_partner(block):
        return pltpu.make_async_remote_copy(
            src_ref=rows_at(block),
            dst_ref=rows_at(block),
            send_sem=across.at[block],
            recv_sem=landed.at[block],
            device_id={"tp": partner},
        )

    def to_pair(q):
        return pltpu.make_async_remote_copy(
            src_ref=rows_at(me),
            dst_ref=rows_at(me),
            send_sem=along.at[q],
            recv_sem=landed.at[me],
            device_id={"tp": q * 2 + core},
        )

    normed = rms_scale(tokens[...].astype(F32), gain[...]).astype(BF16)
    held[pl.ds(pl.multiple_of(me * count, count), count), :] = normed
    pl.semaphore_wait(barrier, pairs)
    for q in others:
        to_pair(q).start()
    to_partner(me).start()

    def step(k, carry):
        q = lax.rem(pair + k, pairs)
        near = q * 2 + core

        @pl.when(k > 0)
        def _():
            to_partner(near).wait_recv()
            to_partner(near).start()

        to_partner(q * 2 + 1 - core).wait_recv()
        at = pl.ds(pl.multiple_of(q * 2 * count, 2 * count), 2 * count)
        for weight, result in zip(weights, outs):
            result[at, :] = jnp.dot(held[at, :], weight[...], preferred_element_type=F32).astype(BF16)
        return carry

    lax.fori_loop(0, pairs, step, 0)
    to_partner(me).wait_send()
    for q in others:
        to_pair(q).wait_send()
        to_partner(q * 2 + core).wait_send()


def mixer_kernel(
    ranks, tp, groups, heads, tile,
    proj_k, proj_v, proj_q, proj_rq, proj_fwd, proj_bwd, proj_rv, cosine, sine, leak, decay, lam, rec_gain, att_gain,
    out,
    kv, rest, swap, stage, state_out, state_in, cums, adds, states, rec_sum, peak, total, mixed,
    kv_send, kv_recv, swap_send, rest_recv, state_send, state_recv, out_send, out_recv,
):
    me = lax.axis_index("sp")
    slot = lax.rem(me, groups)
    mine = lax.div(me, groups)
    mesh_column = lax.axis_index("tp")
    length = proj_k.shape[0]
    piece = length // tp
    rows = groups * length
    width = heads * LANES
    block_count = rows // BLOCK
    partner_slot = groups - 1 - slot
    partner = mine * groups + partner_slot
    blocks = ranks // groups
    own_rows = pl.ds(pl.multiple_of(slot * length, length), length)
    other_rows = pl.ds(pl.multiple_of(partner_slot * length, length), length)

    barrier = pltpu.get_barrier_semaphore()
    peers = []
    for k in range(1, blocks):
        peers.append(lax.rem(mine + k, blocks))
    for peer in peers:
        pl.semaphore_signal(barrier, inc=1, device_id={"sp": peer * groups + slot})
    owners = []
    for dp in range(groups):
        for dt in range(tp):
            owners.append((dp, dt, lax.rem(slot + dp, groups), lax.rem(mesh_column + dt, tp)))
    for dp, dt, p, t in owners[1:]:
        pl.semaphore_signal(barrier, inc=1, device_id={"sp": mine * groups + p, "tp": t})

    lane = lax.broadcasted_iota(jnp.int32, (length, LANES), 1)
    low_half = lax.rem(lane, AK) < AK // 2

    def rotated(raw):
        wide = raw.astype(F32)
        turned = jnp.where(low_half, -pltpu.roll(wide, LANES - AK // 2, 1), pltpu.roll(wide, AK // 2, 1))
        return wide * cosine[...] + turned * sine[...]

    def prepare(head_group, key_value, others):
        def taken(ref, h):
            return ref[:, pl.ds(pl.multiple_of((head_group * heads + h) * LANES, LANES), LANES)]

        for h in range(heads):
            at = h * LANES
            key_value[:, at : at + LANES] = rotated(taken(proj_k, h)).astype(BF16)
            key_value[:, width + at : width + at + LANES] = taken(proj_v, h)
            others[:, at : at + LANES] = (rotated(taken(proj_q, h)) * AK ** (-0.5)).astype(BF16)
            for i, ref in enumerate((proj_rq, proj_fwd, proj_bwd, proj_rv)):
                others[:, (i + 1) * width + at : (i + 1) * width + at + LANES] = taken(ref, h)

    if groups > 1:
        prepare(partner_slot, swap.at[:, : 2 * width], swap.at[:, 2 * width :])
    prepare(slot, kv.at[mine, own_rows], rest.at[own_rows])
    pl.semaphore_wait(barrier, blocks - 1 + groups * tp - 1)

    def block_copy(source_rows, source_slot, peer):
        return pltpu.make_async_remote_copy(
            src_ref=kv.at[mine, source_rows],
            dst_ref=kv.at[mine, source_rows],
            send_sem=kv_send.at[peer, source_slot],
            recv_sem=kv_recv.at[mine, source_slot],
            device_id={"sp": peer * groups + slot},
        )

    def arrival(block, piece):
        piece_rows = pl.ds(pl.multiple_of(piece * length, length), length)
        return pltpu.make_async_remote_copy(
            src_ref=kv.at[block, piece_rows],
            dst_ref=kv.at[block, piece_rows],
            send_sem=kv_send.at[block, piece],
            recv_sem=kv_recv.at[block, piece],
            device_id={"sp": block * groups + slot},
        )

    if groups > 1:
        swap_kv = pltpu.make_async_remote_copy(
            src_ref=swap.at[:, : 2 * width],
            dst_ref=kv.at[mine, own_rows],
            send_sem=swap_send.at[0],
            recv_sem=kv_recv.at[mine, slot],
            device_id={"sp": partner},
        )
        swap_kv.start()
        swap_rest = pltpu.make_async_remote_copy(
            src_ref=swap.at[:, 2 * width :],
            dst_ref=rest.at[own_rows],
            send_sem=swap_send.at[1],
            recv_sem=rest_recv,
            device_id={"sp": partner},
        )
    own_copies = [block_copy(own_rows, slot, peer) for peer in peers]
    for copy in own_copies:
        copy.start()
    other_copies = []
    if groups > 1:
        swap_rest.start()
        arrival(mine, partner_slot).wait_recv()
        other_copies = [block_copy(other_rows, partner_slot, peer) for peer in peers]
        for copy in other_copies:
            copy.start()
        swap_rest.wait_recv()

    row_at = lax.broadcasted_iota(jnp.int32, (BLOCK, BLOCK), 0)
    col_at = lax.broadcasted_iota(jnp.int32, (BLOCK, BLOCK), 1)
    earlier = (row_at >= col_at, row_at <= col_at)
    triangles = tuple(mask.astype(F32) for mask in earlier)
    ends = (BLOCK - 1, 0)
    middles = (BLOCK // 2 - 1, BLOCK // 2)

    def rows_of(direction, step):
        index = step if direction == 0 else block_count - 1 - step
        return index, pl.ds(pl.multiple_of(index * BLOCK, BLOCK), BLOCK)

    def part(at, index, h):
        return rest[at, (index * heads + h) * LANES : (index * heads + h + 1) * LANES].astype(F32)

    def keys_of(at, direction, h):
        return leak[h, direction : direction + 1, :] * jax.nn.sigmoid(-part(at, 2 + direction, h))

    states[...] = jnp.zeros_like(states)
    rec_sum[...] = jnp.zeros_like(rec_sum)

    def first_pass(step, totals):
        after = []
        for h in range(heads):
            for d in range(2):
                index, at = rows_of(d, step)
                keys = keys_of(at, d, h)
                column = d * heads + h
                logs = jnp.log1p(-keys) + decay[at, column : column + 1]
                cum = jnp.dot(triangles[d], logs, precision=HIGHEST, preferred_element_type=F32)
                cums[h, d, at, :] = cum
                last = cum[ends[d] : ends[d] + 1, :]
                scaled = (keys * jnp.exp(last - cum)).astype(BF16)
                added = dot_0(part(at, 4, h).astype(BF16), scaled)
                adds[h, d, index] = added
                states[h, d] = states[h, d] * jnp.exp(last) + added
                after.append(totals[h * 2 + d] + last)
        return tuple(after)

    nothing = tuple(jnp.zeros((1, LANES), F32) for _ in range(2 * heads))
    sums = lax.fori_loop(0, block_count, first_pass, nothing, unroll=2)
    for h in range(heads):
        for d in range(2):
            state_out[d, h, :LANES, :] = states[h, d].astype(BF16)
            factor = jnp.broadcast_to(jnp.exp(sums[h * 2 + d]), (PAD, LANES))
            coarse = factor.astype(BF16)
            fine = (factor - coarse.astype(F32)).astype(BF16)
            first_row = lax.broadcasted_iota(jnp.int32, (PAD, LANES), 0) == 0
            state_out[d, h, LANES:, :] = jnp.where(first_row, coarse.astype(F32), fine.astype(F32)).astype(BF16)
    state_copies = []
    for peer in peers:
        copy = pltpu.make_async_remote_copy(
            src_ref=state_out.at[jnp.where(peer > mine, 0, 1)],
            dst_ref=state_in.at[mine],
            send_sem=state_send.at[peer],
            recv_sem=state_recv.at[mine],
            device_id={"sp": peer * groups + slot},
        )
        copy.start()
        state_copies.append(copy)

    lane_q = lax.broadcasted_iota(jnp.int32, (tile, LANES), 1)
    tiles = rows // tile
    peak[...] = jnp.full_like(peak, -jnp.inf)
    total[...] = jnp.zeros_like(total)
    mixed[...] = jnp.zeros_like(mixed)

    def attend(block):
        for h in range(heads):
            at = h * LANES

            def one_tile(index, carry):
                q_rows = pl.ds(pl.multiple_of(index * tile, tile), tile)
                queries = rest[q_rows, at : at + LANES]
                zero = jnp.zeros_like(queries)
                both = jnp.concatenate(
                    [jnp.where(lane_q < AK, queries, zero), jnp.where(lane_q < AK, zero, queries)], axis=0
                )
                scores = dot_t(both, kv[block, :, at : at + LANES])
                before = peak[h, index][:, :1]
                raised = jnp.maximum(before, jnp.max(scores, axis=-1, keepdims=True))
                shrink = jnp.exp(before - raised)
                expo = jnp.exp(scores - raised)
                sums_now = total[h, index][:, :1] * shrink + jnp.sum(expo, axis=-1, keepdims=True)
                product = jnp.dot(
                    expo.astype(BF16), kv[block, :, width + at : width + at + LANES], preferred_element_type=F32
                )
                mixed[h, index] = mixed[h, index] * shrink + product
                peak[h, index] = jnp.broadcast_to(raised, (2 * tile, LANES))
                total[h, index] = jnp.broadcast_to(sums_now, (2 * tile, LANES))
                return carry

            lax.fori_loop(0, tiles, one_tile, 0)

    attend(mine)

    def state_arrival(block):
        return pltpu.make_async_remote_copy(
            src_ref=state_out.at[0],
            dst_ref=state_in.at[block],
            send_sem=state_send.at[block],
            recv_sem=state_recv.at[block],
            device_id={"sp": block * groups + slot},
        )

    states[...] = jnp.zeros_like(states)

    def compose(d):
        def body(step, carry):
            block = step if d == 0 else blocks - 1 - step
            state_arrival(block).wait_recv()
            for h in range(heads):
                rows_last = state_in[block, h, LANES:, :].astype(F32)
                factor = rows_last[0:1] + rows_last[1:2]
                states[h, d] = states[h, d] * factor + state_in[block, h, :LANES, :].astype(F32)
            return carry

        return body

    lax.fori_loop(0, mine, compose(0), 0)
    lax.fori_loop(0, blocks - 1 - mine, compose(1), 0)

    def second_pass(step, carry):
        for h in range(heads):
            for d in range(2):
                index, at = rows_of(d, step)
                queries = jax.nn.silu(part(at, 1, h))
                keys = keys_of(at, d, h)
                cum = cums[h, d, at, :]
                middle = cum[middles[d] : middles[d] + 1, :]
                last = cum[ends[d] : ends[d] + 1, :]
                scores = dot_t(
                    (queries * jnp.exp(cum - middle)).astype(BF16), (keys * jnp.exp(middle - cum)).astype(BF16)
                )
                scores = jnp.where(earlier[d], scores, 0.0)
                within = jnp.dot(scores.astype(BF16), part(at, 4, h).astype(BF16), preferred_element_type=F32)
                before = states[h, d]
                carried = dot_t_state(queries * jnp.exp(cum), before)
                span = slice(h * LANES, (h + 1) * LANES)
                rec_sum[at, span] = rec_sum[at, span] + within + carried
                states[h, d] = before * jnp.exp(last) + adds[h, d, index]
        return carry

    def dot_t_state(reads, state):
        return dot_t(reads.astype(BF16), state.astype(BF16))

    lax.fori_loop(0, block_count, second_pass, 0, unroll=2)

    for h in range(heads):
        span = slice(h * LANES, (h + 1) * LANES)
        stage[:, span] = rms_scale(rec_sum[:, span], rec_gain[...]).astype(BF16)

    def hand_over(which, owner):
        dp, dt, p, t = owner
        columns = slice(which * width, (which + 1) * width)
        source = stage.at[pl.ds(pl.multiple_of(p * length + t * piece, piece), piece), columns]
        target = out.at[mesh_column, slot, :, columns]
        if dp == 0 and dt == 0:
            return pltpu.make_async_copy(source, target, out_send.at[which, dp, dt])
        return pltpu.make_async_remote_copy(
            src_ref=source,
            dst_ref=target,
            send_sem=out_send.at[which, dp, dt],
            recv_sem=out_recv.at[which, mesh_column, slot],
            device_id={"sp": mine * groups + p, "tp": t},
        )

    def taken_over(which, owner):
        dp, dt, p, t = owner
        columns = slice(which * width, (which + 1) * width)
        target = out.at[t, p, :, columns]
        return pltpu.make_async_remote_copy(
            src_ref=target,
            dst_ref=target,
            send_sem=out_send.at[which, dp, dt],
            recv_sem=out_recv.at[which, t, p],
            device_id={"sp": mine * groups + p, "tp": t},
        )

    for owner in owners:
        hand_over(0, owner).start()

    def next_block(turn, carry):
        near = lax.div(turn + 1, 2)
        away = jnp.where(lax.rem(turn, 2) == 1, near, blocks - near)
        block = lax.rem(mine + away, blocks)
        for piece in range(groups):
            arrival(block, piece).wait_recv()
        attend(block)
        return carry

    lax.fori_loop(1, blocks, next_block, 0)

    for h in range(heads):
        span = slice(width + h * LANES, width + (h + 1) * LANES)
        for index in range(tiles):
            ratio = mixed[h, index] / total[h, index][:, :1]
            values = ratio[:tile] - lam[h] * ratio[tile:]
            stage[index * tile : (index + 1) * tile, span] = rms_scale(values, att_gain[...]).astype(BF16)
    for owner in owners:
        hand_over(1, owner).start()

    for copy in own_copies + other_copies + state_copies:
        copy.wait_send()
    if groups > 1:
        swap_kv.wait_send()
        swap_rest.wait_send()
    for which in range(2):
        hand_over(which, owners[0]).wait()
        for owner in owners[1:]:
            hand_over(which, owner).wait_send()
            taken_over(which, owner).wait_recv()


def on_device_general(
    tokens, norm_gain, rec_query, fwd_gate, bwd_gate, rec_value, gate_leak, log_decay, rec_gain,
    att_query, att_key, att_value, lambdas, att_gain, out_rec, out_att,
):
    ranks = lax.axis_size("sp")
    tp = lax.axis_size("tp")
    local_heads = rec_query.shape[1] // HK
    groups = 2 if local_heads % 2 == 0 and ranks % 2 == 0 else 1
    heads = local_heads // groups
    width = heads * LANES
    slot = lax.axis_index("sp") % groups

    order = (att_key, att_value, att_query, rec_query, fwd_gate, bwd_gate, rec_value)
    length = tokens.shape[0] * tp
    vmem = pl.BlockSpec(memory_space=pltpu.VMEM)
    dma = pltpu.SemaphoreType.DMA
    projected = pl.pallas_call(
        functools.partial(gather_kernel, tp),
        out_shape=[jax.ShapeDtypeStruct((length, weight.shape[1]), BF16) for weight in order],
        in_specs=[vmem] * (2 + len(order)),
        out_specs=[vmem] * len(order),
        scratch_shapes=[
            pltpu.VMEM((length, tokens.shape[1]), BF16),
            dma((tp,)),
            dma((tp // 2,)),
            dma((tp,)),
        ],
        compiler_params=pltpu.CompilerParams(
            collective_id=1, has_side_effects=True, vmem_limit_bytes=40 * 1024 * 1024
        ),
        cost_estimate=pl.CostEstimate(flops=4 * 10**9, bytes_accessed=10**7, transcendentals=0),
    )(tokens, norm_gain.reshape(1, -1), *order)

    positions = (lax.axis_index("sp") * length + jnp.arange(length, dtype=jnp.int32)).astype(F32)
    frequency = THETA ** (-(jnp.arange(AK // 2, dtype=F32) * 2.0 / AK))
    angles = jnp.tile(positions[:, None] * frequency[None, :], (1, LANES // (AK // 2)))
    cosine, sine = jnp.cos(angles), jnp.sin(angles)

    by_head = log_decay.reshape(2, length, groups, heads).transpose(2, 1, 0, 3).reshape(groups, length, 2 * heads)
    own_decay = lax.dynamic_index_in_dim(by_head, slot, 0, keepdims=False)
    if groups > 1:
        swapped = lax.ppermute(
            lax.dynamic_index_in_dim(by_head, groups - 1 - slot, 0, keepdims=False),
            "sp",
            [(i, i + 1 - 2 * (i % 2)) for i in range(ranks)],
        )
        decay = jnp.where(
            slot == 0, jnp.concatenate([own_decay, swapped]), jnp.concatenate([swapped, own_decay])
        )
    else:
        decay = own_decay
    leak = lax.dynamic_index_in_dim(
        gate_leak.reshape(2, groups, heads, HK).transpose(1, 2, 0, 3), slot, 0, keepdims=False
    )
    lam = lax.dynamic_index_in_dim(lambdas.reshape(groups, heads), slot, 0, keepdims=False)
    lam = jnp.broadcast_to(lam[:, None, None], (heads, 1, LANES))

    blocks = ranks // groups
    rows = groups * length
    tile = min(256, length)
    mixers = pl.pallas_call(
        functools.partial(mixer_kernel, ranks, tp, groups, heads, tile),
        out_shape=jax.ShapeDtypeStruct((tp, groups, length // tp, 2 * width), BF16),
        in_specs=[vmem] * 14,
        out_specs=vmem,
        scratch_shapes=[
            pltpu.VMEM((blocks, rows, 2 * width), BF16),
            pltpu.VMEM((rows, 5 * width), BF16),
            pltpu.VMEM((length, 7 * width), BF16),
            pltpu.VMEM((rows, 2 * width), BF16),
            pltpu.VMEM((2, heads, LANES + PAD, LANES), BF16),
            pltpu.VMEM((blocks, heads, LANES + PAD, LANES), BF16),
            pltpu.VMEM((heads, 2, rows, LANES), F32),
            pltpu.VMEM((heads, 2, rows // BLOCK, LANES, LANES), F32),
            pltpu.VMEM((heads, 2, LANES, LANES), F32),
            pltpu.VMEM((rows, width), F32),
            pltpu.VMEM((heads, rows // tile, 2 * tile, LANES), F32),
            pltpu.VMEM((heads, rows // tile, 2 * tile, LANES), F32),
            pltpu.VMEM((heads, rows // tile, 2 * tile, LANES), F32),
            dma((blocks, groups)),
            dma((blocks, groups)),
            dma((2,)),
            dma,
            dma((blocks,)),
            dma((blocks,)),
            dma((2, groups, tp)),
            dma((2, tp, groups)),
        ],
        compiler_params=pltpu.CompilerParams(
            collective_id=0, has_side_effects=True, vmem_limit_bytes=56 * 1024 * 1024
        ),
        cost_estimate=pl.CostEstimate(flops=10**10, bytes_accessed=10**7, transcendentals=10**7),
    )(*projected, cosine, sine, leak, decay, lam, rec_gain.reshape(1, LANES), att_gain.reshape(1, LANES))

    shares = mixers.reshape(tp, groups, length // tp, 2, heads, LANES)
    both = shares.transpose(2, 3, 0, 1, 4, 5).reshape(length // tp, 2, -1)
    result = jnp.dot(both[:, 0], out_rec, preferred_element_type=F32) + jnp.dot(
        both[:, 1], out_att, preferred_element_type=F32
    )
    return result.astype(BF16)


def fused_kernel(
    ranks, tp, heads, planes,
    tokens_in, norm_in, w_key, w_value, w_query, w_rq, w_fwd, w_bwd, w_rv, leak_in, decay_in, rec_gain_in,
    lam_in, att_gain_in, out_rec_in, out_att_in, rotary_in,
    out,
    tokens, gain, weights, leak, decay, rec_gain, lam, att_gain, w_out_rec, w_out_att, rotary,
    held, cosine, sine, lam_own, lam_pair, stage, land, recp, cum_reads, facts, adds, rec_sum,
    state, fade, pair_out, pair_in, plane_out, plane_in, plane_sum, next_out, next_in, before_block,
    rec_stage, rec_all, score_a, score_b, top_a, top_b, acc, peak, att_stage, att_all, total,
    in_sem, across_send, across_recv, core_send, core_recv, lam_send, lam_recv,
    qkv_send, qkv_recv, side_send, side_recv, near_send, near_recv,
    pair_send, pair_recv, plane_send, plane_recv, next_send, next_recv,
    rec_send, rec_recv, att_send, att_recv,
):
    sp = lax.axis_index("sp")
    me = lax.axis_index("tp")
    x = lax.rem(sp, 2)
    z = lax.div(sp, 2)
    core = lax.rem(me, 2)
    y = lax.div(me, 2)
    piece = tokens.shape[0]
    half = piece // 2
    length = piece * tp
    width = heads * LANES
    here = {"sp": sp, "tp": me}
    partner = {"tp": y * 2 + 1 - core}
    opposite = {"tp": (1 - y) * 2 + core}
    beside = {"sp": z * 2 + 1 - x}

    sources = (
        tokens_in, norm_in, rotary_in, lam_in, w_key, w_value, w_query, w_rq, w_fwd, w_bwd, w_rv,
        leak_in, decay_in, rec_gain_in, att_gain_in, out_rec_in, out_att_in,
    )
    targets = (
        tokens, gain, rotary, lam, *(weights.at[i] for i in range(7)),
        leak, decay, rec_gain, att_gain, w_out_rec, w_out_att,
    )
    fetches = [pltpu.make_async_copy(a, b, in_sem.at[i]) for i, (a, b) in enumerate(zip(sources, targets))]
    for fetch in fetches:
        fetch.start()

    barrier = pltpu.get_barrier_semaphore()
    for dz in range(planes):
        for dt in range(tp):
            if dz or dt:
                to = {"sp": lax.rem(z + dz, planes) * 2 + x, "tp": lax.rem(me + dt, tp)}
                pl.semaphore_signal(barrier, inc=1, device_id=to)
    pl.semaphore_signal(barrier, inc=1, device_id=beside)

    def remote(source, target, send, recv, to):
        return pltpu.make_async_remote_copy(
            src_ref=source, dst_ref=target, send_sem=send, recv_sem=recv, device_id=to
        )

    fetches[2].wait()
    lane = lax.broadcasted_iota(jnp.int32, (piece, LANES), 1)
    low_half = lax.rem(lane, AK) < AK // 2
    for t in range(tp):
        first = 2 * piece + sp * tp + t
        cos_base = rotary[pl.ds(first, 1), :]
        sin_base = rotary[pl.ds(first + ranks * tp, 1), :]
        cos_row, sin_row = rotary[:piece, :], rotary[piece : 2 * piece, :]
        cosine[t * piece : (t + 1) * piece, :] = cos_base * cos_row - sin_base * sin_row
        turned = sin_base * cos_row + cos_base * sin_row
        sine[t * piece : (t + 1) * piece, :] = jnp.where(low_half, -turned, turned)

    def rows_of_piece(t, begin, count):
        return held.at[pl.ds(pl.multiple_of(t * piece + begin, half), count)]

    def across(part):
        rows = rows_of_piece(me, part * half, half)
        return remote(rows, rows, across_send.at[part], across_recv.at[part], opposite)

    def from_across(part):
        rows = rows_of_piece((1 - y) * 2 + core, part * half, half)
        return remote(rows, rows, across_send.at[part], across_recv.at[part], opposite)

    def to_core(t, slot, begin, count):
        rows = rows_of_piece(t, begin, count)
        return remote(rows, rows, core_send.at[slot], core_recv.at[slot], partner)

    fetches[0].wait()
    fetches[1].wait()
    for part in range(2):
        rows = tokens[part * half : (part + 1) * half, :].astype(F32)
        held[pl.ds(pl.multiple_of(me * piece + part * half, half), half), :] = rms_scale(rows, gain[...]).astype(BF16)
        if part == 0:
            pl.semaphore_wait(barrier, planes * tp)
        across(part).start()
    to_core(me, 0, 0, piece).start()
    fetches[3].wait()
    for i in range(heads):
        lam_own[i] = jnp.broadcast_to(lam[:, i : i + 1], (8, LANES))
    lam_copy = remote(lam_own, lam_pair, lam_send, lam_recv, partner)
    lam_copy.start()

    def rotated(wide, at):
        turned = jnp.where(
            jnp.concatenate([low_half] * 2, axis=0),
            pltpu.roll(wide, LANES - AK // 2, 1), pltpu.roll(wide, AK // 2, 1),
        )
        return wide * cosine[at, :] + turned * sine[at, :]

    def phase_rows(phase):
        owner = y if phase == 0 else 1 - y
        return pl.ds(pl.multiple_of(owner * 2 * piece, 2 * piece), 2 * piece)

    def project(phase, index):
        return jnp.dot(held[phase_rows(phase), :], weights[index], preferred_element_type=F32)

    def qkv_target(i, c):
        return core * heads + i, c

    def qkv_copy(phase, i, c):
        return remote(
            stage.at[phase, i, c], land.at[0, phase, z], qkv_send.at[phase, i, c], qkv_recv.at[phase, z],
            {"sp": (core * heads + i) * 2 + x, "tp": y * 2 + c},
        )

    def qkv_is_own(i, c):
        return jnp.logical_and(core * heads + i == z, core == c)

    def attention_inputs(phase):
        at = phase_rows(phase)
        if phase == 0:
            fetches[4].wait()
        keys = project(phase, 0).astype(BF16).astype(F32)
        if phase == 0:
            fetches[5].wait()
        values = project(phase, 1).astype(BF16).astype(F32)
        if phase == 0:
            fetches[6].wait()
        queries = project(phase, 2).astype(BF16).astype(F32)
        for i in range(heads):
            span = slice(i * LANES, (i + 1) * LANES)
            key = rotated(keys[:, span], at).astype(BF16)
            value = values[:, span].T.astype(BF16)
            query = (rotated(queries[:, span], at) * AK ** (-0.5)).astype(BF16)
            for c in range(2):
                part = slice(c * piece, (c + 1) * piece)
                stage[phase, i, c, :piece, :] = key[part]
                stage[phase, i, c, piece : 2 * piece, :] = value[:, part]
                stage[phase, i, c, 2 * piece :, :] = query[part]
        for i in range(heads):
            for c in range(2):
                own = qkv_is_own(i, c)

                @pl.when(own)
                def _():
                    pltpu.make_async_copy(
                        stage.at[phase, i, c], land.at[0, phase, z], qkv_recv.at[phase, z]
                    ).start()

                @pl.when(jnp.logical_not(own))
                def _():
                    qkv_copy(phase, i, c).start()

    def recurrence_inputs(phase):
        for i in range(4):
            if phase == 0:
                fetches[7 + i].wait()
            recp[i, phase_rows(phase), :] = project(phase, 3 + i).astype(BF16)

    def plane_at(k):
        return (z, z + 1 - 2 * lax.rem(z, 2), lax.rem(z + 2, 4), planes - 1 - z)[k] if planes == 4 else lax.rem(z + k, planes)

    def kv_of(origin, phase, plane):
        return land.at[origin, phase, plane, : 2 * piece]

    def to_side(phase, plane):
        return remote(
            kv_of(0, phase, plane), kv_of(2, phase, plane),
            side_send.at[phase, plane], side_recv.at[phase, plane], beside,
        )

    def to_near(origin, phase, plane):
        return remote(
            kv_of(origin, phase, plane), kv_of(origin + 1, phase, plane),
            near_send.at[origin // 2, phase, plane], near_recv.at[origin // 2, phase, plane], partner,
        )

    def relay_plane(phase, k):
        plane = plane_at(k)
        remote(
            land.at[0, phase, plane], land.at[0, phase, plane],
            qkv_send.at[phase, 0, 0], qkv_recv.at[phase, plane], partner,
        ).wait_recv()
        to_side(phase, plane).start()
        to_near(0, phase, plane).start()

    def relay_side(phase, k):
        plane = plane_at(k)
        to_side(phase, plane).wait_recv()
        to_near(2, phase, plane).start()

    def settle(phase):
        for k in range(planes):
            for origin in (0, 2):
                to_near(origin, phase, plane_at(k)).wait_recv()

    row_at = lax.broadcasted_iota(jnp.int32, (BLOCK, 3 * BLOCK), 0)
    col_at = lax.rem(lax.broadcasted_iota(jnp.int32, (BLOCK, 3 * BLOCK), 1), BLOCK)
    triangles = (jnp.where(row_at >= col_at, 1.0, 0.0).astype(BF16), jnp.where(row_at <= col_at, 1.0, 0.0).astype(BF16))
    row_in = lax.broadcasted_iota(jnp.int32, (BLOCK, BLOCK), 0)
    col_in = lax.broadcasted_iota(jnp.int32, (BLOCK, BLOCK), 1)
    earlier = (row_in >= col_in, row_in <= col_in)
    ends = (BLOCK - 1, 0)
    middles = (BLOCK // 2 - 1, BLOCK // 2)
    blocks = length // BLOCK
    spans = [slice(h * LANES, (h + 1) * LANES) for h in range(heads)]

    def within_block(b):
        at = pl.ds(pl.multiple_of(b * BLOCK, BLOCK), BLOCK)
        queries = jax.nn.silu(recp[0, at, :].astype(F32))
        values = recp[3, at, :]
        scores, tails = [], []
        for d in range(2):
            keys = leak[d : d + 1, :] * jax.nn.sigmoid(-recp[1 + d, at, :].astype(F32))
            added = jnp.concatenate(
                [jnp.broadcast_to(decay[d, at, h : h + 1], (BLOCK, LANES)) for h in range(heads)], axis=1
            )
            logs = jnp.log1p(-keys) + added
            coarse = logs.astype(BF16)
            rest = logs - coarse.astype(F32)
            fine = rest.astype(BF16)
            finest = (rest - fine.astype(F32)).astype(BF16)
            cum = jnp.dot(
                triangles[d], jnp.concatenate([coarse, fine, finest], axis=0), preferred_element_type=F32
            )
            middle = cum[middles[d] : middles[d] + 1, :]
            last = cum[ends[d] : ends[d] + 1, :]
            reads = (queries * jnp.exp(cum - middle)).astype(BF16)
            writes = (keys * jnp.exp(middle - cum)).astype(BF16)
            tails.append((keys * jnp.exp(last - cum)).astype(BF16))
            carried = (queries * jnp.exp(cum)).astype(BF16)
            facts[b, d] = jnp.broadcast_to(jnp.exp(last), (8, width))
            scores.append([jnp.where(earlier[d], dot_t(reads[:, s], writes[:, s]), 0.0) for s in spans])
            for h in range(heads):
                cum_reads[h, at, d * LANES : (d + 1) * LANES] = carried[:, spans[h]]
        for h in range(heads):
            both = (scores[0][h] + scores[1][h]).astype(BF16)
            rec_sum[at, spans[h]] = jnp.dot(both, values[:, spans[h]], preferred_element_type=F32)
            adds[b, h] = dot_0(
                values[:, spans[h]], jnp.concatenate([tails[0][:, spans[h]], tails[1][:, spans[h]]], axis=1)
            )

    def within_phase(phase):
        owner = y if phase == 0 else 1 - y
        count = blocks // 2

        def some(j, carry):
            within_block(owner * count + 2 * j)
            within_block(owner * count + 2 * j + 1)
            return carry

        lax.fori_loop(0, count // 2, some, 0)

    def order(d):
        return range(blocks) if d == 0 else range(blocks - 1, -1, -1)

    def half_of(d):
        return slice(d * LANES, (d + 1) * LANES)

    first_row = lax.broadcasted_iota(jnp.int32, (PAD, LANES), 0) == 0

    def pack(target, moved, factor):
        target[:LANES, :] = moved.astype(BF16)
        wide = jnp.broadcast_to(factor, (PAD, LANES))
        coarse = wide.astype(BF16).astype(F32)
        target[LANES:, :] = jnp.where(first_row, coarse, wide - coarse).astype(BF16)

    def unpack(source):
        last = source[LANES:, :].astype(F32)
        return source[:LANES, :].astype(F32), last[0:1] + last[1:2]

    def local_states():
        for h in range(heads):
            for d in range(2):
                moved = jnp.zeros((LANES, LANES), F32)
                factor = jnp.ones((1, LANES), F32)
                for b in order(d):
                    step = facts[b, d, 0:1, spans[h]]
                    moved = moved * step + adds[b, h, :, half_of(d)]
                    factor = factor * step
                state[d, h] = moved
                fade[d, h] = jnp.broadcast_to(factor, (8, LANES))
                pack(pair_out.at[d, h], moved, factor)

    pair_copy = remote(pair_out, pair_in, pair_send, pair_recv, beside)

    def pair_states():
        pair_copy.wait_recv()
        for d in range(2):
            mine, factor = state[d, x], fade[d, x][0:1]
            other, other_factor = unpack(pair_in.at[d, x])
            joined = jnp.where(x == d, mine * other_factor + other, other * factor + mine)
            pack(plane_out.at[d], joined, factor * other_factor)
        for dz in range(1, planes):
            to_plane(lax.rem(z + dz, planes)).start()

    def to_plane(target):
        return remote(
            plane_out.at[jnp.where(target > z, 0, 1)], plane_in.at[z],
            plane_send.at[target], plane_recv.at[z], {"sp": target * 2 + x},
        )

    def from_plane(source):
        return remote(
            plane_out.at[0], plane_in.at[source],
            plane_send.at[source], plane_recv.at[source], {"sp": source * 2 + x},
        )

    next_copy = remote(next_out, next_in, next_send, next_recv, beside)

    def plane_states():
        plane_sum[...] = jnp.zeros_like(plane_sum)

        def fold(d):
            def one(step, carry):
                plane = step if d == 0 else planes - 1 - step
                from_plane(plane).wait_recv()
                moved, factor = unpack(plane_in.at[plane])
                plane_sum[d] = plane_sum[d] * factor + moved
                return carry

            return one

        lax.fori_loop(0, z, fold(0), 0)
        lax.fori_loop(0, planes - 1 - z, fold(1), 0)
        next_out[...] = plane_sum[...].astype(BF16)
        next_copy.start()

    def second_pass():
        next_copy.wait_recv()
        for h in range(heads):
            for d in range(2):
                entering = jnp.where(x == h, plane_sum[d], next_in[d].astype(F32))
                other, other_factor = unpack(pair_in.at[d, h])
                running = jnp.where(x == d, entering, entering * other_factor + other)
                for b in order(d):
                    before_block[b, h, :, half_of(d)] = running.astype(BF16)
                    running = running * facts[b, d, 0:1, spans[h]] + adds[b, h, :, half_of(d)]
            for b in range(blocks):
                at = slice(b * BLOCK, (b + 1) * BLOCK)
                whole = rec_sum[at, spans[h]] + dot_t(cum_reads[h, at, :], before_block[b, h])
                rec_stage[at, spans[h]] = rms_scale(whole, rec_gain[...]).astype(BF16)
        for dt in range(tp):
            rec_copy(dt).start()

    def rec_copy(dt):
        t = lax.rem(me + dt, tp)
        source = rec_stage.at[pl.ds(pl.multiple_of(t * piece, piece), piece)]
        if dt == 0:
            return pltpu.make_async_copy(source, rec_all.at[me], rec_recv.at[me])
        return remote(source, rec_all.at[me], rec_send.at[dt], rec_recv.at[me], {"tp": t})

    def rec_arrival(dt):
        t = lax.rem(me + dt, tp)
        return remote(rec_all.at[t], rec_all.at[t], rec_send.at[dt], rec_recv.at[t], {"tp": t})

    acc[...] = jnp.zeros_like(acc)
    peak[...] = jnp.full_like(peak, -jnp.inf)
    sub = 2 * piece
    ones = jnp.ones((PAD, sub), BF16)
    low_map = lane < AK
    sub_count = 4 * planes * piece // sub

    def key_block(phase, u, part):
        block = 2 * u + part
        return block // planes, phase, block % planes

    def attend_step(phase, made, made_score, made_top, used, used_score):
        if made is not None:
            q_phase, tile = made
            query = land[0, q_phase, tile, 2 * piece :, :]
            none = jnp.zeros_like(query)
            both = jnp.concatenate([jnp.where(low_map, query, none), jnp.where(low_map, none, query)], axis=0)
            top = None
        if used is not None:
            q_phase_used, tile_used, used_top = used
            slot = q_phase_used * planes + tile_used
            before = peak[slot][0:1]
            now = jnp.maximum(before, jnp.max(used_top[...], axis=0, keepdims=True))
            mixed = acc[slot] * jnp.exp(before - now)
        for u in range(sub_count):
            at = slice(u * sub, (u + 1) * sub)
            if made is not None:
                keys = jnp.concatenate(
                    [land[(*key_block(phase, u, part), slice(0, piece))] for part in range(2)], axis=0
                )
                scores = dot_t(keys, both)
                made_score[at, :] = scores
                high = jnp.max(scores.reshape(sub // 8, 8, 2 * piece), axis=0)
                top = high if top is None else jnp.maximum(top, high)
            if used is not None:
                expo = jnp.exp(used_score[at, :] - now).astype(BF16)
                values = jnp.concatenate(
                    [land[(*key_block(phase, u, part), slice(piece, 2 * piece))] for part in range(2)], axis=1
                )
                values = jnp.concatenate([values, ones], axis=0)
                mixed = mixed + jnp.dot(values, expo, preferred_element_type=F32)
        if used is not None:
            acc[slot] = mixed
            peak[slot] = jnp.broadcast_to(now, (8, 2 * piece))
        if made is not None:
            made_top[...] = top

    def attend(q_phase, phase, after):
        attend_step(phase, (q_phase, 0), score_a, top_a, None, None)
        buffers = ((score_a, top_a), (score_b, top_b))
        for tile in range(1, planes + 1):
            used_score, used_top = buffers[(tile - 1) % 2]
            made_score, made_top = buffers[tile % 2]
            made = (q_phase, tile) if tile < planes else None
            attend_step(phase, made, made_score, made_top, (q_phase, tile - 1, used_top), used_score)
            after(tile - 1)

    def att_target(q_phase, tile):
        owner = y if q_phase == 0 else 1 - y
        return owner, {"sp": tile * 2 + x, "tp": owner * 2 + core}

    def att_copy(q_phase, tile):
        owner, to = att_target(q_phase, tile)
        return remote(
            att_stage.at[q_phase, tile], att_all.at[y * planes + z],
            att_send.at[q_phase, tile], att_recv.at[y * planes + z], to,
        )

    def finish(q_phase, tile):
        whole = acc[q_phase * planes + tile]
        ratio = whole[:LANES] / whole[LANES : LANES + 1]
        weight = jnp.where(core == lax.div(z, heads), lam_own[lax.rem(z, heads)], lam_pair[lax.rem(z, heads)])[0:1]
        values = ratio[:, :piece] - weight * ratio[:, piece:]
        scale = lax.rsqrt(jnp.mean(values * values, axis=0, keepdims=True) + EPS)
        att_stage[q_phase, tile] = ((values * scale).T * att_gain[...]).astype(BF16)
        if q_phase == 0:
            own = tile == z

            @pl.when(own)
            def _():
                pltpu.make_async_copy(
                    att_stage.at[q_phase, tile], att_all.at[y * planes + z], att_recv.at[y * planes + z]
                ).start()

            @pl.when(jnp.logical_not(own))
            def _():
                att_copy(q_phase, tile).start()
        else:
            att_copy(q_phase, tile).start()

    def att_arrival(index):
        return remote(att_all.at[index], att_all.at[index], att_send.at[0, 0], att_recv.at[index], partner)

    def nothing(tile):
        pass

    columns = min(512, out.shape[1])

    to_core(y * 2 + 1 - core, 0, 0, piece).wait_recv()
    attention_inputs(0)
    recurrence_inputs(0)
    for i in range(11, 15):
        fetches[i].wait()
    relay_plane(0, 0)
    within_phase(0)
    relay_plane(0, 1)
    for part in range(2):
        from_across(part).wait_recv()
        to_core((1 - y) * 2 + core, 1 + part, part * half, half).start()
    relay_side(0, 0)
    for part in range(2):
        to_core((1 - y) * 2 + 1 - core, 1 + part, part * half, half).wait_recv()
    attention_inputs(1)
    relay_plane(0, 2)
    relay_plane(0, 3)
    relay_side(0, 1)
    recurrence_inputs(1)
    within_phase(1)
    local_states()
    pair_copy.start()
    relay_plane(1, 0)
    relay_side(0, 2)
    relay_side(0, 3)
    settle(0)
    lam_copy.wait_recv()

    def while_early(tile):
        if tile == 0:
            pair_states()
            relay_plane(1, 1)
        if tile == 1:
            relay_plane(1, 2)
            relay_side(1, 0)
        if tile == 2:
            relay_plane(1, 3)

    attend(0, 0, while_early)

    def while_later(tile):
        if tile == 0:
            relay_side(1, 1)
            plane_states()
        if tile == 1:
            relay_side(1, 2)
        if tile == 2:
            relay_side(1, 3)

    attend(1, 0, while_later)
    second_pass()
    settle(1)
    attend(0, 1, functools.partial(finish, 0))
    fetches[15].wait()
    fetches[16].wait()
    for dt in range(tp):
        rec_arrival(dt).wait_recv()
    rec_rows = jnp.concatenate([rec_all[t] for t in range(tp)], axis=1)
    for n in range(0, out.shape[1], columns):
        total[:, n : n + columns] = jnp.dot(rec_rows, w_out_rec[:, n : n + columns], preferred_element_type=F32)
    attend(1, 1, functools.partial(finish, 1))
    for index in range(2 * planes):
        att_arrival(index).wait_recv()
    att_rows = jnp.concatenate([att_all[i] for i in range(2 * planes)], axis=1)
    for n in range(0, out.shape[1], columns):
        out[:, n : n + columns] = (
            total[:, n : n + columns]
            + jnp.dot(att_rows, w_out_att[:, n : n + columns], preferred_element_type=F32)
        ).astype(BF16)

    for part in range(2):
        across(part).wait_send()
        to_core((1 - y) * 2 + core, 1 + part, part * half, half).wait_send()
    to_core(me, 0, 0, piece).wait_send()
    lam_copy.wait_send()
    for phase in range(2):
        for i in range(heads):
            for c in range(2):

                @pl.when(jnp.logical_not(qkv_is_own(i, c)))
                def _():
                    qkv_copy(phase, i, c).wait_send()

        for k in range(planes):
            to_side(phase, plane_at(k)).wait_send()
            to_near(0, phase, plane_at(k)).wait_send()
            to_near(2, phase, plane_at(k)).wait_send()
    pair_copy.wait_send()
    next_copy.wait_send()
    for dz in range(1, planes):
        to_plane(lax.rem(z + dz, planes)).wait_send()
    for dt in range(1, tp):
        rec_copy(dt).wait_send()
    for tile in range(planes):

        @pl.when(tile != z)
        def _():
            att_copy(0, tile).wait_send()

        att_copy(1, tile).wait_send()


def rotary_table(piece, pieces):
    frequency = THETA ** (-(np.arange(LANES) % (AK // 2)) * 2.0 / AK)
    inside = np.arange(piece)[:, None] * frequency[None, :]
    base = (np.arange(pieces) * piece)[:, None] * frequency[None, :]
    return np.concatenate([np.cos(inside), np.sin(inside), np.cos(base), np.sin(base)]).astype(np.float32)


def on_device(
    tokens, norm_gain, rec_query, fwd_gate, bwd_gate, rec_value, gate_leak, log_decay, rec_gain,
    att_query, att_key, att_value, lambdas, att_gain, out_rec, out_att,
):
    ranks = lax.axis_size("sp")
    tp = lax.axis_size("tp")
    heads = rec_query.shape[1] // HK
    planes = ranks // 2
    piece, model = tokens.shape
    if tp != 4 or planes != 2 * heads or planes != 4 or piece != LANES:
        return on_device_general(
            tokens, norm_gain, rec_query, fwd_gate, bwd_gate, rec_value, gate_leak, log_decay, rec_gain,
            att_query, att_key, att_value, lambdas, att_gain, out_rec, out_att,
        )
    length = piece * tp
    width = heads * LANES
    blocks = length // BLOCK
    keys = 4 * planes * piece
    anywhere = pl.BlockSpec(memory_space=pl.ANY)
    dma = pltpu.SemaphoreType.DMA
    vmem = pltpu.VMEM
    table = jnp.asarray(rotary_table(piece, ranks * tp))
    return pl.pallas_call(
        functools.partial(fused_kernel, ranks, tp, heads, planes),
        out_shape=jax.ShapeDtypeStruct((piece, model), BF16),
        in_specs=[anywhere] * 17,
        out_specs=pl.BlockSpec(memory_space=pltpu.VMEM),
        scratch_shapes=[
            vmem((piece, model), BF16),
            vmem((1, model), F32),
            vmem((7, model, width), BF16),
            vmem((2, width), F32),
            vmem((2, length, heads), F32),
            vmem((1, LANES), F32),
            vmem((1, heads), F32),
            vmem((1, LANES), F32),
            vmem(out_rec.shape, BF16),
            vmem(out_att.shape, BF16),
            vmem(table.shape, F32),
            vmem((length, model), BF16),
            vmem((length, LANES), F32),
            vmem((length, LANES), F32),
            vmem((heads, 8, LANES), F32),
            vmem((heads, 8, LANES), F32),
            vmem((2, heads, 2, 3 * piece, LANES), BF16),
            vmem((4, 2, planes, 3 * piece, LANES), BF16),
            vmem((4, length, width), BF16),
            vmem((heads, length, 2 * LANES), BF16),
            vmem((blocks, 2, 8, width), F32),
            vmem((blocks, heads, LANES, 2 * LANES), F32),
            vmem((length, width), F32),
            vmem((2, heads, LANES, LANES), F32),
            vmem((2, heads, 8, LANES), F32),
            vmem((2, heads, LANES + PAD, LANES), BF16),
            vmem((2, heads, LANES + PAD, LANES), BF16),
            vmem((2, LANES + PAD, LANES), BF16),
            vmem((planes, LANES + PAD, LANES), BF16),
            vmem((2, LANES, LANES), F32),
            vmem((2, LANES, LANES), BF16),
            vmem((2, LANES, LANES), BF16),
            vmem((blocks, heads, LANES, 2 * LANES), BF16),
            vmem((length, width), BF16),
            vmem((tp, piece, width), BF16),
            vmem((keys, 2 * piece), F32),
            vmem((keys, 2 * piece), F32),
            vmem((8, 2 * piece), F32),
            vmem((8, 2 * piece), F32),
            vmem((2 * planes, LANES + PAD, 2 * piece), F32),
            vmem((2 * planes, 8, 2 * piece), F32),
            vmem((2, planes, piece, LANES), BF16),
            vmem((2 * planes, piece, LANES), BF16),
            vmem((piece, model), F32),
            dma((17,)), dma((2,)), dma((2,)), dma((3,)), dma((3,)), dma, dma,
            dma((2, heads, 2)), dma((2, planes)), dma((2, planes)), dma((2, planes)),
            dma((2, 2, planes)), dma((2, 2, planes)),
            dma, dma, dma((planes,)), dma((planes,)), dma, dma,
            dma((tp,)), dma((tp,)), dma((2, planes)), dma((2 * planes,)),
        ],
        compiler_params=pltpu.CompilerParams(
            collective_id=2, has_side_effects=True, vmem_limit_bytes=60 * 1024 * 1024
        ),
        cost_estimate=pl.CostEstimate(flops=10**10, bytes_accessed=10**7, transcendentals=10**7),
    )(
        tokens, norm_gain.reshape(1, -1), att_key, att_value, att_query, rec_query, fwd_gate, bwd_gate, rec_value,
        gate_leak, log_decay, rec_gain.reshape(1, LANES), lambdas.reshape(1, heads), att_gain.reshape(1, LANES),
        out_rec, out_att, table,
    )


def solution(mesh):
    placed = (
        P(("sp", "tp"), None), P(), P(None, "tp"), P(None, "tp"), P(None, "tp"), P(None, "tp"),
        P(None, "tp"), P(None, "sp", "tp"), P(), P(None, "tp"), P(None, "tp"), P(None, "tp"),
        P("tp"), P(), P(), P(),
    )
    return jax.shard_map(
        on_device, mesh=mesh, in_specs=placed, out_specs=P(("sp", "tp"), None), check_vma=False
    )
```

```python
import functools

import jax
import jax.numpy as jnp
import numpy as np
from jax import lax
from jax.experimental import pallas as pl
from jax.experimental.pallas import tpu as pltpu
from jax.sharding import PartitionSpec as P

HK = 128
AK = 64
BLOCK = 64
LANES = 128
EPS = 1e-06
THETA = 500000.0
HIGHEST = lax.Precision.HIGHEST
F32 = jnp.float32
BF16 = jnp.bfloat16
PAD = 16


def rms_scale(values, gain):
    return values * lax.rsqrt(jnp.mean(values * values, axis=-1, keepdims=True) + EPS) * gain


def dot_t(a, b):
    return lax.dot_general(a, b, (((1,), (1,)), ((), ())), preferred_element_type=F32)


def dot_0(a, b):
    return lax.dot_general(a, b, (((0,), (0,)), ((), ())), preferred_element_type=F32)


def gather_kernel(tp, tokens, gain, *refs):
    weights, outs = refs[:7], refs[7:14]
    held, across, along, landed = refs[14:]
    me = lax.axis_index("tp")
    core = lax.rem(me, 2)
    pair = lax.div(me, 2)
    pairs = tp // 2
    count = tokens.shape[0]
    partner = pair * 2 + 1 - core
    others = [lax.rem(pair + k, pairs) for k in range(1, pairs)]
    barrier = pltpu.get_barrier_semaphore()
    pl.semaphore_signal(barrier, inc=1, device_id={"tp": partner})
    for q in others:
        pl.semaphore_signal(barrier, inc=1, device_id={"tp": q * 2 + core})

    def rows_at(block):
        return held.at[pl.ds(pl.multiple_of(block * count, count), count)]

    def to_partner(block):
        return pltpu.make_async_remote_copy(
            src_ref=rows_at(block),
            dst_ref=rows_at(block),
            send_sem=across.at[block],
            recv_sem=landed.at[block],
            device_id={"tp": partner},
        )

    def to_pair(q):
        return pltpu.make_async_remote_copy(
            src_ref=rows_at(me),
            dst_ref=rows_at(me),
            send_sem=along.at[q],
            recv_sem=landed.at[me],
            device_id={"tp": q * 2 + core},
        )

    normed = rms_scale(tokens[...].astype(F32), gain[...]).astype(BF16)
    held[pl.ds(pl.multiple_of(me * count, count), count), :] = normed
    pl.semaphore_wait(barrier, pairs)
    for q in others:
        to_pair(q).start()
    to_partner(me).start()

    def step(k, carry):
        q = lax.rem(pair + k, pairs)
        near = q * 2 + core

        @pl.when(k > 0)
        def _():
            to_partner(near).wait_recv()
            to_partner(near).start()

        to_partner(q * 2 + 1 - core).wait_recv()
        at = pl.ds(pl.multiple_of(q * 2 * count, 2 * count), 2 * count)
        for weight, result in zip(weights, outs):
            result[at, :] = jnp.dot(held[at, :], weight[...], preferred_element_type=F32).astype(BF16)
        return carry

    lax.fori_loop(0, pairs, step, 0)
    to_partner(me).wait_send()
    for q in others:
        to_pair(q).wait_send()
        to_partner(q * 2 + core).wait_send()


def mixer_kernel(
    ranks, tp, groups, heads, tile,
    proj_k, proj_v, proj_q, proj_rq, proj_fwd, proj_bwd, proj_rv, cosine, sine, leak, decay, lam, rec_gain, att_gain,
    out,
    kv, rest, swap, stage, state_out, state_in, cums, adds, states, rec_sum, peak, total, mixed,
    kv_send, kv_recv, swap_send, rest_recv, state_send, state_recv, out_send, out_recv,
):
    me = lax.axis_index("sp")
    slot = lax.rem(me, groups)
    mine = lax.div(me, groups)
    mesh_column = lax.axis_index("tp")
    length = proj_k.shape[0]
    piece = length // tp
    rows = groups * length
    width = heads * LANES
    block_count = rows // BLOCK
    partner_slot = groups - 1 - slot
    partner = mine * groups + partner_slot
    blocks = ranks // groups
    own_rows = pl.ds(pl.multiple_of(slot * length, length), length)
    other_rows = pl.ds(pl.multiple_of(partner_slot * length, length), length)

    barrier = pltpu.get_barrier_semaphore()
    peers = []
    for k in range(1, blocks):
        peers.append(lax.rem(mine + k, blocks))
    for peer in peers:
        pl.semaphore_signal(barrier, inc=1, device_id={"sp": peer * groups + slot})
    owners = []
    for dp in range(groups):
        for dt in range(tp):
            owners.append((dp, dt, lax.rem(slot + dp, groups), lax.rem(mesh_column + dt, tp)))
    for dp, dt, p, t in owners[1:]:
        pl.semaphore_signal(barrier, inc=1, device_id={"sp": mine * groups + p, "tp": t})

    lane = lax.broadcasted_iota(jnp.int32, (length, LANES), 1)
    low_half = lax.rem(lane, AK) < AK // 2

    def rotated(raw):
        wide = raw.astype(F32)
        turned = jnp.where(low_half, -pltpu.roll(wide, LANES - AK // 2, 1), pltpu.roll(wide, AK // 2, 1))
        return wide * cosine[...] + turned * sine[...]

    def prepare(head_group, key_value, others):
        def taken(ref, h):
            return ref[:, pl.ds(pl.multiple_of((head_group * heads + h) * LANES, LANES), LANES)]

        for h in range(heads):
            at = h * LANES
            key_value[:, at : at + LANES] = rotated(taken(proj_k, h)).astype(BF16)
            key_value[:, width + at : width + at + LANES] = taken(proj_v, h)
            others[:, at : at + LANES] = (rotated(taken(proj_q, h)) * AK ** (-0.5)).astype(BF16)
            for i, ref in enumerate((proj_rq, proj_fwd, proj_bwd, proj_rv)):
                others[:, (i + 1) * width + at : (i + 1) * width + at + LANES] = taken(ref, h)

    if groups > 1:
        prepare(partner_slot, swap.at[:, : 2 * width], swap.at[:, 2 * width :])
    prepare(slot, kv.at[mine, own_rows], rest.at[own_rows])
    pl.semaphore_wait(barrier, blocks - 1 + groups * tp - 1)

    def block_copy(source_rows, source_slot, peer):
        return pltpu.make_async_remote_copy(
            src_ref=kv.at[mine, source_rows],
            dst_ref=kv.at[mine, source_rows],
            send_sem=kv_send.at[peer, source_slot],
            recv_sem=kv_recv.at[mine, source_slot],
            device_id={"sp": peer * groups + slot},
        )

    def arrival(block, piece):
        piece_rows = pl.ds(pl.multiple_of(piece * length, length), length)
        return pltpu.make_async_remote_copy(
            src_ref=kv.at[block, piece_rows],
            dst_ref=kv.at[block, piece_rows],
            send_sem=kv_send.at[block, piece],
            recv_sem=kv_recv.at[block, piece],
            device_id={"sp": block * groups + slot},
        )

    if groups > 1:
        swap_kv = pltpu.make_async_remote_copy(
            src_ref=swap.at[:, : 2 * width],
            dst_ref=kv.at[mine, own_rows],
            send_sem=swap_send.at[0],
            recv_sem=kv_recv.at[mine, slot],
            device_id={"sp": partner},
        )
        swap_kv.start()
        swap_rest = pltpu.make_async_remote_copy(
            src_ref=swap.at[:, 2 * width :],
            dst_ref=rest.at[own_rows],
            send_sem=swap_send.at[1],
            recv_sem=rest_recv,
            device_id={"sp": partner},
        )
    own_copies = [block_copy(own_rows, slot, peer) for peer in peers]
    for copy in own_copies:
        copy.start()
    other_copies = []
    if groups > 1:
        swap_rest.start()
        arrival(mine, partner_slot).wait_recv()
        other_copies = [block_copy(other_rows, partner_slot, peer) for peer in peers]
        for copy in other_copies:
            copy.start()
        swap_rest.wait_recv()

    row_at = lax.broadcasted_iota(jnp.int32, (BLOCK, BLOCK), 0)
    col_at = lax.broadcasted_iota(jnp.int32, (BLOCK, BLOCK), 1)
    earlier = (row_at >= col_at, row_at <= col_at)
    triangles = tuple(mask.astype(F32) for mask in earlier)
    ends = (BLOCK - 1, 0)
    middles = (BLOCK // 2 - 1, BLOCK // 2)

    def rows_of(direction, step):
        index = step if direction == 0 else block_count - 1 - step
        return index, pl.ds(pl.multiple_of(index * BLOCK, BLOCK), BLOCK)

    def part(at, index, h):
        return rest[at, (index * heads + h) * LANES : (index * heads + h + 1) * LANES].astype(F32)

    def keys_of(at, direction, h):
        return leak[h, direction : direction + 1, :] * jax.nn.sigmoid(-part(at, 2 + direction, h))

    states[...] = jnp.zeros_like(states)
    rec_sum[...] = jnp.zeros_like(rec_sum)

    def first_pass(step, totals):
        after = []
        for h in range(heads):
            for d in range(2):
                index, at = rows_of(d, step)
                keys = keys_of(at, d, h)
                column = d * heads + h
                logs = jnp.log1p(-keys) + decay[at, column : column + 1]
                cum = jnp.dot(triangles[d], logs, precision=HIGHEST, preferred_element_type=F32)
                cums[h, d, at, :] = cum
                last = cum[ends[d] : ends[d] + 1, :]
                scaled = (keys * jnp.exp(last - cum)).astype(BF16)
                added = dot_0(part(at, 4, h).astype(BF16), scaled)
                adds[h, d, index] = added
                states[h, d] = states[h, d] * jnp.exp(last) + added
                after.append(totals[h * 2 + d] + last)
        return tuple(after)

    nothing = tuple(jnp.zeros((1, LANES), F32) for _ in range(2 * heads))
    sums = lax.fori_loop(0, block_count, first_pass, nothing, unroll=2)
    for h in range(heads):
        for d in range(2):
            state_out[d, h, :LANES, :] = states[h, d].astype(BF16)
            factor = jnp.broadcast_to(jnp.exp(sums[h * 2 + d]), (PAD, LANES))
            coarse = factor.astype(BF16)
            fine = (factor - coarse.astype(F32)).astype(BF16)
            first_row = lax.broadcasted_iota(jnp.int32, (PAD, LANES), 0) == 0
            state_out[d, h, LANES:, :] = jnp.where(first_row, coarse.astype(F32), fine.astype(F32)).astype(BF16)
    state_copies = []
    for peer in peers:
        copy = pltpu.make_async_remote_copy(
            src_ref=state_out.at[jnp.where(peer > mine, 0, 1)],
            dst_ref=state_in.at[mine],
            send_sem=state_send.at[peer],
            recv_sem=state_recv.at[mine],
            device_id={"sp": peer * groups + slot},
        )
        copy.start()
        state_copies.append(copy)

    lane_q = lax.broadcasted_iota(jnp.int32, (tile, LANES), 1)
    tiles = rows // tile
    peak[...] = jnp.full_like(peak, -jnp.inf)
    total[...] = jnp.zeros_like(total)
    mixed[...] = jnp.zeros_like(mixed)

    def attend(block):
        for h in range(heads):
            at = h * LANES

            def one_tile(index, carry):
                q_rows = pl.ds(pl.multiple_of(index * tile, tile), tile)
                queries = rest[q_rows, at : at + LANES]
                zero = jnp.zeros_like(queries)
                both = jnp.concatenate(
                    [jnp.where(lane_q < AK, queries, zero), jnp.where(lane_q < AK, zero, queries)], axis=0
                )
                scores = dot_t(both, kv[block, :, at : at + LANES])
                before = peak[h, index][:, :1]
                raised = jnp.maximum(before, jnp.max(scores, axis=-1, keepdims=True))
                shrink = jnp.exp(before - raised)
                expo = jnp.exp(scores - raised)
                sums_now = total[h, index][:, :1] * shrink + jnp.sum(expo, axis=-1, keepdims=True)
                product = jnp.dot(
                    expo.astype(BF16), kv[block, :, width + at : width + at + LANES], preferred_element_type=F32
                )
                mixed[h, index] = mixed[h, index] * shrink + product
                peak[h, index] = jnp.broadcast_to(raised, (2 * tile, LANES))
                total[h, index] = jnp.broadcast_to(sums_now, (2 * tile, LANES))
                return carry

            lax.fori_loop(0, tiles, one_tile, 0)

    attend(mine)

    def state_arrival(block):
        return pltpu.make_async_remote_copy(
            src_ref=state_out.at[0],
            dst_ref=state_in.at[block],
            send_sem=state_send.at[block],
            recv_sem=state_recv.at[block],
            device_id={"sp": block * groups + slot},
        )

    states[...] = jnp.zeros_like(states)

    def compose(d):
        def body(step, carry):
            block = step if d == 0 else blocks - 1 - step
            state_arrival(block).wait_recv()
            for h in range(heads):
                rows_last = state_in[block, h, LANES:, :].astype(F32)
                factor = rows_last[0:1] + rows_last[1:2]
                states[h, d] = states[h, d] * factor + state_in[block, h, :LANES, :].astype(F32)
            return carry

        return body

    lax.fori_loop(0, mine, compose(0), 0)
    lax.fori_loop(0, blocks - 1 - mine, compose(1), 0)

    def second_pass(step, carry):
        for h in range(heads):
            for d in range(2):
                index, at = rows_of(d, step)
                queries = jax.nn.silu(part(at, 1, h))
                keys = keys_of(at, d, h)
                cum = cums[h, d, at, :]
                middle = cum[middles[d] : middles[d] + 1, :]
                last = cum[ends[d] : ends[d] + 1, :]
                scores = dot_t(
                    (queries * jnp.exp(cum - middle)).astype(BF16), (keys * jnp.exp(middle - cum)).astype(BF16)
                )
                scores = jnp.where(earlier[d], scores, 0.0)
                within = jnp.dot(scores.astype(BF16), part(at, 4, h).astype(BF16), preferred_element_type=F32)
                before = states[h, d]
                carried = dot_t_state(queries * jnp.exp(cum), before)
                span = slice(h * LANES, (h + 1) * LANES)
                rec_sum[at, span] = rec_sum[at, span] + within + carried
                states[h, d] = before * jnp.exp(last) + adds[h, d, index]
        return carry

    def dot_t_state(reads, state):
        return dot_t(reads.astype(BF16), state.astype(BF16))

    lax.fori_loop(0, block_count, second_pass, 0, unroll=2)

    for h in range(heads):
        span = slice(h * LANES, (h + 1) * LANES)
        stage[:, span] = rms_scale(rec_sum[:, span], rec_gain[...]).astype(BF16)

    def hand_over(which, owner):
        dp, dt, p, t = owner
        columns = slice(which * width, (which + 1) * width)
        source = stage.at[pl.ds(pl.multiple_of(p * length + t * piece, piece), piece), columns]
        target = out.at[mesh_column, slot, :, columns]
        if dp == 0 and dt == 0:
            return pltpu.make_async_copy(source, target, out_send.at[which, dp, dt])
        return pltpu.make_async_remote_copy(
            src_ref=source,
            dst_ref=target,
            send_sem=out_send.at[which, dp, dt],
            recv_sem=out_recv.at[which, mesh_column, slot],
            device_id={"sp": mine * groups + p, "tp": t},
        )

    def taken_over(which, owner):
        dp, dt, p, t = owner
        columns = slice(which * width, (which + 1) * width)
        target = out.at[t, p, :, columns]
        return pltpu.make_async_remote_copy(
            src_ref=target,
            dst_ref=target,
            send_sem=out_send.at[which, dp, dt],
            recv_sem=out_recv.at[which, t, p],
            device_id={"sp": mine * groups + p, "tp": t},
        )

    for owner in owners:
        hand_over(0, owner).start()

    def next_block(turn, carry):
        near = lax.div(turn + 1, 2)
        away = jnp.where(lax.rem(turn, 2) == 1, near, blocks - near)
        block = lax.rem(mine + away, blocks)
        for piece in range(groups):
            arrival(block, piece).wait_recv()
        attend(block)
        return carry

    lax.fori_loop(1, blocks, next_block, 0)

    for h in range(heads):
        span = slice(width + h * LANES, width + (h + 1) * LANES)
        for index in range(tiles):
            ratio = mixed[h, index] / total[h, index][:, :1]
            values = ratio[:tile] - lam[h] * ratio[tile:]
            stage[index * tile : (index + 1) * tile, span] = rms_scale(values, att_gain[...]).astype(BF16)
    for owner in owners:
        hand_over(1, owner).start()

    for copy in own_copies + other_copies + state_copies:
        copy.wait_send()
    if groups > 1:
        swap_kv.wait_send()
        swap_rest.wait_send()
    for which in range(2):
        hand_over(which, owners[0]).wait()
        for owner in owners[1:]:
            hand_over(which, owner).wait_send()
            taken_over(which, owner).wait_recv()


def on_device_general(
    tokens, norm_gain, rec_query, fwd_gate, bwd_gate, rec_value, gate_leak, log_decay, rec_gain,
    att_query, att_key, att_value, lambdas, att_gain, out_rec, out_att,
):
    ranks = lax.axis_size("sp")
    tp = lax.axis_size("tp")
    local_heads = rec_query.shape[1] // HK
    groups = 2 if local_heads % 2 == 0 and ranks % 2 == 0 else 1
    heads = local_heads // groups
    width = heads * LANES
    slot = lax.axis_index("sp") % groups

    order = (att_key, att_value, att_query, rec_query, fwd_gate, bwd_gate, rec_value)
    length = tokens.shape[0] * tp
    vmem = pl.BlockSpec(memory_space=pltpu.VMEM)
    dma = pltpu.SemaphoreType.DMA
    projected = pl.pallas_call(
        functools.partial(gather_kernel, tp),
        out_shape=[jax.ShapeDtypeStruct((length, weight.shape[1]), BF16) for weight in order],
        in_specs=[vmem] * (2 + len(order)),
        out_specs=[vmem] * len(order),
        scratch_shapes=[
            pltpu.VMEM((length, tokens.shape[1]), BF16),
            dma((tp,)),
            dma((tp // 2,)),
            dma((tp,)),
        ],
        compiler_params=pltpu.CompilerParams(
            collective_id=1, has_side_effects=True, vmem_limit_bytes=40 * 1024 * 1024
        ),
        cost_estimate=pl.CostEstimate(flops=4 * 10**9, bytes_accessed=10**7, transcendentals=0),
    )(tokens, norm_gain.reshape(1, -1), *order)

    positions = (lax.axis_index("sp") * length + jnp.arange(length, dtype=jnp.int32)).astype(F32)
    frequency = THETA ** (-(jnp.arange(AK // 2, dtype=F32) * 2.0 / AK))
    angles = jnp.tile(positions[:, None] * frequency[None, :], (1, LANES // (AK // 2)))
    cosine, sine = jnp.cos(angles), jnp.sin(angles)

    by_head = log_decay.reshape(2, length, groups, heads).transpose(2, 1, 0, 3).reshape(groups, length, 2 * heads)
    own_decay = lax.dynamic_index_in_dim(by_head, slot, 0, keepdims=False)
    if groups > 1:
        swapped = lax.ppermute(
            lax.dynamic_index_in_dim(by_head, groups - 1 - slot, 0, keepdims=False),
            "sp",
            [(i, i + 1 - 2 * (i % 2)) for i in range(ranks)],
        )
        decay = jnp.where(
            slot == 0, jnp.concatenate([own_decay, swapped]), jnp.concatenate([swapped, own_decay])
        )
    else:
        decay = own_decay
    leak = lax.dynamic_index_in_dim(
        gate_leak.reshape(2, groups, heads, HK).transpose(1, 2, 0, 3), slot, 0, keepdims=False
    )
    lam = lax.dynamic_index_in_dim(lambdas.reshape(groups, heads), slot, 0, keepdims=False)
    lam = jnp.broadcast_to(lam[:, None, None], (heads, 1, LANES))

    blocks = ranks // groups
    rows = groups * length
    tile = min(256, length)
    mixers = pl.pallas_call(
        functools.partial(mixer_kernel, ranks, tp, groups, heads, tile),
        out_shape=jax.ShapeDtypeStruct((tp, groups, length // tp, 2 * width), BF16),
        in_specs=[vmem] * 14,
        out_specs=vmem,
        scratch_shapes=[
            pltpu.VMEM((blocks, rows, 2 * width), BF16),
            pltpu.VMEM((rows, 5 * width), BF16),
            pltpu.VMEM((length, 7 * width), BF16),
            pltpu.VMEM((rows, 2 * width), BF16),
            pltpu.VMEM((2, heads, LANES + PAD, LANES), BF16),
            pltpu.VMEM((blocks, heads, LANES + PAD, LANES), BF16),
            pltpu.VMEM((heads, 2, rows, LANES), F32),
            pltpu.VMEM((heads, 2, rows // BLOCK, LANES, LANES), F32),
            pltpu.VMEM((heads, 2, LANES, LANES), F32),
            pltpu.VMEM((rows, width), F32),
            pltpu.VMEM((heads, rows // tile, 2 * tile, LANES), F32),
            pltpu.VMEM((heads, rows // tile, 2 * tile, LANES), F32),
            pltpu.VMEM((heads, rows // tile, 2 * tile, LANES), F32),
            dma((blocks, groups)),
            dma((blocks, groups)),
            dma((2,)),
            dma,
            dma((blocks,)),
            dma((blocks,)),
            dma((2, groups, tp)),
            dma((2, tp, groups)),
        ],
        compiler_params=pltpu.CompilerParams(
            collective_id=0, has_side_effects=True, vmem_limit_bytes=56 * 1024 * 1024
        ),
        cost_estimate=pl.CostEstimate(flops=10**10, bytes_accessed=10**7, transcendentals=10**7),
    )(*projected, cosine, sine, leak, decay, lam, rec_gain.reshape(1, LANES), att_gain.reshape(1, LANES))

    shares = mixers.reshape(tp, groups, length // tp, 2, heads, LANES)
    both = shares.transpose(2, 3, 0, 1, 4, 5).reshape(length // tp, 2, -1)
    result = jnp.dot(both[:, 0], out_rec, preferred_element_type=F32) + jnp.dot(
        both[:, 1], out_att, preferred_element_type=F32
    )
    return result.astype(BF16)


def fused_kernel(
    ranks, tp, heads, planes,
    tokens_in, norm_in, w_key, w_value, w_query, w_rq, w_fwd, w_bwd, w_rv, leak_in, decay_in, rec_gain_in,
    lam_in, att_gain_in, out_rec_in, out_att_in, rotary_in,
    out,
    tokens, gain, weights, leak, decay, decay_rows, rec_gain, lam, att_gain, w_out_rec, w_out_att, rotary,
    held, cosine, sine, lam_own, lam_pair, stage_kv, stage_q, kv, query, recp, cum_reads, facts, adds, rec_sum,
    state, fade, pair_out, pair_in, plane_out, plane_in, plane_sum, next_out, next_in, before_block,
    rec_stage, rec_all, score_a, score_b, top_a, top_b, acc, peak, att_stage, att_all, total,
    in_sem, across_send, across_recv, core_send, core_recv, lam_send, lam_recv,
    kv_send, kv_recv, q_send, q_recv, side_send, side_recv, near_send, near_recv,
    pair_send, pair_recv, plane_send, plane_recv, next_send, next_recv,
    rec_send, rec_recv, att_send, att_recv,
):
    sp = lax.axis_index("sp")
    me = lax.axis_index("tp")
    x = lax.rem(sp, 2)
    z = lax.div(sp, 2)
    core = lax.rem(me, 2)
    y = lax.div(me, 2)
    piece = tokens.shape[0]
    half = piece // 2
    length = piece * tp
    width = heads * LANES
    partner = {"tp": y * 2 + 1 - core}
    opposite = {"tp": (1 - y) * 2 + core}
    beside = {"sp": z * 2 + 1 - x}

    small = (
        (rotary_in, rotary), (lam_in, lam), (leak_in, leak), (decay_in, decay),
        (rec_gain_in, rec_gain), (att_gain_in, att_gain),
    )
    inputs = (w_key, w_value, w_query, w_rq, w_fwd, w_bwd, w_rv)
    moves = (
        [(tokens_in, tokens), (norm_in, gain)]
        + [(a, weights.at[i]) for i, a in enumerate(inputs)]
        + list(small) + [(out_rec_in, w_out_rec), (out_att_in, w_out_att)]
    )
    fetches = [pltpu.make_async_copy(a, b, in_sem.at[i]) for i, (a, b) in enumerate(moves)]
    f_rotary, f_lam, f_leak, f_decay, f_rec_gain, f_att_gain = fetches[9:15]
    for fetch in fetches[:2] + fetches[9:11]:
        fetch.start()

    barrier = pltpu.get_barrier_semaphore()
    for dz in range(planes):
        for dt in range(tp):
            if dz or dt:
                to = {"sp": lax.rem(z + dz, planes) * 2 + x, "tp": lax.rem(me + dt, tp)}
                pl.semaphore_signal(barrier, inc=1, device_id=to)
    pl.semaphore_signal(barrier, inc=1, device_id=beside)

    def remote(source, target, send, recv, to):
        return pltpu.make_async_remote_copy(
            src_ref=source, dst_ref=target, send_sem=send, recv_sem=recv, device_id=to
        )

    def held_at(owner, part, side):
        return owner * 2 * piece + part * piece + side * half

    def held_rows(owner, part, side):
        return held.at[pl.ds(pl.multiple_of(held_at(owner, part, side), half), half)]

    def across(part, owner):
        rows = held_rows(owner, part, core)
        return remote(rows, rows, across_send.at[part], across_recv.at[part], opposite)

    def to_core(owner, part, side, slot):
        rows = held_rows(owner, part, side)
        return remote(rows, rows, core_send.at[slot], core_recv.at[slot], partner)

    fetches[0].wait()
    fetches[1].wait()
    for fetch in fetches[2:9] + fetches[11:15]:
        fetch.start()
    for part in range(2):
        rows = tokens[part * half : (part + 1) * half, :].astype(F32)
        at = pl.ds(pl.multiple_of(held_at(y, part, core), half), half)
        held[at, :] = rms_scale(rows, gain[...]).astype(BF16)
        if part == 0:
            pl.semaphore_wait(barrier, planes * tp)
        across(part, y).start()
        to_core(y, part, core, part).start()
    f_lam.wait()
    for i in range(heads):
        lam_own[i] = jnp.broadcast_to(lam[:, i : i + 1], (8, LANES))
    lam_copy = remote(lam_own, lam_pair, lam_send, lam_recv, partner)
    lam_copy.start()

    f_rotary.wait()
    lane = lax.broadcasted_iota(jnp.int32, (piece, LANES), 1)
    low_half = lax.rem(lane, AK) < AK // 2
    for t in range(tp):
        begin = 2 * piece + sp * tp + t
        cos_base = rotary[pl.ds(begin, 1), :]
        sin_base = rotary[pl.ds(begin + ranks * tp, 1), :]
        cos_row, sin_row = rotary[:piece, :], rotary[piece : 2 * piece, :]
        turned = sin_base * cos_row + cos_base * sin_row
        cos_here = cos_base * cos_row - sin_base * sin_row
        sin_here = jnp.where(low_half, -turned, turned)
        for part in range(2):
            to = held_at(t // 2, part, t % 2)
            cosine[to : to + half, :] = cos_here[part * half : (part + 1) * half]
            sine[to : to + half, :] = sin_here[part * half : (part + 1) * half]

    def rotated(wide, cos_at, sin_at):
        rows = wide.shape[0]
        low = jnp.concatenate([low_half] * (rows // piece), axis=0)
        turned = jnp.where(low, pltpu.roll(wide, LANES - AK // 2, 1), pltpu.roll(wide, AK // 2, 1))
        return wide * cos_at + turned * sin_at

    def owner_of(phase):
        return y if phase < 2 else 1 - y

    def plane_copy(phase, i, kind):
        return remote(
            stage_kv.at[phase, i, kind], kv.at[kind, 0, phase, z], kv_send.at[phase, i, kind], kv_recv.at[phase, z],
            {"sp": (core * heads + i) * 2 + x, "tp": y * 2 + kind},
        )

    def query_rows(phase, plane):
        return query.at[phase, pl.ds(pl.multiple_of(plane * half, half), half)]

    def query_copy(phase, i, c):
        return remote(
            stage_q.at[phase, i, c], query_rows(phase, z), q_send.at[phase, i, c], q_recv.at[phase, z],
            {"sp": (core * heads + i) * 2 + x, "tp": y * 2 + c},
        )

    def is_own(i, c):
        return jnp.logical_and(core * heads + i == z, core == c)

    def project(at, index):
        return jnp.dot(held[at, :], weights[index], preferred_element_type=F32)

    def attention_inputs(phases):
        count = len(phases) * piece
        owner = owner_of(phases[0])
        at = pl.ds(pl.multiple_of(held_at(owner, phases[0] % 2, 0), piece), count)
        cos_at, sin_at = cosine[at, :], sine[at, :]
        if phases[0] == 0:
            fetches[2].wait()
        keys = project(at, 0).astype(BF16).astype(F32)
        if phases[0] == 0:
            fetches[3].wait()
        values = project(at, 1).astype(BF16).astype(F32)
        for i in range(heads):
            span = slice(i * LANES, (i + 1) * LANES)
            value = values[:, span].T.astype(BF16)
            key = rotated(keys[:, span], cos_at, sin_at).astype(BF16)
            for n, phase in enumerate(phases):
                part = slice(n * piece, (n + 1) * piece)
                stage_kv[phase, i, 0] = value[:, part]
                stage_kv[phase, i, 1] = key[part]
        for phase in phases:
            send_each(phase, plane_copy, kv_recv, lambda i, c: (stage_kv.at[phase, i, c], kv.at[c, 0, phase, z]))
        if phases[0] == 0:
            fetches[4].wait()
        queries = project(at, 2).astype(BF16).astype(F32)
        for i in range(heads):
            span = slice(i * LANES, (i + 1) * LANES)
            turned = (rotated(queries[:, span], cos_at, sin_at) * AK ** (-0.5)).astype(BF16)
            for n, phase in enumerate(phases):
                for c in range(2):
                    stage_q[phase, i, c] = turned[n * piece + c * half : n * piece + (c + 1) * half]
        for phase in phases:
            send_each(phase, query_copy, q_recv, lambda i, c: (stage_q.at[phase, i, c], query_rows(phase, z)))

    def send_each(phase, copy, recv, local):
        for i in range(heads):
            for c in range(2):
                own = is_own(i, c)

                @pl.when(own)
                def _():
                    source, target = local(i, c)
                    pltpu.make_async_copy(source, target, recv.at[phase, z]).start()

                @pl.when(jnp.logical_not(own))
                def _():
                    copy(phase, i, c).start()

    def recurrence_inputs(owner, wait):
        at = pl.ds(pl.multiple_of(held_at(owner, 0, 0), 2 * piece), 2 * piece)
        for i in range(4):
            if wait:
                fetches[5 + i].wait()
            recp[i, at, :] = project(at, 3 + i).astype(BF16)

    def plane_at(k):
        return (z, z + 1 - 2 * lax.rem(z, 2), lax.rem(z + 2, planes), planes - 1 - z)[k]

    def mine_of(origin, phase, plane):
        return kv.at[core, origin, phase, plane]

    def to_side(phase, plane):
        return remote(
            mine_of(0, phase, plane), mine_of(1, phase, plane),
            side_send.at[phase, plane], side_recv.at[phase, plane], beside,
        )

    def to_near(origin, phase, plane):
        block = mine_of(origin, phase, plane)
        return remote(
            block, block, near_send.at[origin, phase, plane], near_recv.at[origin, phase, plane], partner
        )

    def from_near(origin, phase, plane):
        block = kv.at[1 - core, origin, phase, plane]
        return remote(
            block, block, near_send.at[origin, phase, plane], near_recv.at[origin, phase, plane], partner
        )

    def relay_plane(phase, k):
        plane = plane_at(k)
        block = mine_of(0, phase, plane)
        remote(block, block, near_send.at[0, phase, plane], kv_recv.at[phase, plane], partner).wait_recv()
        to_side(phase, plane).start()
        to_near(0, phase, plane).start()

    def relay_side(phase, k):
        plane = plane_at(k)
        block = mine_of(1, phase, plane)
        remote(block, block, side_send.at[phase, plane], side_recv.at[phase, plane], beside).wait_recv()
        to_near(1, phase, plane).start()

    def settle(phase):
        for k in range(planes):
            for origin in range(2):
                from_near(origin, phase, plane_at(k)).wait_recv()

    def settle_queries(phase):
        for k in range(planes):
            rows = query_rows(phase, plane_at(k))
            remote(rows, rows, q_send.at[phase, 0, 0], q_recv.at[phase, plane_at(k)], partner).wait_recv()

    row_at = lax.broadcasted_iota(jnp.int32, (BLOCK, 3 * BLOCK), 0)
    col_at = lax.rem(lax.broadcasted_iota(jnp.int32, (BLOCK, 3 * BLOCK), 1), BLOCK)
    triangles = (jnp.where(row_at >= col_at, 1.0, 0.0).astype(BF16), jnp.where(row_at <= col_at, 1.0, 0.0).astype(BF16))
    row_in = lax.broadcasted_iota(jnp.int32, (BLOCK, BLOCK), 0)
    col_in = lax.broadcasted_iota(jnp.int32, (BLOCK, BLOCK), 1)
    earlier = (row_in >= col_in, row_in <= col_in)
    ends = (BLOCK - 1, 0)
    middles = (BLOCK // 2 - 1, BLOCK // 2)
    blocks = length // BLOCK
    spans = [slice(h * LANES, (h + 1) * LANES) for h in range(heads)]

    def within_block(b):
        at = pl.ds(pl.multiple_of(b * BLOCK, BLOCK), BLOCK)
        t = lax.div(b, 2)
        stored = held_at(lax.div(t, 2), lax.rem(b, 2), lax.rem(t, 2))
        held_block = pl.ds(pl.multiple_of(stored, BLOCK), BLOCK)
        queries = jax.nn.silu(recp[0, held_block, :].astype(F32))
        values = recp[3, held_block, :]
        scores, tails = [], []
        for d in range(2):
            keys = leak[d : d + 1, :] * jax.nn.sigmoid(-recp[1 + d, held_block, :].astype(F32))
            added = jnp.concatenate(
                [jnp.broadcast_to(decay_rows[at, d * heads + h : d * heads + h + 1], (BLOCK, LANES)) for h in range(heads)],
                axis=1,
            )
            logs = jnp.log1p(-keys) + added
            coarse = logs.astype(BF16)
            rest = logs - coarse.astype(F32)
            fine = rest.astype(BF16)
            finest = (rest - fine.astype(F32)).astype(BF16)
            cum = jnp.dot(
                triangles[d], jnp.concatenate([coarse, fine, finest], axis=0), preferred_element_type=F32
            )
            middle = cum[middles[d] : middles[d] + 1, :]
            last = cum[ends[d] : ends[d] + 1, :]
            reads = (queries * jnp.exp(cum - middle)).astype(BF16)
            writes = (keys * jnp.exp(middle - cum)).astype(BF16)
            tails.append((keys * jnp.exp(last - cum)).astype(BF16))
            carried = (queries * jnp.exp(cum)).astype(BF16)
            facts[b, d] = jnp.broadcast_to(jnp.exp(last), (8, width))
            scores.append([jnp.where(earlier[d], dot_t(reads[:, s], writes[:, s]), 0.0) for s in spans])
            for h in range(heads):
                cum_reads[h, at, d * LANES : (d + 1) * LANES] = carried[:, spans[h]]
        for h in range(heads):
            both = (scores[0][h] + scores[1][h]).astype(BF16)
            rec_sum[at, spans[h]] = jnp.dot(both, values[:, spans[h]], preferred_element_type=F32)
            adds[b, h] = dot_0(
                values[:, spans[h]], jnp.concatenate([tails[0][:, spans[h]], tails[1][:, spans[h]]], axis=1)
            )

    def within_rows(owner):
        count = blocks // 2

        def some(j, carry):
            within_block(owner * count + 2 * j)
            within_block(owner * count + 2 * j + 1)
            return carry

        lax.fori_loop(0, count // 2, some, 0)

    def order(d):
        return range(blocks) if d == 0 else range(blocks - 1, -1, -1)

    def half_of(d):
        return slice(d * LANES, (d + 1) * LANES)

    first_row = lax.broadcasted_iota(jnp.int32, (PAD, LANES), 0) == 0

    def pack(target, moved, factor):
        target[:LANES, :] = moved.astype(BF16)
        wide = jnp.broadcast_to(factor, (PAD, LANES))
        coarse = wide.astype(BF16).astype(F32)
        target[LANES:, :] = jnp.where(first_row, coarse, wide - coarse).astype(BF16)

    def unpack(source):
        last = source[LANES:, :].astype(F32)
        return source[:LANES, :].astype(F32), last[0:1] + last[1:2]

    def local_states():
        for h in range(heads):
            for d in range(2):
                moved = jnp.zeros((LANES, LANES), F32)
                factor = jnp.ones((1, LANES), F32)
                for b in order(d):
                    step = facts[b, d, 0:1, spans[h]]
                    moved = moved * step + adds[b, h, :, half_of(d)]
                    factor = factor * step
                state[d, h] = moved
                fade[d, h] = jnp.broadcast_to(factor, (8, LANES))
                pack(pair_out.at[d, h], moved, factor)

    pair_copy = remote(pair_out, pair_in, pair_send, pair_recv, beside)

    def pair_states():
        pair_copy.wait_recv()
        for d in range(2):
            mine, factor = state[d, x], fade[d, x][0:1]
            other, other_factor = unpack(pair_in.at[d, x])
            joined = jnp.where(x == d, mine * other_factor + other, other * factor + mine)
            pack(plane_out.at[d], joined, factor * other_factor)
        for dz in range(1, planes):
            to_plane(lax.rem(z + dz, planes)).start()

    def to_plane(target):
        return remote(
            plane_out.at[jnp.where(target > z, 0, 1)], plane_in.at[z],
            plane_send.at[target], plane_recv.at[z], {"sp": target * 2 + x},
        )

    def from_plane(source):
        return remote(
            plane_out.at[0], plane_in.at[source],
            plane_send.at[source], plane_recv.at[source], {"sp": source * 2 + x},
        )

    next_copy = remote(next_out, next_in, next_send, next_recv, beside)

    def plane_states():
        plane_sum[...] = jnp.zeros_like(plane_sum)

        def fold(d):
            def one(step, carry):
                plane = step if d == 0 else planes - 1 - step
                from_plane(plane).wait_recv()
                moved, factor = unpack(plane_in.at[plane])
                plane_sum[d] = plane_sum[d] * factor + moved
                return carry

            return one

        lax.fori_loop(0, z, fold(0), 0)
        lax.fori_loop(0, planes - 1 - z, fold(1), 0)
        next_out[...] = plane_sum[...].astype(BF16)
        next_copy.start()

    def second_pass():
        next_copy.wait_recv()
        for h in range(heads):
            for d in range(2):
                entering = jnp.where(x == h, plane_sum[d], next_in[d].astype(F32))
                other, other_factor = unpack(pair_in.at[d, h])
                running = jnp.where(x == d, entering, entering * other_factor + other)
                for b in order(d):
                    before_block[b, h, :, half_of(d)] = running.astype(BF16)
                    running = running * facts[b, d, 0:1, spans[h]] + adds[b, h, :, half_of(d)]
            for b in range(blocks):
                at = slice(b * BLOCK, (b + 1) * BLOCK)
                whole = rec_sum[at, spans[h]] + dot_t(cum_reads[h, at, :], before_block[b, h])
                rec_stage[at, spans[h]] = rms_scale(whole, rec_gain[...]).astype(BF16)
        for dt in range(tp):
            rec_copy(dt).start()

    def rec_copy(dt):
        t = lax.rem(me + dt, tp)
        source = rec_stage.at[pl.ds(pl.multiple_of(t * piece, piece), piece)]
        if dt == 0:
            return pltpu.make_async_copy(source, rec_all.at[me], rec_recv.at[me])
        return remote(source, rec_all.at[me], rec_send.at[dt], rec_recv.at[me], {"tp": t})

    def rec_arrival(dt):
        t = lax.rem(me + dt, tp)
        return remote(rec_all.at[t], rec_all.at[t], rec_send.at[dt], rec_recv.at[t], {"tp": t})

    acc[...] = jnp.zeros_like(acc)
    peak[...] = jnp.full_like(peak, -jnp.inf)
    sub = 2 * piece
    ones = jnp.ones((PAD, sub), BF16)
    low_map = lane < AK
    chunk_blocks = 2 * planes
    buffers = ((score_a, top_a), (score_b, top_b))

    def attend_step(made, made_buffer, used, used_buffer):
        if made is not None:
            q_phase, tile, made_phase = made
            rows = query[q_phase, tile * piece : (tile + 1) * piece, :]
            none = jnp.zeros_like(rows)
            both = jnp.concatenate([jnp.where(low_map, rows, none), jnp.where(low_map, none, rows)], axis=0)
            top = None
        if used is not None:
            slot, used_phase = used[0] * 2 + used[1], used[2]
            used_score, used_top = used_buffer
            before = peak[slot][0:1]
            now = jnp.maximum(before, jnp.max(used_top[...], axis=0, keepdims=True))
            mixed = acc[slot] * jnp.exp(before - now)
        for u in range(0, chunk_blocks, 2):
            at = slice(u * piece, (u + 2) * piece)
            where = [((u + n) // planes, (u + n) % planes) for n in range(2)]
            if made is not None:
                keys = jnp.concatenate([kv[1, o, made_phase, p] for o, p in where], axis=0)
                scores = dot_t(keys, both)
                made_buffer[0][at, :] = scores
                high = jnp.max(scores.reshape(sub // 8, 8, 2 * piece), axis=0)
                top = high if top is None else jnp.maximum(top, high)
            if used is not None:
                expo = jnp.exp(used_score[at, :] - now).astype(BF16)
                values = jnp.concatenate([kv[0, o, used_phase, p] for o, p in where], axis=1)
                values = jnp.concatenate([values, ones], axis=0)
                mixed = mixed + jnp.dot(values, expo, preferred_element_type=F32)
        if used is not None:
            acc[slot] = mixed
            peak[slot] = jnp.broadcast_to(now, (8, 2 * piece))
        if made is not None:
            made_buffer[1][...] = top

    def att_copy(q_phase, plane):
        owner, part = owner_of(q_phase), q_phase % 2
        return remote(
            att_stage.at[q_phase, plane], att_all.at[y * planes + z, part * half : (part + 1) * half],
            att_send.at[q_phase, plane], att_recv.at[y * planes + z, part],
            {"sp": plane * 2 + x, "tp": owner * 2 + core},
        )

    def finish(q_phase, tile):
        whole = acc[q_phase * 2 + tile]
        ratio = whole[:LANES] / whole[LANES : LANES + 1]
        weight = jnp.where(core == lax.div(z, heads), lam_own[lax.rem(z, heads)], lam_pair[lax.rem(z, heads)])[0:1]
        values = ratio[:, :piece] - weight * ratio[:, piece:]
        scale = lax.rsqrt(jnp.mean(values * values, axis=0, keepdims=True) + EPS)
        rows = ((values * scale).T * att_gain[...]).astype(BF16)
        part = q_phase % 2
        for n in range(2):
            plane = 2 * tile + n
            att_stage[q_phase, plane] = rows[n * half : (n + 1) * half]
            if q_phase < 2:

                @pl.when(plane == z)
                def _():
                    pltpu.make_async_copy(
                        att_stage.at[q_phase, plane],
                        att_all.at[y * planes + z, part * half : (part + 1) * half],
                        att_recv.at[y * planes + z, part],
                    ).start()

                @pl.when(plane != z)
                def _():
                    att_copy(q_phase, plane).start()
            else:
                att_copy(q_phase, plane).start()

    def att_arrival(index, part):
        rows = att_all.at[index, part * half : (part + 1) * half]
        return remote(rows, rows, att_send.at[0, 0], att_recv.at[index, part], partner)

    columns = min(512, out.shape[1])

    def rec_total():
        for fetch in fetches[15:17]:
            fetch.wait()
        for dt in range(tp):
            rec_arrival(dt).wait_recv()
        rec_rows = jnp.concatenate([rec_all[t] for t in range(tp)], axis=1)
        for n in range(0, out.shape[1], columns):
            total[:, n : n + columns] = jnp.dot(rec_rows, w_out_rec[:, n : n + columns], preferred_element_type=F32)

    def both_tiles(q_phase, key_phase):
        return [(q_phase, tile, key_phase) for tile in range(2)]

    def plan():
        units, before = [], {}

        def at_next(*actions):
            before.setdefault(len(units), []).extend(actions)

        def call(f, *args):
            return functools.partial(f, *args)

        at_next(call(settle, 0), call(settle_queries, 0))
        units += both_tiles(0, 0)
        at_next(*(call(relay_side, 1, k) for k in range(4)))
        at_next(call(settle_queries, 1))
        units += both_tiles(1, 0)
        at_next(call(settle, 1))
        units += both_tiles(0, 1)
        at_next(pair_states, call(relay_plane, 2, 0), call(relay_plane, 2, 1))
        units += both_tiles(1, 1)
        at_next(call(relay_plane, 2, 2), call(relay_plane, 2, 3), call(settle_queries, 2))
        units += [(2, 0, 0)]
        at_next(*(call(relay_side, 2, k) for k in range(2)))
        units += [(2, 1, 0)]
        at_next(plane_states, call(relay_plane, 3, 0))
        units += [(2, 0, 1)]
        at_next(*(call(relay_side, 2, k) for k in range(2, 4)))
        at_next(call(relay_plane, 3, 1))
        units += [(2, 1, 1)]
        at_next(call(settle, 2))
        units += [(0, 0, 2)]
        at_next(call(relay_plane, 3, 2))
        units += [(0, 1, 2)]
        at_next(call(relay_plane, 3, 3))
        units += [(1, 0, 2)]
        at_next(call(relay_side, 3, 0), call(relay_side, 3, 1))
        units += [(1, 1, 2)]
        at_next(call(relay_side, 3, 2))
        units += both_tiles(2, 2)
        at_next(call(relay_side, 3, 3), second_pass, call(settle_queries, 3))
        units += both_tiles(3, 0) + both_tiles(3, 1) + both_tiles(3, 2)
        at_next(call(settle, 3))
        units += both_tiles(0, 3)
        at_next(rec_total)
        units += both_tiles(1, 3) + both_tiles(2, 3) + both_tiles(3, 3)
        return units, before

    for part in range(2):
        to_core(y, part, 1 - core, part).wait_recv()
    attention_inputs((0, 1))
    for fetch in fetches[15:17]:
        fetch.start()
    recurrence_inputs(y, True)
    for fetch in (f_leak, f_decay, f_rec_gain, f_att_gain):
        fetch.wait()
    by_row = jnp.concatenate([decay[d] for d in range(2)] + [jnp.zeros((LANES - 2 * heads, length), F32)], axis=0)
    decay_rows[...] = by_row.T
    relay_plane(0, 0)
    relay_plane(0, 1)
    relay_plane(1, 0)
    within_rows(y)
    across(0, 1 - y).wait_recv()
    to_core(1 - y, 0, core, 2).start()
    relay_plane(0, 2)
    relay_plane(0, 3)
    to_core(1 - y, 0, 1 - core, 2).wait_recv()
    attention_inputs((2,))
    for k in range(4):
        relay_side(0, k)
    relay_plane(1, 1)
    across(1, 1 - y).wait_recv()
    to_core(1 - y, 1, core, 3).start()
    relay_plane(1, 2)
    to_core(1 - y, 1, 1 - core, 3).wait_recv()
    attention_inputs((3,))
    relay_plane(1, 3)
    recurrence_inputs(1 - y, False)
    within_rows(1 - y)
    local_states()
    pair_copy.start()
    lam_copy.wait_recv()

    units, before = plan()
    for n in range(len(units) + 1):
        for action in before.get(n, ()):
            action()
        made = units[n] if n < len(units) else None
        used = units[n - 1] if n else None
        attend_step(made, buffers[n % 2], used, buffers[(n + 1) % 2])
        if used is not None and used[2] == 3:
            finish(used[0], used[1])

    for part in range(2):
        for index in range(2 * planes):
            att_arrival(index, part).wait_recv()
    att_rows = jnp.concatenate([att_all[i] for i in range(2 * planes)], axis=1)
    for n in range(0, out.shape[1], columns):
        out[:, n : n + columns] = (
            total[:, n : n + columns]
            + jnp.dot(att_rows, w_out_att[:, n : n + columns], preferred_element_type=F32)
        ).astype(BF16)

    for part in range(2):
        across(part, y).wait_send()
        to_core(y, part, core, part).wait_send()
        to_core(1 - y, part, core, 2 + part).wait_send()
    lam_copy.wait_send()
    for phase in range(4):
        for i in range(heads):
            for c in range(2):

                @pl.when(jnp.logical_not(is_own(i, c)))
                def _():
                    plane_copy(phase, i, c).wait_send()
                    query_copy(phase, i, c).wait_send()

        for k in range(planes):
            to_side(phase, plane_at(k)).wait_send()
            to_near(0, phase, plane_at(k)).wait_send()
            to_near(1, phase, plane_at(k)).wait_send()
    pair_copy.wait_send()
    next_copy.wait_send()
    for dz in range(1, planes):
        to_plane(lax.rem(z + dz, planes)).wait_send()
    for dt in range(1, tp):
        rec_copy(dt).wait_send()
    for plane in range(planes):
        for phase in range(4):
            if phase < 2:

                @pl.when(plane != z)
                def _():
                    att_copy(phase, plane).wait_send()
            else:
                att_copy(phase, plane).wait_send()


def rotary_table(piece, pieces):
    frequency = THETA ** (-(np.arange(LANES) % (AK // 2)) * 2.0 / AK)
    inside = np.arange(piece)[:, None] * frequency[None, :]
    base = (np.arange(pieces) * piece)[:, None] * frequency[None, :]
    return np.concatenate([np.cos(inside), np.sin(inside), np.cos(base), np.sin(base)]).astype(np.float32)


def on_device(
    tokens, norm_gain, rec_query, fwd_gate, bwd_gate, rec_value, gate_leak, log_decay, rec_gain,
    att_query, att_key, att_value, lambdas, att_gain, out_rec, out_att,
):
    ranks = lax.axis_size("sp")
    tp = lax.axis_size("tp")
    heads = rec_query.shape[1] // HK
    planes = ranks // 2
    piece, model = tokens.shape
    if tp != 4 or planes != 2 * heads or planes != 4 or piece != LANES:
        return on_device_general(
            tokens, norm_gain, rec_query, fwd_gate, bwd_gate, rec_value, gate_leak, log_decay, rec_gain,
            att_query, att_key, att_value, lambdas, att_gain, out_rec, out_att,
        )
    length = piece * tp
    width = heads * LANES
    blocks = length // BLOCK
    keys = 2 * planes * piece
    anywhere = pl.BlockSpec(memory_space=pl.ANY)
    dma = pltpu.SemaphoreType.DMA
    vmem = pltpu.VMEM
    table = jnp.asarray(rotary_table(piece, ranks * tp))
    return pl.pallas_call(
        functools.partial(fused_kernel, ranks, tp, heads, planes),
        out_shape=jax.ShapeDtypeStruct((piece, model), BF16),
        in_specs=[anywhere] * 17,
        out_specs=pl.BlockSpec(memory_space=pltpu.VMEM),
        scratch_shapes=[
            vmem((piece, model), BF16),
            vmem((1, model), F32),
            vmem((7, model, width), BF16),
            vmem((2, width), F32),
            vmem((2, heads, length), F32),
            vmem((length, LANES), F32),
            vmem((1, LANES), F32),
            vmem((1, heads), F32),
            vmem((1, LANES), F32),
            vmem(out_rec.shape, BF16),
            vmem(out_att.shape, BF16),
            vmem(table.shape, F32),
            vmem((length, model), BF16),
            vmem((length, LANES), F32),
            vmem((length, LANES), F32),
            vmem((heads, 8, LANES), F32),
            vmem((heads, 8, LANES), F32),
            vmem((4, heads, 2, piece, LANES), BF16),
            vmem((4, heads, 2, piece // 2, LANES), BF16),
            vmem((2, 2, 4, planes, piece, LANES), BF16),
            vmem((4, planes * piece // 2, LANES), BF16),
            vmem((4, length, width), BF16),
            vmem((heads, length, 2 * LANES), BF16),
            vmem((blocks, 2, 8, width), F32),
            vmem((blocks, heads, LANES, 2 * LANES), F32),
            vmem((length, width), F32),
            vmem((2, heads, LANES, LANES), F32),
            vmem((2, heads, 8, LANES), F32),
            vmem((2, heads, LANES + PAD, LANES), BF16),
            vmem((2, heads, LANES + PAD, LANES), BF16),
            vmem((2, LANES + PAD, LANES), BF16),
            vmem((planes, LANES + PAD, LANES), BF16),
            vmem((2, LANES, LANES), F32),
            vmem((2, LANES, LANES), BF16),
            vmem((2, LANES, LANES), BF16),
            vmem((blocks, heads, LANES, 2 * LANES), BF16),
            vmem((length, width), BF16),
            vmem((tp, piece, width), BF16),
            vmem((keys, 2 * piece), F32),
            vmem((keys, 2 * piece), F32),
            vmem((8, 2 * piece), F32),
            vmem((8, 2 * piece), F32),
            vmem((2 * planes, LANES + PAD, 2 * piece), F32),
            vmem((2 * planes, 8, 2 * piece), F32),
            vmem((4, planes, piece // 2, LANES), BF16),
            vmem((2 * planes, piece, LANES), BF16),
            vmem((piece, model), F32),
            dma((17,)), dma((2,)), dma((2,)), dma((4,)), dma((4,)), dma, dma,
            dma((4, heads, 2)), dma((4, planes)), dma((4, heads, 2)), dma((4, planes)),
            dma((4, planes)), dma((4, planes)), dma((2, 4, planes)), dma((2, 4, planes)),
            dma, dma, dma((planes,)), dma((planes,)), dma, dma,
            dma((tp,)), dma((tp,)), dma((4, planes)), dma((2 * planes, 2)),
        ],
        compiler_params=pltpu.CompilerParams(
            collective_id=2, has_side_effects=True, vmem_limit_bytes=60 * 1024 * 1024
        ),
        cost_estimate=pl.CostEstimate(flops=10**10, bytes_accessed=10**7, transcendentals=10**7),
    )(
        tokens, norm_gain.reshape(1, -1), att_key, att_value, att_query, rec_query, fwd_gate, bwd_gate, rec_value,
        gate_leak, log_decay.transpose(0, 2, 1), rec_gain.reshape(1, LANES), lambdas.reshape(1, heads), att_gain.reshape(1, LANES),
        out_rec, out_att, table,
    )


def solution(mesh):
    placed = (
        P(("sp", "tp"), None), P(), P(None, "tp"), P(None, "tp"), P(None, "tp"), P(None, "tp"),
        P(None, "tp"), P(None, "sp", "tp"), P(), P(None, "tp"), P(None, "tp"), P(None, "tp"),
        P("tp"), P(), P(), P(),
    )
    return jax.shard_map(
        on_device, mesh=mesh, in_specs=placed, out_specs=P(("sp", "tp"), None), check_vma=False
    )
```

```python
import functools

import jax
import jax.numpy as jnp
import numpy as np
from jax import lax
from jax.experimental import pallas as pl
from jax.experimental.pallas import tpu as pltpu
from jax.sharding import PartitionSpec as P

HK = 128
AK = 64
BLOCK = 64
LANES = 128
EPS = 1e-06
THETA = 500000.0
HIGHEST = lax.Precision.HIGHEST
F32 = jnp.float32
BF16 = jnp.bfloat16
PAD = 16


def rms_scale(values, gain):
    return values * lax.rsqrt(jnp.mean(values * values, axis=-1, keepdims=True) + EPS) * gain


def dot_t(a, b):
    return lax.dot_general(a, b, (((1,), (1,)), ((), ())), preferred_element_type=F32)


def dot_0(a, b):
    return lax.dot_general(a, b, (((0,), (0,)), ((), ())), preferred_element_type=F32)


def gather_kernel(tp, tokens, gain, *refs):
    weights, outs = refs[:7], refs[7:14]
    held, across, along, landed = refs[14:]
    me = lax.axis_index("tp")
    core = lax.rem(me, 2)
    pair = lax.div(me, 2)
    pairs = tp // 2
    count = tokens.shape[0]
    partner = pair * 2 + 1 - core
    others = [lax.rem(pair + k, pairs) for k in range(1, pairs)]
    barrier = pltpu.get_barrier_semaphore()
    pl.semaphore_signal(barrier, inc=1, device_id={"tp": partner})
    for q in others:
        pl.semaphore_signal(barrier, inc=1, device_id={"tp": q * 2 + core})

    def rows_at(block):
        return held.at[pl.ds(pl.multiple_of(block * count, count), count)]

    def to_partner(block):
        return pltpu.make_async_remote_copy(
            src_ref=rows_at(block),
            dst_ref=rows_at(block),
            send_sem=across.at[block],
            recv_sem=landed.at[block],
            device_id={"tp": partner},
        )

    def to_pair(q):
        return pltpu.make_async_remote_copy(
            src_ref=rows_at(me),
            dst_ref=rows_at(me),
            send_sem=along.at[q],
            recv_sem=landed.at[me],
            device_id={"tp": q * 2 + core},
        )

    normed = rms_scale(tokens[...].astype(F32), gain[...]).astype(BF16)
    held[pl.ds(pl.multiple_of(me * count, count), count), :] = normed
    pl.semaphore_wait(barrier, pairs)
    for q in others:
        to_pair(q).start()
    to_partner(me).start()

    def step(k, carry):
        q = lax.rem(pair + k, pairs)
        near = q * 2 + core

        @pl.when(k > 0)
        def _():
            to_partner(near).wait_recv()
            to_partner(near).start()

        to_partner(q * 2 + 1 - core).wait_recv()
        at = pl.ds(pl.multiple_of(q * 2 * count, 2 * count), 2 * count)
        for weight, result in zip(weights, outs):
            result[at, :] = jnp.dot(held[at, :], weight[...], preferred_element_type=F32).astype(BF16)
        return carry

    lax.fori_loop(0, pairs, step, 0)
    to_partner(me).wait_send()
    for q in others:
        to_pair(q).wait_send()
        to_partner(q * 2 + core).wait_send()


def mixer_kernel(
    ranks, tp, groups, heads, tile,
    proj_k, proj_v, proj_q, proj_rq, proj_fwd, proj_bwd, proj_rv, cosine, sine, leak, decay, lam, rec_gain, att_gain,
    out,
    kv, rest, swap, stage, state_out, state_in, cums, adds, states, rec_sum, peak, total, mixed,
    kv_send, kv_recv, swap_send, rest_recv, state_send, state_recv, out_send, out_recv,
):
    me = lax.axis_index("sp")
    slot = lax.rem(me, groups)
    mine = lax.div(me, groups)
    mesh_column = lax.axis_index("tp")
    length = proj_k.shape[0]
    piece = length // tp
    rows = groups * length
    width = heads * LANES
    block_count = rows // BLOCK
    partner_slot = groups - 1 - slot
    partner = mine * groups + partner_slot
    blocks = ranks // groups
    own_rows = pl.ds(pl.multiple_of(slot * length, length), length)
    other_rows = pl.ds(pl.multiple_of(partner_slot * length, length), length)

    barrier = pltpu.get_barrier_semaphore()
    peers = []
    for k in range(1, blocks):
        peers.append(lax.rem(mine + k, blocks))
    for peer in peers:
        pl.semaphore_signal(barrier, inc=1, device_id={"sp": peer * groups + slot})
    owners = []
    for dp in range(groups):
        for dt in range(tp):
            owners.append((dp, dt, lax.rem(slot + dp, groups), lax.rem(mesh_column + dt, tp)))
    for dp, dt, p, t in owners[1:]:
        pl.semaphore_signal(barrier, inc=1, device_id={"sp": mine * groups + p, "tp": t})

    lane = lax.broadcasted_iota(jnp.int32, (length, LANES), 1)
    low_half = lax.rem(lane, AK) < AK // 2

    def rotated(raw):
        wide = raw.astype(F32)
        turned = jnp.where(low_half, -pltpu.roll(wide, LANES - AK // 2, 1), pltpu.roll(wide, AK // 2, 1))
        return wide * cosine[...] + turned * sine[...]

    def prepare(head_group, key_value, others):
        def taken(ref, h):
            return ref[:, pl.ds(pl.multiple_of((head_group * heads + h) * LANES, LANES), LANES)]

        for h in range(heads):
            at = h * LANES
            key_value[:, at : at + LANES] = rotated(taken(proj_k, h)).astype(BF16)
            key_value[:, width + at : width + at + LANES] = taken(proj_v, h)
            others[:, at : at + LANES] = (rotated(taken(proj_q, h)) * AK ** (-0.5)).astype(BF16)
            for i, ref in enumerate((proj_rq, proj_fwd, proj_bwd, proj_rv)):
                others[:, (i + 1) * width + at : (i + 1) * width + at + LANES] = taken(ref, h)

    if groups > 1:
        prepare(partner_slot, swap.at[:, : 2 * width], swap.at[:, 2 * width :])
    prepare(slot, kv.at[mine, own_rows], rest.at[own_rows])
    pl.semaphore_wait(barrier, blocks - 1 + groups * tp - 1)

    def block_copy(source_rows, source_slot, peer):
        return pltpu.make_async_remote_copy(
            src_ref=kv.at[mine, source_rows],
            dst_ref=kv.at[mine, source_rows],
            send_sem=kv_send.at[peer, source_slot],
            recv_sem=kv_recv.at[mine, source_slot],
            device_id={"sp": peer * groups + slot},
        )

    def arrival(block, piece):
        piece_rows = pl.ds(pl.multiple_of(piece * length, length), length)
        return pltpu.make_async_remote_copy(
            src_ref=kv.at[block, piece_rows],
            dst_ref=kv.at[block, piece_rows],
            send_sem=kv_send.at[block, piece],
            recv_sem=kv_recv.at[block, piece],
            device_id={"sp": block * groups + slot},
        )

    if groups > 1:
        swap_kv = pltpu.make_async_remote_copy(
            src_ref=swap.at[:, : 2 * width],
            dst_ref=kv.at[mine, own_rows],
            send_sem=swap_send.at[0],
            recv_sem=kv_recv.at[mine, slot],
            device_id={"sp": partner},
        )
        swap_kv.start()
        swap_rest = pltpu.make_async_remote_copy(
            src_ref=swap.at[:, 2 * width :],
            dst_ref=rest.at[own_rows],
            send_sem=swap_send.at[1],
            recv_sem=rest_recv,
            device_id={"sp": partner},
        )
    own_copies = [block_copy(own_rows, slot, peer) for peer in peers]
    for copy in own_copies:
        copy.start()
    other_copies = []
    if groups > 1:
        swap_rest.start()
        arrival(mine, partner_slot).wait_recv()
        other_copies = [block_copy(other_rows, partner_slot, peer) for peer in peers]
        for copy in other_copies:
            copy.start()
        swap_rest.wait_recv()

    row_at = lax.broadcasted_iota(jnp.int32, (BLOCK, BLOCK), 0)
    col_at = lax.broadcasted_iota(jnp.int32, (BLOCK, BLOCK), 1)
    earlier = (row_at >= col_at, row_at <= col_at)
    triangles = tuple(mask.astype(F32) for mask in earlier)
    ends = (BLOCK - 1, 0)
    middles = (BLOCK // 2 - 1, BLOCK // 2)

    def rows_of(direction, step):
        index = step if direction == 0 else block_count - 1 - step
        return index, pl.ds(pl.multiple_of(index * BLOCK, BLOCK), BLOCK)

    def part(at, index, h):
        return rest[at, (index * heads + h) * LANES : (index * heads + h + 1) * LANES].astype(F32)

    def keys_of(at, direction, h):
        return leak[h, direction : direction + 1, :] * jax.nn.sigmoid(-part(at, 2 + direction, h))

    states[...] = jnp.zeros_like(states)
    rec_sum[...] = jnp.zeros_like(rec_sum)

    def first_pass(step, totals):
        after = []
        for h in range(heads):
            for d in range(2):
                index, at = rows_of(d, step)
                keys = keys_of(at, d, h)
                column = d * heads + h
                logs = jnp.log1p(-keys) + decay[at, column : column + 1]
                cum = jnp.dot(triangles[d], logs, precision=HIGHEST, preferred_element_type=F32)
                cums[h, d, at, :] = cum
                last = cum[ends[d] : ends[d] + 1, :]
                scaled = (keys * jnp.exp(last - cum)).astype(BF16)
                added = dot_0(part(at, 4, h).astype(BF16), scaled)
                adds[h, d, index] = added
                states[h, d] = states[h, d] * jnp.exp(last) + added
                after.append(totals[h * 2 + d] + last)
        return tuple(after)

    nothing = tuple(jnp.zeros((1, LANES), F32) for _ in range(2 * heads))
    sums = lax.fori_loop(0, block_count, first_pass, nothing, unroll=2)
    for h in range(heads):
        for d in range(2):
            state_out[d, h, :LANES, :] = states[h, d].astype(BF16)
            factor = jnp.broadcast_to(jnp.exp(sums[h * 2 + d]), (PAD, LANES))
            coarse = factor.astype(BF16)
            fine = (factor - coarse.astype(F32)).astype(BF16)
            first_row = lax.broadcasted_iota(jnp.int32, (PAD, LANES), 0) == 0
            state_out[d, h, LANES:, :] = jnp.where(first_row, coarse.astype(F32), fine.astype(F32)).astype(BF16)
    state_copies = []
    for peer in peers:
        copy = pltpu.make_async_remote_copy(
            src_ref=state_out.at[jnp.where(peer > mine, 0, 1)],
            dst_ref=state_in.at[mine],
            send_sem=state_send.at[peer],
            recv_sem=state_recv.at[mine],
            device_id={"sp": peer * groups + slot},
        )
        copy.start()
        state_copies.append(copy)

    lane_q = lax.broadcasted_iota(jnp.int32, (tile, LANES), 1)
    tiles = rows // tile
    peak[...] = jnp.full_like(peak, -jnp.inf)
    total[...] = jnp.zeros_like(total)
    mixed[...] = jnp.zeros_like(mixed)

    def attend(block):
        for h in range(heads):
            at = h * LANES

            def one_tile(index, carry):
                q_rows = pl.ds(pl.multiple_of(index * tile, tile), tile)
                queries = rest[q_rows, at : at + LANES]
                zero = jnp.zeros_like(queries)
                both = jnp.concatenate(
                    [jnp.where(lane_q < AK, queries, zero), jnp.where(lane_q < AK, zero, queries)], axis=0
                )
                scores = dot_t(both, kv[block, :, at : at + LANES])
                before = peak[h, index][:, :1]
                raised = jnp.maximum(before, jnp.max(scores, axis=-1, keepdims=True))
                shrink = jnp.exp(before - raised)
                expo = jnp.exp(scores - raised)
                sums_now = total[h, index][:, :1] * shrink + jnp.sum(expo, axis=-1, keepdims=True)
                product = jnp.dot(
                    expo.astype(BF16), kv[block, :, width + at : width + at + LANES], preferred_element_type=F32
                )
                mixed[h, index] = mixed[h, index] * shrink + product
                peak[h, index] = jnp.broadcast_to(raised, (2 * tile, LANES))
                total[h, index] = jnp.broadcast_to(sums_now, (2 * tile, LANES))
                return carry

            lax.fori_loop(0, tiles, one_tile, 0)

    attend(mine)

    def state_arrival(block):
        return pltpu.make_async_remote_copy(
            src_ref=state_out.at[0],
            dst_ref=state_in.at[block],
            send_sem=state_send.at[block],
            recv_sem=state_recv.at[block],
            device_id={"sp": block * groups + slot},
        )

    states[...] = jnp.zeros_like(states)

    def compose(d):
        def body(step, carry):
            block = step if d == 0 else blocks - 1 - step
            state_arrival(block).wait_recv()
            for h in range(heads):
                rows_last = state_in[block, h, LANES:, :].astype(F32)
                factor = rows_last[0:1] + rows_last[1:2]
                states[h, d] = states[h, d] * factor + state_in[block, h, :LANES, :].astype(F32)
            return carry

        return body

    lax.fori_loop(0, mine, compose(0), 0)
    lax.fori_loop(0, blocks - 1 - mine, compose(1), 0)

    def second_pass(step, carry):
        for h in range(heads):
            for d in range(2):
                index, at = rows_of(d, step)
                queries = jax.nn.silu(part(at, 1, h))
                keys = keys_of(at, d, h)
                cum = cums[h, d, at, :]
                middle = cum[middles[d] : middles[d] + 1, :]
                last = cum[ends[d] : ends[d] + 1, :]
                scores = dot_t(
                    (queries * jnp.exp(cum - middle)).astype(BF16), (keys * jnp.exp(middle - cum)).astype(BF16)
                )
                scores = jnp.where(earlier[d], scores, 0.0)
                within = jnp.dot(scores.astype(BF16), part(at, 4, h).astype(BF16), preferred_element_type=F32)
                before = states[h, d]
                carried = dot_t_state(queries * jnp.exp(cum), before)
                span = slice(h * LANES, (h + 1) * LANES)
                rec_sum[at, span] = rec_sum[at, span] + within + carried
                states[h, d] = before * jnp.exp(last) + adds[h, d, index]
        return carry

    def dot_t_state(reads, state):
        return dot_t(reads.astype(BF16), state.astype(BF16))

    lax.fori_loop(0, block_count, second_pass, 0, unroll=2)

    for h in range(heads):
        span = slice(h * LANES, (h + 1) * LANES)
        stage[:, span] = rms_scale(rec_sum[:, span], rec_gain[...]).astype(BF16)

    def hand_over(which, owner):
        dp, dt, p, t = owner
        columns = slice(which * width, (which + 1) * width)
        source = stage.at[pl.ds(pl.multiple_of(p * length + t * piece, piece), piece), columns]
        target = out.at[mesh_column, slot, :, columns]
        if dp == 0 and dt == 0:
            return pltpu.make_async_copy(source, target, out_send.at[which, dp, dt])
        return pltpu.make_async_remote_copy(
            src_ref=source,
            dst_ref=target,
            send_sem=out_send.at[which, dp, dt],
            recv_sem=out_recv.at[which, mesh_column, slot],
            device_id={"sp": mine * groups + p, "tp": t},
        )

    def taken_over(which, owner):
        dp, dt, p, t = owner
        columns = slice(which * width, (which + 1) * width)
        target = out.at[t, p, :, columns]
        return pltpu.make_async_remote_copy(
            src_ref=target,
            dst_ref=target,
            send_sem=out_send.at[which, dp, dt],
            recv_sem=out_recv.at[which, t, p],
            device_id={"sp": mine * groups + p, "tp": t},
        )

    for owner in owners:
        hand_over(0, owner).start()

    def next_block(turn, carry):
        near = lax.div(turn + 1, 2)
        away = jnp.where(lax.rem(turn, 2) == 1, near, blocks - near)
        block = lax.rem(mine + away, blocks)
        for piece in range(groups):
            arrival(block, piece).wait_recv()
        attend(block)
        return carry

    lax.fori_loop(1, blocks, next_block, 0)

    for h in range(heads):
        span = slice(width + h * LANES, width + (h + 1) * LANES)
        for index in range(tiles):
            ratio = mixed[h, index] / total[h, index][:, :1]
            values = ratio[:tile] - lam[h] * ratio[tile:]
            stage[index * tile : (index + 1) * tile, span] = rms_scale(values, att_gain[...]).astype(BF16)
    for owner in owners:
        hand_over(1, owner).start()

    for copy in own_copies + other_copies + state_copies:
        copy.wait_send()
    if groups > 1:
        swap_kv.wait_send()
        swap_rest.wait_send()
    for which in range(2):
        hand_over(which, owners[0]).wait()
        for owner in owners[1:]:
            hand_over(which, owner).wait_send()
            taken_over(which, owner).wait_recv()


def on_device_general(
    tokens, norm_gain, rec_query, fwd_gate, bwd_gate, rec_value, gate_leak, log_decay, rec_gain,
    att_query, att_key, att_value, lambdas, att_gain, out_rec, out_att,
):
    ranks = lax.axis_size("sp")
    tp = lax.axis_size("tp")
    local_heads = rec_query.shape[1] // HK
    groups = 2 if local_heads % 2 == 0 and ranks % 2 == 0 else 1
    heads = local_heads // groups
    width = heads * LANES
    slot = lax.axis_index("sp") % groups

    order = (att_key, att_value, att_query, rec_query, fwd_gate, bwd_gate, rec_value)
    length = tokens.shape[0] * tp
    vmem = pl.BlockSpec(memory_space=pltpu.VMEM)
    dma = pltpu.SemaphoreType.DMA
    projected = pl.pallas_call(
        functools.partial(gather_kernel, tp),
        out_shape=[jax.ShapeDtypeStruct((length, weight.shape[1]), BF16) for weight in order],
        in_specs=[vmem] * (2 + len(order)),
        out_specs=[vmem] * len(order),
        scratch_shapes=[
            pltpu.VMEM((length, tokens.shape[1]), BF16),
            dma((tp,)),
            dma((tp // 2,)),
            dma((tp,)),
        ],
        compiler_params=pltpu.CompilerParams(
            collective_id=1, has_side_effects=True, vmem_limit_bytes=40 * 1024 * 1024
        ),
        cost_estimate=pl.CostEstimate(flops=4 * 10**9, bytes_accessed=10**7, transcendentals=0),
    )(tokens, norm_gain.reshape(1, -1), *order)

    positions = (lax.axis_index("sp") * length + jnp.arange(length, dtype=jnp.int32)).astype(F32)
    frequency = THETA ** (-(jnp.arange(AK // 2, dtype=F32) * 2.0 / AK))
    angles = jnp.tile(positions[:, None] * frequency[None, :], (1, LANES // (AK // 2)))
    cosine, sine = jnp.cos(angles), jnp.sin(angles)

    by_head = log_decay.reshape(2, length, groups, heads).transpose(2, 1, 0, 3).reshape(groups, length, 2 * heads)
    own_decay = lax.dynamic_index_in_dim(by_head, slot, 0, keepdims=False)
    if groups > 1:
        swapped = lax.ppermute(
            lax.dynamic_index_in_dim(by_head, groups - 1 - slot, 0, keepdims=False),
            "sp",
            [(i, i + 1 - 2 * (i % 2)) for i in range(ranks)],
        )
        decay = jnp.where(
            slot == 0, jnp.concatenate([own_decay, swapped]), jnp.concatenate([swapped, own_decay])
        )
    else:
        decay = own_decay
    leak = lax.dynamic_index_in_dim(
        gate_leak.reshape(2, groups, heads, HK).transpose(1, 2, 0, 3), slot, 0, keepdims=False
    )
    lam = lax.dynamic_index_in_dim(lambdas.reshape(groups, heads), slot, 0, keepdims=False)
    lam = jnp.broadcast_to(lam[:, None, None], (heads, 1, LANES))

    blocks = ranks // groups
    rows = groups * length
    tile = min(256, length)
    mixers = pl.pallas_call(
        functools.partial(mixer_kernel, ranks, tp, groups, heads, tile),
        out_shape=jax.ShapeDtypeStruct((tp, groups, length // tp, 2 * width), BF16),
        in_specs=[vmem] * 14,
        out_specs=vmem,
        scratch_shapes=[
            pltpu.VMEM((blocks, rows, 2 * width), BF16),
            pltpu.VMEM((rows, 5 * width), BF16),
            pltpu.VMEM((length, 7 * width), BF16),
            pltpu.VMEM((rows, 2 * width), BF16),
            pltpu.VMEM((2, heads, LANES + PAD, LANES), BF16),
            pltpu.VMEM((blocks, heads, LANES + PAD, LANES), BF16),
            pltpu.VMEM((heads, 2, rows, LANES), F32),
            pltpu.VMEM((heads, 2, rows // BLOCK, LANES, LANES), F32),
            pltpu.VMEM((heads, 2, LANES, LANES), F32),
            pltpu.VMEM((rows, width), F32),
            pltpu.VMEM((heads, rows // tile, 2 * tile, LANES), F32),
            pltpu.VMEM((heads, rows // tile, 2 * tile, LANES), F32),
            pltpu.VMEM((heads, rows // tile, 2 * tile, LANES), F32),
            dma((blocks, groups)),
            dma((blocks, groups)),
            dma((2,)),
            dma,
            dma((blocks,)),
            dma((blocks,)),
            dma((2, groups, tp)),
            dma((2, tp, groups)),
        ],
        compiler_params=pltpu.CompilerParams(
            collective_id=0, has_side_effects=True, vmem_limit_bytes=56 * 1024 * 1024
        ),
        cost_estimate=pl.CostEstimate(flops=10**10, bytes_accessed=10**7, transcendentals=10**7),
    )(*projected, cosine, sine, leak, decay, lam, rec_gain.reshape(1, LANES), att_gain.reshape(1, LANES))

    shares = mixers.reshape(tp, groups, length // tp, 2, heads, LANES)
    both = shares.transpose(2, 3, 0, 1, 4, 5).reshape(length // tp, 2, -1)
    result = jnp.dot(both[:, 0], out_rec, preferred_element_type=F32) + jnp.dot(
        both[:, 1], out_att, preferred_element_type=F32
    )
    return result.astype(BF16)


def fused_kernel(
    ranks, tp, heads, planes,
    tokens_in, norm_in, w_key, w_value, w_query, w_rq, w_fwd, w_bwd, w_rv, leak_in, decay_in, rec_gain_in,
    lam_in, att_gain_in, out_rec_in, out_att_in, rotary_in,
    out,
    tokens, gain, weights, leak, decay, decay_rows, rec_gain, lam, att_gain, w_out, rotary,
    held, cosine, sine, lam_own, lam_pair, stage_kv, stage_q, kv, query, recp, cum_reads, facts, adds, rec_sum,
    state, fade, pair_out, pair_in, plane_out, plane_in, plane_sum, next_out, next_in, before_block,
    rec_stage, rec_all, score_a, score_b, top_a, top_b, acc, peak, att_stage, att_all, total,
    up, down, in_sem, across_send, across_recv, core_send, core_recv, lam_send, lam_recv,
    kv_send, kv_recv, q_send, q_recv, side_send, side_recv, near_send, near_recv,
    pair_send, pair_recv, plane_send, plane_recv, next_send, next_recv,
    rec_send, rec_recv, att_send, att_recv,
):
    sp = lax.axis_index("sp")
    me = lax.axis_index("tp")
    x = lax.rem(sp, 2)
    z = lax.div(sp, 2)
    core = lax.rem(me, 2)
    y = lax.div(me, 2)
    piece = tokens.shape[0]
    half = piece // 2
    length = piece * tp
    width = heads * LANES
    partner = {"tp": y * 2 + 1 - core}
    opposite = {"tp": (1 - y) * 2 + core}
    beside = {"sp": z * 2 + 1 - x}

    small = (
        (rotary_in, rotary), (lam_in, lam), (leak_in, leak), (decay_in, decay),
        (rec_gain_in, rec_gain), (att_gain_in, att_gain),
    )
    inputs = (w_key, w_value, w_query, w_rq, w_fwd, w_bwd, w_rv)
    moves = (
        [(tokens_in, tokens), (norm_in, gain)]
        + [(a, weights.at[i]) for i, a in enumerate(inputs)]
        + list(small) + [(out_rec_in, w_out.at[0]), (out_att_in, w_out.at[1])]
    )
    slots = (0, 1, 2, 3, 4, 5, 5, 5, 5, 6, 7, 8, 9, 10, 11, 12, 12)
    fetches = [pltpu.make_async_copy(a, b, in_sem.at[i]) for i, (a, b) in zip(slots, moves)]
    f_rotary, f_lam, f_leak, f_decay, f_rec_gain, f_att_gain = fetches[9:15]
    for fetch in fetches[:2] + fetches[9:11]:
        fetch.start()

    barrier = pltpu.get_barrier_semaphore()
    above = {"sp": sp + 2}
    below = {"sp": sp - 2}
    for to in (partner, opposite, {"tp": (1 - y) * 2 + 1 - core}, beside):
        pl.semaphore_signal(barrier, inc=1, device_id=to)

    @pl.when(z > 0)
    def _():
        pl.semaphore_signal(barrier, inc=1, device_id=below)

    @pl.when(z < planes - 1)
    def _():
        pl.semaphore_signal(barrier, inc=1, device_id=above)

    neighbours = 4 + lax.div(z + planes - 2, planes - 1) + lax.div(2 * planes - 3 - z, planes - 1)

    def chains():
        def pass_up():
            @pl.when(z > 0)
            def _():
                pl.semaphore_wait(up, 1)

            @pl.when(z < planes - 1)
            def _():
                pl.semaphore_signal(up, inc=1, device_id=above)

        def pass_down():
            @pl.when(z < planes - 1)
            def _():
                pl.semaphore_wait(down, 1)

            @pl.when(z > 0)
            def _():
                pl.semaphore_signal(down, inc=1, device_id=below)

        @pl.when(2 * z < planes)
        def _():
            pass_up()
            pass_down()

        @pl.when(2 * z >= planes)
        def _():
            pass_down()
            pass_up()

    def remote(source, target, send, recv, to):
        return pltpu.make_async_remote_copy(
            src_ref=source, dst_ref=target, send_sem=send, recv_sem=recv, device_id=to
        )

    def held_at(owner, part, side):
        return owner * 2 * piece + part * piece + side * half

    def held_rows(owner, part, side):
        return held.at[pl.ds(pl.multiple_of(held_at(owner, part, side), half), half)]

    def across(part, owner):
        rows = held_rows(owner, part, core)
        return remote(rows, rows, across_send, across_recv.at[part], opposite)

    def to_core(owner, part, side, slot):
        rows = held_rows(owner, part, side)
        return remote(rows, rows, core_send, core_recv.at[slot], partner)

    fetches[0].wait()
    fetches[1].wait()
    for fetch in fetches[2:9] + fetches[11:15]:
        fetch.start()
    for part in range(2):
        rows = tokens[part * half : (part + 1) * half, :].astype(F32)
        at = pl.ds(pl.multiple_of(held_at(y, part, core), half), half)
        held[at, :] = rms_scale(rows, gain[...]).astype(BF16)
        if part == 0:
            pl.semaphore_wait(barrier, neighbours)
        across(part, y).start()
        to_core(y, part, core, part).start()
    f_lam.wait()
    for i in range(heads):
        lam_own[i] = jnp.broadcast_to(lam[:, i : i + 1], (8, LANES))
    lam_copy = remote(lam_own, lam_pair, lam_send, lam_recv, partner)
    lam_copy.start()

    f_rotary.wait()
    lane = lax.broadcasted_iota(jnp.int32, (piece, LANES), 1)
    low_half = lax.rem(lane, AK) < AK // 2
    for t in range(tp):
        begin = 2 * piece + sp * tp + t
        cos_base = rotary[pl.ds(begin, 1), :]
        sin_base = rotary[pl.ds(begin + ranks * tp, 1), :]
        cos_row, sin_row = rotary[:piece, :], rotary[piece : 2 * piece, :]
        turned = sin_base * cos_row + cos_base * sin_row
        cos_here = cos_base * cos_row - sin_base * sin_row
        sin_here = jnp.where(low_half, -turned, turned)
        for part in range(2):
            to = held_at(t // 2, part, t % 2)
            cosine[to : to + half, :] = cos_here[part * half : (part + 1) * half]
            sine[to : to + half, :] = sin_here[part * half : (part + 1) * half]

    def rotated(wide, cos_at, sin_at):
        rows = wide.shape[0]
        low = jnp.concatenate([low_half] * (rows // piece), axis=0)
        turned = jnp.where(low, pltpu.roll(wide, LANES - AK // 2, 1), pltpu.roll(wide, AK // 2, 1))
        return wide * cos_at + turned * sin_at

    def owner_of(phase):
        return y if phase < 2 else 1 - y

    def plane_copy(phase, i, kind):
        return remote(
            stage_kv.at[phase, i, kind], kv.at[kind, 0, phase, z], kv_send, kv_recv.at[phase, z],
            {"sp": (core * heads + i) * 2 + x, "tp": y * 2 + kind},
        )

    def query_rows(phase, plane):
        return query.at[phase, pl.ds(pl.multiple_of(plane * half, half), half)]

    def query_copy(phase, i, c):
        return remote(
            stage_q.at[phase, i, c], query_rows(phase, z), q_send, q_recv.at[phase],
            {"sp": (core * heads + i) * 2 + x, "tp": y * 2 + c},
        )

    def is_own(i, c):
        return jnp.logical_and(core * heads + i == z, core == c)

    def project(at, index):
        return jnp.dot(held[at, :], weights[index], preferred_element_type=F32)

    def attention_inputs(phases):
        count = len(phases) * piece
        owner = owner_of(phases[0])
        at = pl.ds(pl.multiple_of(held_at(owner, phases[0] % 2, 0), piece), count)
        cos_at, sin_at = cosine[at, :], sine[at, :]
        if phases[0] == 0:
            fetches[2].wait()
        keys = project(at, 0).astype(BF16).astype(F32)
        if phases[0] == 0:
            fetches[3].wait()
        values = project(at, 1).astype(BF16).astype(F32)
        for i in range(heads):
            span = slice(i * LANES, (i + 1) * LANES)
            value = values[:, span].T.astype(BF16)
            key = rotated(keys[:, span], cos_at, sin_at).astype(BF16)
            for n, phase in enumerate(phases):
                part = slice(n * piece, (n + 1) * piece)
                stage_kv[phase, i, 0] = value[:, part]
                stage_kv[phase, i, 1] = key[part]
        if phases[0] == 0:
            chains()
        for phase in phases:
            send_each(phase, plane_copy, kv_recv.at[phase, z], lambda i, c: (stage_kv.at[phase, i, c], kv.at[c, 0, phase, z]))
        if phases[0] == 0:
            fetches[4].wait()
        queries = project(at, 2).astype(BF16).astype(F32)
        for i in range(heads):
            span = slice(i * LANES, (i + 1) * LANES)
            turned = (rotated(queries[:, span], cos_at, sin_at) * AK ** (-0.5)).astype(BF16)
            for n, phase in enumerate(phases):
                for c in range(2):
                    stage_q[phase, i, c] = turned[n * piece + c * half : n * piece + (c + 1) * half]
        for phase in phases:
            send_each(phase, query_copy, q_recv.at[phase], lambda i, c: (stage_q.at[phase, i, c], query_rows(phase, z)))

    def send_each(phase, copy, recv, local):
        for i in range(heads):
            for c in range(2):
                own = is_own(i, c)

                @pl.when(own)
                def _():
                    source, target = local(i, c)
                    pltpu.make_async_copy(source, target, recv).start()

                @pl.when(jnp.logical_not(own))
                def _():
                    copy(phase, i, c).start()

    def recurrence_inputs(owner, wait):
        at = pl.ds(pl.multiple_of(held_at(owner, 0, 0), 2 * piece), 2 * piece)
        if wait:
            pltpu.make_async_copy(weights.at[3:7], weights.at[3:7], in_sem.at[5]).wait()
        for i in range(4):
            recp[i, at, :] = project(at, 3 + i).astype(BF16)

    def plane_at(k):
        return (z, z + 1 - 2 * lax.rem(z, 2), lax.rem(z + 2, planes), planes - 1 - z)[k]

    def mine_of(origin, phase, plane):
        return kv.at[core, origin, phase, plane]

    def to_side(phase, plane):
        return remote(
            mine_of(0, phase, plane), mine_of(1, phase, plane),
            side_send, side_recv.at[phase, plane], beside,
        )

    def to_near(origin, phase, plane):
        block = mine_of(origin, phase, plane)
        return remote(
            block, block, near_send, near_recv.at[phase], partner
        )

    def relay_plane(phase, k):
        plane = plane_at(k)
        block = mine_of(0, phase, plane)
        remote(block, block, near_send, kv_recv.at[phase, plane], partner).wait_recv()
        to_side(phase, plane).start()
        to_near(0, phase, plane).start()

    def relay_side(phase, k):
        plane = plane_at(k)
        block = mine_of(1, phase, plane)
        remote(block, block, side_send, side_recv.at[phase, plane], beside).wait_recv()
        to_near(1, phase, plane).start()

    def settle(phase):
        blocks_in = kv.at[1 - core, :, phase]
        remote(blocks_in, blocks_in, near_send, near_recv.at[phase], partner).wait_recv()

    def settle_queries(phase):
        rows = query.at[phase]
        remote(rows, rows, q_send, q_recv.at[phase], partner).wait_recv()

    row_at = lax.broadcasted_iota(jnp.int32, (BLOCK, 3 * BLOCK), 0)
    col_at = lax.rem(lax.broadcasted_iota(jnp.int32, (BLOCK, 3 * BLOCK), 1), BLOCK)
    triangles = (jnp.where(row_at >= col_at, 1.0, 0.0).astype(BF16), jnp.where(row_at <= col_at, 1.0, 0.0).astype(BF16))
    row_in = lax.broadcasted_iota(jnp.int32, (BLOCK, BLOCK), 0)
    col_in = lax.broadcasted_iota(jnp.int32, (BLOCK, BLOCK), 1)
    earlier = (row_in >= col_in, row_in <= col_in)
    ends = (BLOCK - 1, 0)
    middles = (BLOCK // 2 - 1, BLOCK // 2)
    blocks = length // BLOCK
    spans = [slice(h * LANES, (h + 1) * LANES) for h in range(heads)]

    def within_block(b):
        at = pl.ds(pl.multiple_of(b * BLOCK, BLOCK), BLOCK)
        t = lax.div(b, 2)
        stored = held_at(lax.div(t, 2), lax.rem(b, 2), lax.rem(t, 2))
        held_block = pl.ds(pl.multiple_of(stored, BLOCK), BLOCK)
        queries = jax.nn.silu(recp[0, held_block, :].astype(F32))
        values = recp[3, held_block, :]
        scores, tails = [], []
        for d in range(2):
            keys = leak[d : d + 1, :] * jax.nn.sigmoid(-recp[1 + d, held_block, :].astype(F32))
            added = jnp.concatenate(
                [jnp.broadcast_to(decay_rows[at, d * heads + h : d * heads + h + 1], (BLOCK, LANES)) for h in range(heads)],
                axis=1,
            )
            logs = jnp.log1p(-keys) + added
            coarse = logs.astype(BF16)
            rest = logs - coarse.astype(F32)
            fine = rest.astype(BF16)
            finest = (rest - fine.astype(F32)).astype(BF16)
            cum = jnp.dot(
                triangles[d], jnp.concatenate([coarse, fine, finest], axis=0), preferred_element_type=F32
            )
            middle = cum[middles[d] : middles[d] + 1, :]
            last = cum[ends[d] : ends[d] + 1, :]
            reads = (queries * jnp.exp(cum - middle)).astype(BF16)
            writes = (keys * jnp.exp(middle - cum)).astype(BF16)
            tails.append((keys * jnp.exp(last - cum)).astype(BF16))
            carried = (queries * jnp.exp(cum)).astype(BF16)
            facts[b, d] = jnp.broadcast_to(jnp.exp(last), (8, width))
            scores.append([jnp.where(earlier[d], dot_t(reads[:, s], writes[:, s]), 0.0) for s in spans])
            for h in range(heads):
                cum_reads[h, at, d * LANES : (d + 1) * LANES] = carried[:, spans[h]]
        for h in range(heads):
            both = (scores[0][h] + scores[1][h]).astype(BF16)
            rec_sum[at, spans[h]] = jnp.dot(both, values[:, spans[h]], preferred_element_type=F32)
            adds[b, h] = dot_0(
                values[:, spans[h]], jnp.concatenate([tails[0][:, spans[h]], tails[1][:, spans[h]]], axis=1)
            )

    def within_rows(owner):
        count = blocks // 2

        def some(j, carry):
            within_block(owner * count + 2 * j)
            within_block(owner * count + 2 * j + 1)
            return carry

        lax.fori_loop(0, count // 2, some, 0)

    def order(d):
        return range(blocks) if d == 0 else range(blocks - 1, -1, -1)

    def half_of(d):
        return slice(d * LANES, (d + 1) * LANES)

    first_row = lax.broadcasted_iota(jnp.int32, (PAD, LANES), 0) == 0

    def pack(target, moved, factor):
        target[:LANES, :] = moved.astype(BF16)
        wide = jnp.broadcast_to(factor, (PAD, LANES))
        coarse = wide.astype(BF16).astype(F32)
        target[LANES:, :] = jnp.where(first_row, coarse, wide - coarse).astype(BF16)

    def unpack(source):
        last = source[LANES:, :].astype(F32)
        return source[:LANES, :].astype(F32), last[0:1] + last[1:2]

    def local_states():
        for h in range(heads):
            for d in range(2):
                moved = jnp.zeros((LANES, LANES), F32)
                factor = jnp.ones((1, LANES), F32)
                for b in order(d):
                    step = facts[b, d, 0:1, spans[h]]
                    moved = moved * step + adds[b, h, :, half_of(d)]
                    factor = factor * step
                state[d, h] = moved
                fade[d, h] = jnp.broadcast_to(factor, (8, LANES))
                pack(pair_out.at[d, h], moved, factor)

    pair_copy = remote(pair_out, pair_in, pair_send, pair_recv, beside)

    def pair_states():
        pair_copy.wait_recv()
        for d in range(2):
            mine, factor = state[d, x], fade[d, x][0:1]
            other, other_factor = unpack(pair_in.at[d, x])
            joined = jnp.where(x == d, mine * other_factor + other, other * factor + mine)
            pack(plane_out.at[d], joined, factor * other_factor)
        for dz in range(1, planes):
            to_plane(lax.rem(z + dz, planes)).start()

    def to_plane(target):
        return remote(
            plane_out.at[jnp.where(target > z, 0, 1)], plane_in.at[z],
            plane_send, plane_recv, {"sp": target * 2 + x},
        )

    def other_planes():
        blocks_in = plane_in.at[: planes - 1]
        return remote(blocks_in, blocks_in, plane_send, plane_recv, partner)

    next_copy = remote(next_out, next_in, next_send, next_recv, beside)

    def plane_states():
        other_planes().wait_recv()
        plane_sum[...] = jnp.zeros_like(plane_sum)

        def fold(d):
            def one(step, carry):
                plane = step if d == 0 else planes - 1 - step
                moved, factor = unpack(plane_in.at[plane])
                plane_sum[d] = plane_sum[d] * factor + moved
                return carry

            return one

        lax.fori_loop(0, z, fold(0), 0)
        lax.fori_loop(0, planes - 1 - z, fold(1), 0)
        next_out[...] = plane_sum[...].astype(BF16)
        next_copy.start()

    def second_pass():
        next_copy.wait_recv()
        for h in range(heads):
            for d in range(2):
                entering = jnp.where(x == h, plane_sum[d], next_in[d].astype(F32))
                other, other_factor = unpack(pair_in.at[d, h])
                running = jnp.where(x == d, entering, entering * other_factor + other)
                for b in order(d):
                    before_block[b, h, :, half_of(d)] = running.astype(BF16)
                    running = running * facts[b, d, 0:1, spans[h]] + adds[b, h, :, half_of(d)]
            for b in range(blocks):
                at = slice(b * BLOCK, (b + 1) * BLOCK)
                whole = rec_sum[at, spans[h]] + dot_t(cum_reads[h, at, :], before_block[b, h])
                rec_stage[at, spans[h]] = rms_scale(whole, rec_gain[...]).astype(BF16)
        for dt in range(tp):
            rec_copy(dt).start()

    def rec_copy(dt):
        t = lax.rem(me + dt, tp)
        source = rec_stage.at[pl.ds(pl.multiple_of(t * piece, piece), piece)]
        if dt == 0:
            return pltpu.make_async_copy(source, rec_all.at[me], rec_recv)
        return remote(source, rec_all.at[me], rec_send, rec_recv, {"tp": t})

    acc[...] = jnp.zeros_like(acc)
    peak[...] = jnp.full_like(peak, -jnp.inf)
    sub = 2 * piece
    ones = jnp.ones((PAD, sub), BF16)
    low_map = lane < AK
    chunk_blocks = 2 * planes
    buffers = ((score_a, top_a), (score_b, top_b))

    def attend_step(made, made_buffer, used, used_buffer):
        if made is not None:
            q_phase, tile, made_phase = made
            rows = query[q_phase, tile * piece : (tile + 1) * piece, :]
            none = jnp.zeros_like(rows)
            both = jnp.concatenate([jnp.where(low_map, rows, none), jnp.where(low_map, none, rows)], axis=0)
            top = None
        if used is not None:
            slot, used_phase = used[0] * 2 + used[1], used[2]
            used_score, used_top = used_buffer
            before = peak[slot][0:1]
            now = jnp.maximum(before, jnp.max(used_top[...], axis=0, keepdims=True))
            mixed = acc[slot] * jnp.exp(before - now)
        for u in range(0, chunk_blocks, 2):
            at = slice(u * piece, (u + 2) * piece)
            where = [((u + n) // planes, (u + n) % planes) for n in range(2)]
            if made is not None:
                keys = jnp.concatenate([kv[1, o, made_phase, p] for o, p in where], axis=0)
                scores = dot_t(keys, both)
                made_buffer[0][at, :] = scores
                high = jnp.max(scores.reshape(sub // 8, 8, 2 * piece), axis=0)
                top = high if top is None else jnp.maximum(top, high)
            if used is not None:
                expo = jnp.exp(used_score[at, :] - now).astype(BF16)
                values = jnp.concatenate([kv[0, o, used_phase, p] for o, p in where], axis=1)
                values = jnp.concatenate([values, ones], axis=0)
                mixed = mixed + jnp.dot(values, expo, preferred_element_type=F32)
        if used is not None:
            acc[slot] = mixed
            peak[slot] = jnp.broadcast_to(now, (8, 2 * piece))
        if made is not None:
            made_buffer[1][...] = top

    def att_copy(q_phase, plane):
        owner, part = owner_of(q_phase), q_phase % 2
        return remote(
            att_stage.at[q_phase * planes + plane], att_all.at[y * planes + z, part * half : (part + 1) * half],
            att_send, att_recv,
            {"sp": plane * 2 + x, "tp": owner * 2 + core},
        )

    def finish(q_phase, tile):
        whole = acc[q_phase * 2 + tile]
        ratio = whole[:LANES] / whole[LANES : LANES + 1]
        weight = jnp.where(core == lax.div(z, heads), lam_own[lax.rem(z, heads)], lam_pair[lax.rem(z, heads)])[0:1]
        values = ratio[:, :piece] - weight * ratio[:, piece:]
        scale = lax.rsqrt(jnp.mean(values * values, axis=0, keepdims=True) + EPS)
        rows = ((values * scale).T * att_gain[...]).astype(BF16)
        part = q_phase % 2
        for n in range(2):
            plane = 2 * tile + n
            att_stage[q_phase * planes + plane] = rows[n * half : (n + 1) * half]
            if q_phase < 2:

                @pl.when(plane == z)
                def _():
                    pltpu.make_async_copy(
                        att_stage.at[q_phase * planes + plane],
                        att_all.at[y * planes + z, part * half : (part + 1) * half],
                        att_recv,
                    ).start()

                @pl.when(plane != z)
                def _():
                    att_copy(q_phase, plane).start()
            else:
                att_copy(q_phase, plane).start()

    columns = min(512, out.shape[1])

    def rec_total():
        pltpu.make_async_copy(w_out, w_out, in_sem.at[12]).wait()
        remote(rec_all, rec_all, rec_send, rec_recv, partner).wait_recv()
        rec_rows = jnp.concatenate([rec_all[t] for t in range(tp)], axis=1)
        for n in range(0, out.shape[1], columns):
            total[:, n : n + columns] = jnp.dot(rec_rows, w_out[0, :, n : n + columns], preferred_element_type=F32)

    def run_units(units, before):
        for n in range(len(units) + 1):
            for action in before.get(n, ()):
                action()
            made = units[n] if n < len(units) else None
            used = units[n - 1] if n else None
            attend_step(made, buffers[n % 2], used, buffers[(n + 1) % 2])
            if used is not None and used[2] == 3:
                finish(used[0], used[1])

    def both_tiles(q_phase, key_phase):
        return [(q_phase, tile, key_phase) for tile in range(2)]

    def plan():
        units, before = [], {}

        def at_next(*actions):
            before.setdefault(len(units), []).extend(actions)

        def call(f, *args):
            return functools.partial(f, *args)

        units += both_tiles(0, 1)
        at_next(pair_states, *(call(relay_side, 2, k) for k in range(2)))
        units += both_tiles(1, 0)
        at_next(*(call(relay_side, 2, k) for k in range(2, 4)))
        units += both_tiles(1, 1)
        at_next(call(settle_queries, 2), plane_states, *(call(relay_plane, 3, k) for k in range(3)))
        units += both_tiles(2, 0)
        at_next(call(relay_plane, 3, 3), call(settle, 2))
        units += both_tiles(2, 1)
        at_next(call(relay_side, 3, 0), call(relay_side, 3, 1))
        units += both_tiles(0, 2)
        at_next(call(relay_side, 3, 2), call(relay_side, 3, 3))
        units += both_tiles(1, 2)
        at_next(second_pass)
        units += both_tiles(2, 2)
        at_next(call(settle_queries, 3))
        units += both_tiles(3, 0) + both_tiles(3, 1) + both_tiles(3, 2)
        at_next(call(settle, 3))
        units += both_tiles(0, 3)
        at_next(rec_total)
        units += both_tiles(1, 3) + both_tiles(2, 3) + both_tiles(3, 3)
        return units, before

    for part in range(2):
        to_core(y, part, 1 - core, part).wait_recv()
    attention_inputs((0, 1))
    for fetch in fetches[15:17]:
        fetch.start()
    recurrence_inputs(y, True)
    for fetch in (f_leak, f_decay, f_rec_gain, f_att_gain):
        fetch.wait()
    by_row = jnp.concatenate([decay[d] for d in range(2)] + [jnp.zeros((LANES - 2 * heads, length), F32)], axis=0)
    decay_rows[...] = by_row.T
    relay_plane(0, 0)
    within_rows(y)
    relay_plane(0, 1)
    across(0, 1 - y).wait_recv()
    to_core(1 - y, 0, core, 2).start()
    relay_plane(0, 2)
    relay_plane(0, 3)
    to_core(1 - y, 0, 1 - core, 2).wait_recv()
    attention_inputs((2,))
    for k in range(4):
        relay_side(0, k)
    relay_plane(1, 0)
    relay_plane(1, 1)
    lam_copy.wait_recv()
    settle(0)
    settle_queries(0)
    run_units(both_tiles(0, 0), {})
    across(1, 1 - y).wait_recv()
    to_core(1 - y, 1, core, 3).start()
    relay_plane(1, 2)
    relay_plane(1, 3)
    to_core(1 - y, 1, 1 - core, 3).wait_recv()
    attention_inputs((3,))
    for k in range(4):
        relay_side(1, k)
    recurrence_inputs(1 - y, False)
    relay_plane(2, 0)
    within_rows(1 - y)
    local_states()
    pair_copy.start()
    for k in range(1, 4):
        relay_plane(2, k)
    settle(1)
    settle_queries(1)
    run_units(*plan())

    remote(att_all, att_all, att_send, att_recv, partner).wait_recv()
    att_rows = jnp.concatenate([att_all[i] for i in range(2 * planes)], axis=1)
    for n in range(0, out.shape[1], columns):
        out[:, n : n + columns] = (
            total[:, n : n + columns]
            + jnp.dot(att_rows, w_out[1, :, n : n + columns], preferred_element_type=F32)
        ).astype(BF16)

    def sent(ref, sem, recv):
        remote(ref, ref, sem, recv, partner).wait_send()

    sent(held.at[:piece], across_send, core_recv.at[0])
    sent(held.at[: 2 * piece], core_send, core_recv.at[0])
    lam_copy.wait_send()
    is_local = core == lax.div(z, heads)

    @pl.when(is_local)
    def _():
        sent(stage_kv.at[:3], kv_send, near_recv.at[0])
        sent(stage_q.at[:3], q_send, near_recv.at[0])

    @pl.when(jnp.logical_not(is_local))
    def _():
        sent(stage_kv, kv_send, near_recv.at[0])
        sent(stage_q, q_send, near_recv.at[0])

    sent(kv.at[0, 0], side_send, near_recv.at[0])
    sent(kv.at[0], near_send, near_recv.at[0])
    pair_copy.wait_send()
    next_copy.wait_send()
    sent(plane_in.at[: planes - 1], plane_send, plane_recv)
    sent(rec_all.at[: tp - 1], rec_send, rec_recv)
    sent(att_stage.at[: 4 * planes - 2], att_send, att_recv)


def rotary_table(piece, pieces):
    frequency = THETA ** (-(np.arange(LANES) % (AK // 2)) * 2.0 / AK)
    inside = np.arange(piece)[:, None] * frequency[None, :]
    base = (np.arange(pieces) * piece)[:, None] * frequency[None, :]
    return np.concatenate([np.cos(inside), np.sin(inside), np.cos(base), np.sin(base)]).astype(np.float32)


def on_device(
    tokens, norm_gain, rec_query, fwd_gate, bwd_gate, rec_value, gate_leak, log_decay, rec_gain,
    att_query, att_key, att_value, lambdas, att_gain, out_rec, out_att,
):
    ranks = lax.axis_size("sp")
    tp = lax.axis_size("tp")
    heads = rec_query.shape[1] // HK
    planes = ranks // 2
    piece, model = tokens.shape
    if tp != 4 or planes != 2 * heads or planes != 4 or piece != LANES:
        return on_device_general(
            tokens, norm_gain, rec_query, fwd_gate, bwd_gate, rec_value, gate_leak, log_decay, rec_gain,
            att_query, att_key, att_value, lambdas, att_gain, out_rec, out_att,
        )
    length = piece * tp
    width = heads * LANES
    blocks = length // BLOCK
    keys = 2 * planes * piece
    anywhere = pl.BlockSpec(memory_space=pl.ANY)
    dma = pltpu.SemaphoreType.DMA
    vmem = pltpu.VMEM
    table = jnp.asarray(rotary_table(piece, ranks * tp))
    return pl.pallas_call(
        functools.partial(fused_kernel, ranks, tp, heads, planes),
        out_shape=jax.ShapeDtypeStruct((piece, model), BF16),
        in_specs=[anywhere] * 17,
        out_specs=pl.BlockSpec(memory_space=pltpu.VMEM),
        scratch_shapes=[
            vmem((piece, model), BF16),
            vmem((1, model), F32),
            vmem((7, model, width), BF16),
            vmem((2, width), F32),
            vmem((2, heads, length), F32),
            vmem((length, LANES), F32),
            vmem((1, LANES), F32),
            vmem((1, heads), F32),
            vmem((1, LANES), F32),
            vmem((2, *out_rec.shape), BF16),
            vmem(table.shape, F32),
            vmem((length, model), BF16),
            vmem((length, LANES), F32),
            vmem((length, LANES), F32),
            vmem((heads, 8, LANES), F32),
            vmem((heads, 8, LANES), F32),
            vmem((4, heads, 2, piece, LANES), BF16),
            vmem((4, heads, 2, piece // 2, LANES), BF16),
            vmem((2, 2, 4, planes, piece, LANES), BF16),
            vmem((4, planes * piece // 2, LANES), BF16),
            vmem((4, length, width), BF16),
            vmem((heads, length, 2 * LANES), BF16),
            vmem((blocks, 2, 8, width), F32),
            vmem((blocks, heads, LANES, 2 * LANES), F32),
            vmem((length, width), F32),
            vmem((2, heads, LANES, LANES), F32),
            vmem((2, heads, 8, LANES), F32),
            vmem((2, heads, LANES + PAD, LANES), BF16),
            vmem((2, heads, LANES + PAD, LANES), BF16),
            vmem((2, LANES + PAD, LANES), BF16),
            vmem((planes, LANES + PAD, LANES), BF16),
            vmem((2, LANES, LANES), F32),
            vmem((2, LANES, LANES), BF16),
            vmem((2, LANES, LANES), BF16),
            vmem((blocks, heads, LANES, 2 * LANES), BF16),
            vmem((length, width), BF16),
            vmem((tp, piece, width), BF16),
            vmem((keys, 2 * piece), F32),
            vmem((keys, 2 * piece), F32),
            vmem((8, 2 * piece), F32),
            vmem((8, 2 * piece), F32),
            vmem((2 * planes, LANES + PAD, 2 * piece), F32),
            vmem((2 * planes, 8, 2 * piece), F32),
            vmem((4 * planes, piece // 2, LANES), BF16),
            vmem((2 * planes, piece, LANES), BF16),
            vmem((piece, model), F32),
            pltpu.SemaphoreType.REGULAR, pltpu.SemaphoreType.REGULAR,
            dma((13,)), dma, dma((2,)), dma, dma((4,)), dma, dma,
            dma, dma((4, planes)), dma, dma((4,)),
            dma, dma((4, planes)), dma, dma((4,)),
            dma, dma, dma, dma, dma, dma,
            dma, dma, dma, dma,
        ],
        compiler_params=pltpu.CompilerParams(
            collective_id=2, has_side_effects=True, vmem_limit_bytes=60 * 1024 * 1024
        ),
        cost_estimate=pl.CostEstimate(flops=10**10, bytes_accessed=10**7, transcendentals=10**7),
    )(
        tokens, norm_gain.reshape(1, -1), att_key, att_value, att_query, rec_query, fwd_gate, bwd_gate, rec_value,
        gate_leak, log_decay.transpose(0, 2, 1), rec_gain.reshape(1, LANES), lambdas.reshape(1, heads), att_gain.reshape(1, LANES),
        out_rec, out_att, table,
    )


def solution(mesh):
    placed = (
        P(("sp", "tp"), None), P(), P(None, "tp"), P(None, "tp"), P(None, "tp"), P(None, "tp"),
        P(None, "tp"), P(None, "sp", "tp"), P(), P(None, "tp"), P(None, "tp"), P(None, "tp"),
        P("tp"), P(), P(), P(),
    )
    return jax.shard_map(
        on_device, mesh=mesh, in_specs=placed, out_specs=P(("sp", "tp"), None), check_vma=False
    )
```

```python
import functools

import jax
import jax.numpy as jnp
import numpy as np
from jax import lax
from jax.experimental import pallas as pl
from jax.experimental.pallas import tpu as pltpu
from jax.sharding import PartitionSpec as P

HK = 128
AK = 64
BLOCK = 64
LANES = 128
EPS = 1e-06
THETA = 500000.0
HIGHEST = lax.Precision.HIGHEST
F32 = jnp.float32
BF16 = jnp.bfloat16
PAD = 16


def rms_scale(values, gain):
    return values * lax.rsqrt(jnp.mean(values * values, axis=-1, keepdims=True) + EPS) * gain


def dot_t(a, b):
    return lax.dot_general(a, b, (((1,), (1,)), ((), ())), preferred_element_type=F32)


def dot_0(a, b):
    return lax.dot_general(a, b, (((0,), (0,)), ((), ())), preferred_element_type=F32)


def gather_kernel(tp, tokens, gain, *refs):
    weights, outs = refs[:7], refs[7:14]
    held, across, along, landed = refs[14:]
    me = lax.axis_index("tp")
    core = lax.rem(me, 2)
    pair = lax.div(me, 2)
    pairs = tp // 2
    count = tokens.shape[0]
    partner = pair * 2 + 1 - core
    others = [lax.rem(pair + k, pairs) for k in range(1, pairs)]
    barrier = pltpu.get_barrier_semaphore()
    pl.semaphore_signal(barrier, inc=1, device_id={"tp": partner})
    for q in others:
        pl.semaphore_signal(barrier, inc=1, device_id={"tp": q * 2 + core})

    def rows_at(block):
        return held.at[pl.ds(pl.multiple_of(block * count, count), count)]

    def to_partner(block):
        return pltpu.make_async_remote_copy(
            src_ref=rows_at(block),
            dst_ref=rows_at(block),
            send_sem=across.at[block],
            recv_sem=landed.at[block],
            device_id={"tp": partner},
        )

    def to_pair(q):
        return pltpu.make_async_remote_copy(
            src_ref=rows_at(me),
            dst_ref=rows_at(me),
            send_sem=along.at[q],
            recv_sem=landed.at[me],
            device_id={"tp": q * 2 + core},
        )

    normed = rms_scale(tokens[...].astype(F32), gain[...]).astype(BF16)
    held[pl.ds(pl.multiple_of(me * count, count), count), :] = normed
    pl.semaphore_wait(barrier, pairs)
    for q in others:
        to_pair(q).start()
    to_partner(me).start()

    def step(k, carry):
        q = lax.rem(pair + k, pairs)
        near = q * 2 + core

        @pl.when(k > 0)
        def _():
            to_partner(near).wait_recv()
            to_partner(near).start()

        to_partner(q * 2 + 1 - core).wait_recv()
        at = pl.ds(pl.multiple_of(q * 2 * count, 2 * count), 2 * count)
        for weight, result in zip(weights, outs):
            result[at, :] = jnp.dot(held[at, :], weight[...], preferred_element_type=F32).astype(BF16)
        return carry

    lax.fori_loop(0, pairs, step, 0)
    to_partner(me).wait_send()
    for q in others:
        to_pair(q).wait_send()
        to_partner(q * 2 + core).wait_send()


def mixer_kernel(
    ranks, tp, groups, heads, tile,
    proj_k, proj_v, proj_q, proj_rq, proj_fwd, proj_bwd, proj_rv, cosine, sine, leak, decay, lam, rec_gain, att_gain,
    out,
    kv, rest, swap, stage, state_out, state_in, cums, adds, states, rec_sum, peak, total, mixed,
    kv_send, kv_recv, swap_send, rest_recv, state_send, state_recv, out_send, out_recv,
):
    me = lax.axis_index("sp")
    slot = lax.rem(me, groups)
    mine = lax.div(me, groups)
    mesh_column = lax.axis_index("tp")
    length = proj_k.shape[0]
    piece = length // tp
    rows = groups * length
    width = heads * LANES
    block_count = rows // BLOCK
    partner_slot = groups - 1 - slot
    partner = mine * groups + partner_slot
    blocks = ranks // groups
    own_rows = pl.ds(pl.multiple_of(slot * length, length), length)
    other_rows = pl.ds(pl.multiple_of(partner_slot * length, length), length)

    barrier = pltpu.get_barrier_semaphore()
    peers = []
    for k in range(1, blocks):
        peers.append(lax.rem(mine + k, blocks))
    for peer in peers:
        pl.semaphore_signal(barrier, inc=1, device_id={"sp": peer * groups + slot})
    owners = []
    for dp in range(groups):
        for dt in range(tp):
            owners.append((dp, dt, lax.rem(slot + dp, groups), lax.rem(mesh_column + dt, tp)))
    for dp, dt, p, t in owners[1:]:
        pl.semaphore_signal(barrier, inc=1, device_id={"sp": mine * groups + p, "tp": t})

    lane = lax.broadcasted_iota(jnp.int32, (length, LANES), 1)
    low_half = lax.rem(lane, AK) < AK // 2

    def rotated(raw):
        wide = raw.astype(F32)
        turned = jnp.where(low_half, -pltpu.roll(wide, LANES - AK // 2, 1), pltpu.roll(wide, AK // 2, 1))
        return wide * cosine[...] + turned * sine[...]

    def prepare(head_group, key_value, others):
        def taken(ref, h):
            return ref[:, pl.ds(pl.multiple_of((head_group * heads + h) * LANES, LANES), LANES)]

        for h in range(heads):
            at = h * LANES
            key_value[:, at : at + LANES] = rotated(taken(proj_k, h)).astype(BF16)
            key_value[:, width + at : width + at + LANES] = taken(proj_v, h)
            others[:, at : at + LANES] = (rotated(taken(proj_q, h)) * AK ** (-0.5)).astype(BF16)
            for i, ref in enumerate((proj_rq, proj_fwd, proj_bwd, proj_rv)):
                others[:, (i + 1) * width + at : (i + 1) * width + at + LANES] = taken(ref, h)

    if groups > 1:
        prepare(partner_slot, swap.at[:, : 2 * width], swap.at[:, 2 * width :])
    prepare(slot, kv.at[mine, own_rows], rest.at[own_rows])
    pl.semaphore_wait(barrier, blocks - 1 + groups * tp - 1)

    def block_copy(source_rows, source_slot, peer):
        return pltpu.make_async_remote_copy(
            src_ref=kv.at[mine, source_rows],
            dst_ref=kv.at[mine, source_rows],
            send_sem=kv_send.at[peer, source_slot],
            recv_sem=kv_recv.at[mine, source_slot],
            device_id={"sp": peer * groups + slot},
        )

    def arrival(block, piece):
        piece_rows = pl.ds(pl.multiple_of(piece * length, length), length)
        return pltpu.make_async_remote_copy(
            src_ref=kv.at[block, piece_rows],
            dst_ref=kv.at[block, piece_rows],
            send_sem=kv_send.at[block, piece],
            recv_sem=kv_recv.at[block, piece],
            device_id={"sp": block * groups + slot},
        )

    if groups > 1:
        swap_kv = pltpu.make_async_remote_copy(
            src_ref=swap.at[:, : 2 * width],
            dst_ref=kv.at[mine, own_rows],
            send_sem=swap_send.at[0],
            recv_sem=kv_recv.at[mine, slot],
            device_id={"sp": partner},
        )
        swap_kv.start()
        swap_rest = pltpu.make_async_remote_copy(
            src_ref=swap.at[:, 2 * width :],
            dst_ref=rest.at[own_rows],
            send_sem=swap_send.at[1],
            recv_sem=rest_recv,
            device_id={"sp": partner},
        )
    own_copies = [block_copy(own_rows, slot, peer) for peer in peers]
    for copy in own_copies:
        copy.start()
    other_copies = []
    if groups > 1:
        swap_rest.start()
        arrival(mine, partner_slot).wait_recv()
        other_copies = [block_copy(other_rows, partner_slot, peer) for peer in peers]
        for copy in other_copies:
            copy.start()
        swap_rest.wait_recv()

    row_at = lax.broadcasted_iota(jnp.int32, (BLOCK, BLOCK), 0)
    col_at = lax.broadcasted_iota(jnp.int32, (BLOCK, BLOCK), 1)
    earlier = (row_at >= col_at, row_at <= col_at)
    triangles = tuple(mask.astype(F32) for mask in earlier)
    ends = (BLOCK - 1, 0)
    middles = (BLOCK // 2 - 1, BLOCK // 2)

    def rows_of(direction, step):
        index = step if direction == 0 else block_count - 1 - step
        return index, pl.ds(pl.multiple_of(index * BLOCK, BLOCK), BLOCK)

    def part(at, index, h):
        return rest[at, (index * heads + h) * LANES : (index * heads + h + 1) * LANES].astype(F32)

    def keys_of(at, direction, h):
        return leak[h, direction : direction + 1, :] * jax.nn.sigmoid(-part(at, 2 + direction, h))

    states[...] = jnp.zeros_like(states)
    rec_sum[...] = jnp.zeros_like(rec_sum)

    def first_pass(step, totals):
        after = []
        for h in range(heads):
            for d in range(2):
                index, at = rows_of(d, step)
                keys = keys_of(at, d, h)
                column = d * heads + h
                logs = jnp.log1p(-keys) + decay[at, column : column + 1]
                cum = jnp.dot(triangles[d], logs, precision=HIGHEST, preferred_element_type=F32)
                cums[h, d, at, :] = cum
                last = cum[ends[d] : ends[d] + 1, :]
                scaled = (keys * jnp.exp(last - cum)).astype(BF16)
                added = dot_0(part(at, 4, h).astype(BF16), scaled)
                adds[h, d, index] = added
                states[h, d] = states[h, d] * jnp.exp(last) + added
                after.append(totals[h * 2 + d] + last)
        return tuple(after)

    nothing = tuple(jnp.zeros((1, LANES), F32) for _ in range(2 * heads))
    sums = lax.fori_loop(0, block_count, first_pass, nothing, unroll=2)
    for h in range(heads):
        for d in range(2):
            state_out[d, h, :LANES, :] = states[h, d].astype(BF16)
            factor = jnp.broadcast_to(jnp.exp(sums[h * 2 + d]), (PAD, LANES))
            coarse = factor.astype(BF16)
            fine = (factor - coarse.astype(F32)).astype(BF16)
            first_row = lax.broadcasted_iota(jnp.int32, (PAD, LANES), 0) == 0
            state_out[d, h, LANES:, :] = jnp.where(first_row, coarse.astype(F32), fine.astype(F32)).astype(BF16)
    state_copies = []
    for peer in peers:
        copy = pltpu.make_async_remote_copy(
            src_ref=state_out.at[jnp.where(peer > mine, 0, 1)],
            dst_ref=state_in.at[mine],
            send_sem=state_send.at[peer],
            recv_sem=state_recv.at[mine],
            device_id={"sp": peer * groups + slot},
        )
        copy.start()
        state_copies.append(copy)

    lane_q = lax.broadcasted_iota(jnp.int32, (tile, LANES), 1)
    tiles = rows // tile
    peak[...] = jnp.full_like(peak, -jnp.inf)
    total[...] = jnp.zeros_like(total)
    mixed[...] = jnp.zeros_like(mixed)

    def attend(block):
        for h in range(heads):
            at = h * LANES

            def one_tile(index, carry):
                q_rows = pl.ds(pl.multiple_of(index * tile, tile), tile)
                queries = rest[q_rows, at : at + LANES]
                zero = jnp.zeros_like(queries)
                both = jnp.concatenate(
                    [jnp.where(lane_q < AK, queries, zero), jnp.where(lane_q < AK, zero, queries)], axis=0
                )
                scores = dot_t(both, kv[block, :, at : at + LANES])
                before = peak[h, index][:, :1]
                raised = jnp.maximum(before, jnp.max(scores, axis=-1, keepdims=True))
                shrink = jnp.exp(before - raised)
                expo = jnp.exp(scores - raised)
                sums_now = total[h, index][:, :1] * shrink + jnp.sum(expo, axis=-1, keepdims=True)
                product = jnp.dot(
                    expo.astype(BF16), kv[block, :, width + at : width + at + LANES], preferred_element_type=F32
                )
                mixed[h, index] = mixed[h, index] * shrink + product
                peak[h, index] = jnp.broadcast_to(raised, (2 * tile, LANES))
                total[h, index] = jnp.broadcast_to(sums_now, (2 * tile, LANES))
                return carry

            lax.fori_loop(0, tiles, one_tile, 0)

    attend(mine)

    def state_arrival(block):
        return pltpu.make_async_remote_copy(
            src_ref=state_out.at[0],
            dst_ref=state_in.at[block],
            send_sem=state_send.at[block],
            recv_sem=state_recv.at[block],
            device_id={"sp": block * groups + slot},
        )

    states[...] = jnp.zeros_like(states)

    def compose(d):
        def body(step, carry):
            block = step if d == 0 else blocks - 1 - step
            state_arrival(block).wait_recv()
            for h in range(heads):
                rows_last = state_in[block, h, LANES:, :].astype(F32)
                factor = rows_last[0:1] + rows_last[1:2]
                states[h, d] = states[h, d] * factor + state_in[block, h, :LANES, :].astype(F32)
            return carry

        return body

    lax.fori_loop(0, mine, compose(0), 0)
    lax.fori_loop(0, blocks - 1 - mine, compose(1), 0)

    def second_pass(step, carry):
        for h in range(heads):
            for d in range(2):
                index, at = rows_of(d, step)
                queries = jax.nn.silu(part(at, 1, h))
                keys = keys_of(at, d, h)
                cum = cums[h, d, at, :]
                middle = cum[middles[d] : middles[d] + 1, :]
                last = cum[ends[d] : ends[d] + 1, :]
                scores = dot_t(
                    (queries * jnp.exp(cum - middle)).astype(BF16), (keys * jnp.exp(middle - cum)).astype(BF16)
                )
                scores = jnp.where(earlier[d], scores, 0.0)
                within = jnp.dot(scores.astype(BF16), part(at, 4, h).astype(BF16), preferred_element_type=F32)
                before = states[h, d]
                carried = dot_t_state(queries * jnp.exp(cum), before)
                span = slice(h * LANES, (h + 1) * LANES)
                rec_sum[at, span] = rec_sum[at, span] + within + carried
                states[h, d] = before * jnp.exp(last) + adds[h, d, index]
        return carry

    def dot_t_state(reads, state):
        return dot_t(reads.astype(BF16), state.astype(BF16))

    lax.fori_loop(0, block_count, second_pass, 0, unroll=2)

    for h in range(heads):
        span = slice(h * LANES, (h + 1) * LANES)
        stage[:, span] = rms_scale(rec_sum[:, span], rec_gain[...]).astype(BF16)

    def hand_over(which, owner):
        dp, dt, p, t = owner
        columns = slice(which * width, (which + 1) * width)
        source = stage.at[pl.ds(pl.multiple_of(p * length + t * piece, piece), piece), columns]
        target = out.at[mesh_column, slot, :, columns]
        if dp == 0 and dt == 0:
            return pltpu.make_async_copy(source, target, out_send.at[which, dp, dt])
        return pltpu.make_async_remote_copy(
            src_ref=source,
            dst_ref=target,
            send_sem=out_send.at[which, dp, dt],
            recv_sem=out_recv.at[which, mesh_column, slot],
            device_id={"sp": mine * groups + p, "tp": t},
        )

    def taken_over(which, owner):
        dp, dt, p, t = owner
        columns = slice(which * width, (which + 1) * width)
        target = out.at[t, p, :, columns]
        return pltpu.make_async_remote_copy(
            src_ref=target,
            dst_ref=target,
            send_sem=out_send.at[which, dp, dt],
            recv_sem=out_recv.at[which, t, p],
            device_id={"sp": mine * groups + p, "tp": t},
        )

    for owner in owners:
        hand_over(0, owner).start()

    def next_block(turn, carry):
        near = lax.div(turn + 1, 2)
        away = jnp.where(lax.rem(turn, 2) == 1, near, blocks - near)
        block = lax.rem(mine + away, blocks)
        for piece in range(groups):
            arrival(block, piece).wait_recv()
        attend(block)
        return carry

    lax.fori_loop(1, blocks, next_block, 0)

    for h in range(heads):
        span = slice(width + h * LANES, width + (h + 1) * LANES)
        for index in range(tiles):
            ratio = mixed[h, index] / total[h, index][:, :1]
            values = ratio[:tile] - lam[h] * ratio[tile:]
            stage[index * tile : (index + 1) * tile, span] = rms_scale(values, att_gain[...]).astype(BF16)
    for owner in owners:
        hand_over(1, owner).start()

    for copy in own_copies + other_copies + state_copies:
        copy.wait_send()
    if groups > 1:
        swap_kv.wait_send()
        swap_rest.wait_send()
    for which in range(2):
        hand_over(which, owners[0]).wait()
        for owner in owners[1:]:
            hand_over(which, owner).wait_send()
            taken_over(which, owner).wait_recv()


def on_device_general(
    tokens, norm_gain, rec_query, fwd_gate, bwd_gate, rec_value, gate_leak, log_decay, rec_gain,
    att_query, att_key, att_value, lambdas, att_gain, out_rec, out_att,
):
    ranks = lax.axis_size("sp")
    tp = lax.axis_size("tp")
    local_heads = rec_query.shape[1] // HK
    groups = 2 if local_heads % 2 == 0 and ranks % 2 == 0 else 1
    heads = local_heads // groups
    width = heads * LANES
    slot = lax.axis_index("sp") % groups

    order = (att_key, att_value, att_query, rec_query, fwd_gate, bwd_gate, rec_value)
    length = tokens.shape[0] * tp
    vmem = pl.BlockSpec(memory_space=pltpu.VMEM)
    dma = pltpu.SemaphoreType.DMA
    projected = pl.pallas_call(
        functools.partial(gather_kernel, tp),
        out_shape=[jax.ShapeDtypeStruct((length, weight.shape[1]), BF16) for weight in order],
        in_specs=[vmem] * (2 + len(order)),
        out_specs=[vmem] * len(order),
        scratch_shapes=[
            pltpu.VMEM((length, tokens.shape[1]), BF16),
            dma((tp,)),
            dma((tp // 2,)),
            dma((tp,)),
        ],
        compiler_params=pltpu.CompilerParams(
            collective_id=1, has_side_effects=True, vmem_limit_bytes=40 * 1024 * 1024
        ),
        cost_estimate=pl.CostEstimate(flops=4 * 10**9, bytes_accessed=10**7, transcendentals=0),
    )(tokens, norm_gain.reshape(1, -1), *order)

    positions = (lax.axis_index("sp") * length + jnp.arange(length, dtype=jnp.int32)).astype(F32)
    frequency = THETA ** (-(jnp.arange(AK // 2, dtype=F32) * 2.0 / AK))
    angles = jnp.tile(positions[:, None] * frequency[None, :], (1, LANES // (AK // 2)))
    cosine, sine = jnp.cos(angles), jnp.sin(angles)

    by_head = log_decay.reshape(2, length, groups, heads).transpose(2, 1, 0, 3).reshape(groups, length, 2 * heads)
    own_decay = lax.dynamic_index_in_dim(by_head, slot, 0, keepdims=False)
    if groups > 1:
        swapped = lax.ppermute(
            lax.dynamic_index_in_dim(by_head, groups - 1 - slot, 0, keepdims=False),
            "sp",
            [(i, i + 1 - 2 * (i % 2)) for i in range(ranks)],
        )
        decay = jnp.where(
            slot == 0, jnp.concatenate([own_decay, swapped]), jnp.concatenate([swapped, own_decay])
        )
    else:
        decay = own_decay
    leak = lax.dynamic_index_in_dim(
        gate_leak.reshape(2, groups, heads, HK).transpose(1, 2, 0, 3), slot, 0, keepdims=False
    )
    lam = lax.dynamic_index_in_dim(lambdas.reshape(groups, heads), slot, 0, keepdims=False)
    lam = jnp.broadcast_to(lam[:, None, None], (heads, 1, LANES))

    blocks = ranks // groups
    rows = groups * length
    tile = min(256, length)
    mixers = pl.pallas_call(
        functools.partial(mixer_kernel, ranks, tp, groups, heads, tile),
        out_shape=jax.ShapeDtypeStruct((tp, groups, length // tp, 2 * width), BF16),
        in_specs=[vmem] * 14,
        out_specs=vmem,
        scratch_shapes=[
            pltpu.VMEM((blocks, rows, 2 * width), BF16),
            pltpu.VMEM((rows, 5 * width), BF16),
            pltpu.VMEM((length, 7 * width), BF16),
            pltpu.VMEM((rows, 2 * width), BF16),
            pltpu.VMEM((2, heads, LANES + PAD, LANES), BF16),
            pltpu.VMEM((blocks, heads, LANES + PAD, LANES), BF16),
            pltpu.VMEM((heads, 2, rows, LANES), F32),
            pltpu.VMEM((heads, 2, rows // BLOCK, LANES, LANES), F32),
            pltpu.VMEM((heads, 2, LANES, LANES), F32),
            pltpu.VMEM((rows, width), F32),
            pltpu.VMEM((heads, rows // tile, 2 * tile, LANES), F32),
            pltpu.VMEM((heads, rows // tile, 2 * tile, LANES), F32),
            pltpu.VMEM((heads, rows // tile, 2 * tile, LANES), F32),
            dma((blocks, groups)),
            dma((blocks, groups)),
            dma((2,)),
            dma,
            dma((blocks,)),
            dma((blocks,)),
            dma((2, groups, tp)),
            dma((2, tp, groups)),
        ],
        compiler_params=pltpu.CompilerParams(
            collective_id=0, has_side_effects=True, vmem_limit_bytes=56 * 1024 * 1024
        ),
        cost_estimate=pl.CostEstimate(flops=10**10, bytes_accessed=10**7, transcendentals=10**7),
    )(*projected, cosine, sine, leak, decay, lam, rec_gain.reshape(1, LANES), att_gain.reshape(1, LANES))

    shares = mixers.reshape(tp, groups, length // tp, 2, heads, LANES)
    both = shares.transpose(2, 3, 0, 1, 4, 5).reshape(length // tp, 2, -1)
    result = jnp.dot(both[:, 0], out_rec, preferred_element_type=F32) + jnp.dot(
        both[:, 1], out_att, preferred_element_type=F32
    )
    return result.astype(BF16)


def fused_kernel(
    ranks, tp, heads, planes,
    tokens_in, norm_in, w_key, w_value, w_query, w_rq, w_fwd, w_bwd, w_rv, leak_in, decay_in, rec_gain_in,
    lam_in, att_gain_in, out_rec_in, out_att_in, rotary_in,
    out,
    tokens, gain, weights, leak, decay, decay_rows, rec_gain, lam, att_gain, w_out, rotary,
    held, cosine, sine, lam_own, lam_pair, stage_kv, stage_q, kv, query, recp, cum_reads, facts, adds, rec_sum,
    state, fade, pair_out, pair_in, plane_out, plane_in, plane_sum, next_out, next_in, before_block,
    rec_stage, rec_all, score_a, score_b, top_a, top_b, acc, peak, att_stage, att_all, total,
    up, down, in_sem, across_send, across_recv, core_send, core_recv, lam_send, lam_recv,
    kv_send, kv_recv, q_send, q_recv, side_send, side_recv, near_send, near_recv,
    pair_send, pair_recv, plane_send, plane_recv, next_send, next_recv,
    rec_send, rec_recv, att_send, att_recv,
):
    sp = lax.axis_index("sp")
    me = lax.axis_index("tp")
    x = lax.rem(sp, 2)
    z = lax.div(sp, 2)
    core = lax.rem(me, 2)
    y = lax.div(me, 2)
    piece = tokens.shape[0]
    half = piece // 2
    length = piece * tp
    width = heads * LANES
    partner = {"tp": y * 2 + 1 - core}
    opposite = {"tp": (1 - y) * 2 + core}
    beside = {"sp": z * 2 + 1 - x}

    small = (
        (rotary_in, rotary), (lam_in, lam), (leak_in, leak), (decay_in, decay),
        (rec_gain_in, rec_gain), (att_gain_in, att_gain),
    )
    inputs = (w_key, w_value, w_query, w_rq, w_fwd, w_bwd, w_rv)
    moves = (
        [(tokens_in, tokens), (norm_in, gain)]
        + [(a, weights.at[i]) for i, a in enumerate(inputs)]
        + list(small) + [(out_rec_in, w_out.at[0]), (out_att_in, w_out.at[1])]
    )
    slots = (0, 1, 2, 3, 4, 5, 5, 5, 5, 6, 7, 8, 9, 10, 11, 12, 12)
    fetches = [pltpu.make_async_copy(a, b, in_sem.at[i]) for i, (a, b) in zip(slots, moves)]
    f_rotary, f_lam, f_leak, f_decay, f_rec_gain, f_att_gain = fetches[9:15]
    for fetch in fetches[:2] + fetches[9:11]:
        fetch.start()

    barrier = pltpu.get_barrier_semaphore()
    above = {"sp": sp + 2}
    below = {"sp": sp - 2}
    for to in (partner, opposite, {"tp": (1 - y) * 2 + 1 - core}, beside):
        pl.semaphore_signal(barrier, inc=1, device_id=to)

    @pl.when(z > 0)
    def _():
        pl.semaphore_signal(barrier, inc=1, device_id=below)

    @pl.when(z < planes - 1)
    def _():
        pl.semaphore_signal(barrier, inc=1, device_id=above)

    neighbours = 4 + lax.div(z + planes - 2, planes - 1) + lax.div(2 * planes - 3 - z, planes - 1)

    def chains():
        def pass_up():
            @pl.when(z > 0)
            def _():
                pl.semaphore_wait(up, 1)

            @pl.when(z < planes - 1)
            def _():
                pl.semaphore_signal(up, inc=1, device_id=above)

        def pass_down():
            @pl.when(z < planes - 1)
            def _():
                pl.semaphore_wait(down, 1)

            @pl.when(z > 0)
            def _():
                pl.semaphore_signal(down, inc=1, device_id=below)

        @pl.when(2 * z < planes)
        def _():
            pass_up()
            pass_down()

        @pl.when(2 * z >= planes)
        def _():
            pass_down()
            pass_up()

    def remote(source, target, send, recv, to):
        return pltpu.make_async_remote_copy(
            src_ref=source, dst_ref=target, send_sem=send, recv_sem=recv, device_id=to
        )

    def held_at(owner, part, side):
        return owner * 2 * piece + part * piece + side * half

    def held_rows(owner, part, side):
        return held.at[pl.ds(pl.multiple_of(held_at(owner, part, side), half), half)]

    def across(part, owner):
        rows = held_rows(owner, part, core)
        return remote(rows, rows, across_send, across_recv.at[part], opposite)

    def to_core(owner, part, side, slot):
        rows = held_rows(owner, part, side)
        return remote(rows, rows, core_send, core_recv.at[slot], partner)

    fetches[0].wait()
    fetches[1].wait()
    for fetch in fetches[2:9] + fetches[11:15]:
        fetch.start()
    for part in range(2):
        rows = tokens[part * half : (part + 1) * half, :].astype(F32)
        at = pl.ds(pl.multiple_of(held_at(y, part, core), half), half)
        held[at, :] = rms_scale(rows, gain[...]).astype(BF16)
        if part == 0:
            pl.semaphore_wait(barrier, neighbours)
        across(part, y).start()
        to_core(y, part, core, part).start()
    f_lam.wait()
    for i in range(heads):
        lam_own[i] = jnp.broadcast_to(lam[:, i : i + 1], (8, LANES))
    lam_copy = remote(lam_own, lam_pair, lam_send, lam_recv, partner)
    lam_copy.start()

    f_rotary.wait()
    lane = lax.broadcasted_iota(jnp.int32, (piece, LANES), 1)
    low_half = lax.rem(lane, AK) < AK // 2
    for t in range(tp):
        begin = 2 * piece + sp * tp + t
        cos_base = rotary[pl.ds(begin, 1), :]
        sin_base = rotary[pl.ds(begin + ranks * tp, 1), :]
        cos_row, sin_row = rotary[:piece, :], rotary[piece : 2 * piece, :]
        turned = sin_base * cos_row + cos_base * sin_row
        cos_here = cos_base * cos_row - sin_base * sin_row
        sin_here = jnp.where(low_half, -turned, turned)
        for part in range(2):
            to = held_at(t // 2, part, t % 2)
            cosine[to : to + half, :] = cos_here[part * half : (part + 1) * half]
            sine[to : to + half, :] = sin_here[part * half : (part + 1) * half]

    def rotated(wide, cos_at, sin_at):
        rows = wide.shape[0]
        low = jnp.concatenate([low_half] * (rows // piece), axis=0)
        turned = jnp.where(low, pltpu.roll(wide, LANES - AK // 2, 1), pltpu.roll(wide, AK // 2, 1))
        return wide * cos_at + turned * sin_at

    def owner_of(phase):
        return y if phase < 2 else 1 - y

    def plane_copy(phase, i, kind):
        return remote(
            stage_kv.at[phase, i, kind], kv.at[kind, 0, phase, z], kv_send, kv_recv.at[phase, z],
            {"sp": (core * heads + i) * 2 + x, "tp": y * 2 + kind},
        )

    def query_rows(phase, plane):
        return query.at[phase, pl.ds(pl.multiple_of(plane * half, half), half)]

    def query_copy(phase, i, c):
        return remote(
            stage_q.at[phase, i, c], query_rows(phase, z), q_send, q_recv.at[phase],
            {"sp": (core * heads + i) * 2 + x, "tp": y * 2 + c},
        )

    def is_own(i, c):
        return jnp.logical_and(core * heads + i == z, core == c)

    def project(at, index):
        return jnp.dot(held[at, :], weights[index], preferred_element_type=F32)

    def attention_inputs(phases):
        count = len(phases) * piece
        owner = owner_of(phases[0])
        at = pl.ds(pl.multiple_of(held_at(owner, phases[0] % 2, 0), piece), count)
        cos_at, sin_at = cosine[at, :], sine[at, :]
        if phases[0] == 0:
            fetches[2].wait()
        keys = project(at, 0).astype(BF16).astype(F32)
        if phases[0] == 0:
            fetches[3].wait()
        values = project(at, 1).astype(BF16).astype(F32)
        for i in range(heads):
            span = slice(i * LANES, (i + 1) * LANES)
            value = values[:, span].T.astype(BF16)
            key = rotated(keys[:, span], cos_at, sin_at).astype(BF16)
            for n, phase in enumerate(phases):
                part = slice(n * piece, (n + 1) * piece)
                stage_kv[phase, i, 0] = value[:, part]
                stage_kv[phase, i, 1] = key[part]
        if phases[0] == 0:
            chains()
        for phase in phases:
            send_each(phase, plane_copy, kv_recv.at[phase, z], lambda i, c: (stage_kv.at[phase, i, c], kv.at[c, 0, phase, z]))
        if phases[0] == 0:
            fetches[4].wait()
        queries = project(at, 2).astype(BF16).astype(F32)
        for i in range(heads):
            span = slice(i * LANES, (i + 1) * LANES)
            turned = (rotated(queries[:, span], cos_at, sin_at) * AK ** (-0.5)).astype(BF16)
            for n, phase in enumerate(phases):
                for c in range(2):
                    stage_q[phase, i, c] = turned[n * piece + c * half : n * piece + (c + 1) * half]
        for phase in phases:
            send_each(phase, query_copy, q_recv.at[phase], lambda i, c: (stage_q.at[phase, i, c], query_rows(phase, z)))

    def send_each(phase, copy, recv, local):
        for i in range(heads):
            for c in range(2):
                own = is_own(i, c)

                @pl.when(own)
                def _():
                    source, target = local(i, c)
                    pltpu.make_async_copy(source, target, recv).start()

                @pl.when(jnp.logical_not(own))
                def _():
                    copy(phase, i, c).start()

    def recurrence_inputs(owner, wait):
        at = pl.ds(pl.multiple_of(held_at(owner, 0, 0), 2 * piece), 2 * piece)
        if wait:
            pltpu.make_async_copy(weights.at[3:7], weights.at[3:7], in_sem.at[5]).wait()
        for i in range(4):
            recp[i, at, :] = project(at, 3 + i).astype(BF16)

    def plane_at(k):
        return (z, z + 1 - 2 * lax.rem(z, 2), lax.rem(z + 2, planes), planes - 1 - z)[k]

    def mine_of(origin, phase, plane):
        return kv.at[core, origin, phase, plane]

    def to_side(phase, plane):
        return remote(
            mine_of(0, phase, plane), mine_of(1, phase, plane),
            side_send, side_recv.at[phase, plane], beside,
        )

    def to_near(origin, phase, plane):
        block = mine_of(origin, phase, plane)
        return remote(
            block, block, near_send, near_recv.at[phase], partner
        )

    def relay_plane(phase, k):
        plane = plane_at(k)
        block = mine_of(0, phase, plane)
        remote(block, block, near_send, kv_recv.at[phase, plane], partner).wait_recv()
        to_side(phase, plane).start()
        to_near(0, phase, plane).start()

    def relay_side(phase, k):
        plane = plane_at(k)
        block = mine_of(1, phase, plane)
        remote(block, block, side_send, side_recv.at[phase, plane], beside).wait_recv()
        to_near(1, phase, plane).start()

    def settle(phase):
        blocks_in = kv.at[1 - core, :, phase]
        remote(blocks_in, blocks_in, near_send, near_recv.at[phase], partner).wait_recv()

    def settle_queries(phase):
        rows = query.at[phase]
        remote(rows, rows, q_send, q_recv.at[phase], partner).wait_recv()

    row_at = lax.broadcasted_iota(jnp.int32, (BLOCK, 3 * BLOCK), 0)
    col_at = lax.rem(lax.broadcasted_iota(jnp.int32, (BLOCK, 3 * BLOCK), 1), BLOCK)
    triangles = (jnp.where(row_at >= col_at, 1.0, 0.0).astype(BF16), jnp.where(row_at <= col_at, 1.0, 0.0).astype(BF16))
    row_in = lax.broadcasted_iota(jnp.int32, (BLOCK, BLOCK), 0)
    col_in = lax.broadcasted_iota(jnp.int32, (BLOCK, BLOCK), 1)
    earlier = (row_in >= col_in, row_in <= col_in)
    ends = (BLOCK - 1, 0)
    middles = (BLOCK // 2 - 1, BLOCK // 2)
    blocks = length // BLOCK
    spans = [slice(h * LANES, (h + 1) * LANES) for h in range(heads)]

    def within_block(b):
        at = pl.ds(pl.multiple_of(b * BLOCK, BLOCK), BLOCK)
        t = lax.div(b, 2)
        stored = held_at(lax.div(t, 2), lax.rem(b, 2), lax.rem(t, 2))
        held_block = pl.ds(pl.multiple_of(stored, BLOCK), BLOCK)
        queries = jax.nn.silu(recp[0, held_block, :].astype(F32))
        values = recp[3, held_block, :]
        scores, tails = [], []
        for d in range(2):
            keys = leak[d : d + 1, :] * jax.nn.sigmoid(-recp[1 + d, held_block, :].astype(F32))
            added = jnp.concatenate(
                [jnp.broadcast_to(decay_rows[at, d * heads + h : d * heads + h + 1], (BLOCK, LANES)) for h in range(heads)],
                axis=1,
            )
            logs = jnp.log1p(-keys) + added
            coarse = logs.astype(BF16)
            rest = logs - coarse.astype(F32)
            fine = rest.astype(BF16)
            finest = (rest - fine.astype(F32)).astype(BF16)
            cum = jnp.dot(
                triangles[d], jnp.concatenate([coarse, fine, finest], axis=0), preferred_element_type=F32
            )
            middle = cum[middles[d] : middles[d] + 1, :]
            last = cum[ends[d] : ends[d] + 1, :]
            reads = (queries * jnp.exp(cum - middle)).astype(BF16)
            writes = (keys * jnp.exp(middle - cum)).astype(BF16)
            tails.append((keys * jnp.exp(last - cum)).astype(BF16))
            carried = (queries * jnp.exp(cum)).astype(BF16)
            facts[b, d] = jnp.broadcast_to(jnp.exp(last), (8, width))
            scores.append([jnp.where(earlier[d], dot_t(reads[:, s], writes[:, s]), 0.0) for s in spans])
            for h in range(heads):
                cum_reads[h, at, d * LANES : (d + 1) * LANES] = carried[:, spans[h]]
        for h in range(heads):
            both = (scores[0][h] + scores[1][h]).astype(BF16)
            rec_sum[at, spans[h]] = jnp.dot(both, values[:, spans[h]], preferred_element_type=F32)
            adds[b, h] = dot_0(
                values[:, spans[h]], jnp.concatenate([tails[0][:, spans[h]], tails[1][:, spans[h]]], axis=1)
            )

    def within_rows(owner):
        count = blocks // 2

        def some(j, carry):
            within_block(owner * count + 2 * j)
            within_block(owner * count + 2 * j + 1)
            return carry

        lax.fori_loop(0, count // 2, some, 0)

    def order(d):
        return range(blocks) if d == 0 else range(blocks - 1, -1, -1)

    def half_of(d):
        return slice(d * LANES, (d + 1) * LANES)

    first_row = lax.broadcasted_iota(jnp.int32, (PAD, LANES), 0) == 0

    def pack(target, moved, factor):
        target[:LANES, :] = moved.astype(BF16)
        wide = jnp.broadcast_to(factor, (PAD, LANES))
        coarse = wide.astype(BF16).astype(F32)
        target[LANES:, :] = jnp.where(first_row, coarse, wide - coarse).astype(BF16)

    def unpack(source):
        last = source[LANES:, :].astype(F32)
        return source[:LANES, :].astype(F32), last[0:1] + last[1:2]

    def local_states():
        for h in range(heads):
            for d in range(2):
                moved = jnp.zeros((LANES, LANES), F32)
                factor = jnp.ones((1, LANES), F32)
                for b in order(d):
                    step = facts[b, d, 0:1, spans[h]]
                    moved = moved * step + adds[b, h, :, half_of(d)]
                    factor = factor * step
                state[d, h] = moved
                fade[d, h] = jnp.broadcast_to(factor, (8, LANES))
                pack(pair_out.at[d, h], moved, factor)

    pair_copy = remote(pair_out, pair_in, pair_send, pair_recv, beside)

    def pair_states():
        pair_copy.wait_recv()
        for d in range(2):
            mine, factor = state[d, x], fade[d, x][0:1]
            other, other_factor = unpack(pair_in.at[d, x])
            joined = jnp.where(x == d, mine * other_factor + other, other * factor + mine)
            pack(plane_out.at[d], joined, factor * other_factor)
        for dz in range(1, planes):
            to_plane(lax.rem(z + dz, planes)).start()

    def to_plane(target):
        return remote(
            plane_out.at[jnp.where(target > z, 0, 1)], plane_in.at[z],
            plane_send, plane_recv, {"sp": target * 2 + x},
        )

    def other_planes():
        blocks_in = plane_in.at[: planes - 1]
        return remote(blocks_in, blocks_in, plane_send, plane_recv, partner)

    next_copy = remote(next_out, next_in, next_send, next_recv, beside)

    def plane_states():
        other_planes().wait_recv()
        plane_sum[...] = jnp.zeros_like(plane_sum)

        def fold(d):
            def one(step, carry):
                plane = step if d == 0 else planes - 1 - step
                moved, factor = unpack(plane_in.at[plane])
                plane_sum[d] = plane_sum[d] * factor + moved
                return carry

            return one

        lax.fori_loop(0, z, fold(0), 0)
        lax.fori_loop(0, planes - 1 - z, fold(1), 0)
        next_out[...] = plane_sum[...].astype(BF16)
        next_copy.start()

    def second_pass():
        next_copy.wait_recv()
        for h in range(heads):
            for d in range(2):
                entering = jnp.where(x == h, plane_sum[d], next_in[d].astype(F32))
                other, other_factor = unpack(pair_in.at[d, h])
                running = jnp.where(x == d, entering, entering * other_factor + other)
                for b in order(d):
                    before_block[b, h, :, half_of(d)] = running.astype(BF16)
                    running = running * facts[b, d, 0:1, spans[h]] + adds[b, h, :, half_of(d)]
            for b in range(blocks):
                at = slice(b * BLOCK, (b + 1) * BLOCK)
                whole = rec_sum[at, spans[h]] + dot_t(cum_reads[h, at, :], before_block[b, h])
                rec_stage[at, spans[h]] = rms_scale(whole, rec_gain[...]).astype(BF16)
        for dt in range(tp):
            rec_copy(dt).start()

    def rec_copy(dt):
        t = lax.rem(me + dt, tp)
        source = rec_stage.at[pl.ds(pl.multiple_of(t * piece, piece), piece)]
        if dt == 0:
            return pltpu.make_async_copy(source, rec_all.at[me], rec_recv)
        return remote(source, rec_all.at[me], rec_send, rec_recv, {"tp": t})

    acc[...] = jnp.zeros_like(acc)
    peak[...] = jnp.full_like(peak, -jnp.inf)
    sub = 2 * piece
    ones = jnp.ones((PAD, sub), BF16)
    low_map = lane < AK
    buffers = ((score_a, top_a), (score_b, top_b))

    def attend_step(made, made_buffer, used, used_buffer):
        if made is not None:
            q_phase, tile, made_phases = made
            chunk = made_phases
            rows = query[q_phase, tile * piece : (tile + 1) * piece, :]
            none = jnp.zeros_like(rows)
            both = jnp.concatenate([jnp.where(low_map, rows, none), jnp.where(low_map, none, rows)], axis=0)
            top = None
        if used is not None:
            slot, chunk = used[0] * 2 + used[1], used[2]
            used_score, used_top = used_buffer
            before = peak[slot][0:1]
            now = jnp.maximum(before, jnp.max(used_top[...], axis=0, keepdims=True))
            mixed = acc[slot] * jnp.exp(before - now)
        for u in range(0, 2 * planes * len(chunk), 2):
            at = slice(u * piece, (u + 2) * piece)
            turn, pair = u // (2 * planes), u % (2 * planes)
            where = [((pair + n) // planes, (pair + n) % planes) for n in range(2)]
            if made is not None:
                keys = jnp.concatenate([kv[1, o, made_phases[turn], p] for o, p in where], axis=0)
                scores = dot_t(keys, both)
                made_buffer[0][at, :] = scores
                high = jnp.max(scores.reshape(sub // 8, 8, 2 * piece), axis=0)
                top = high if top is None else jnp.maximum(top, high)
            if used is not None:
                expo = jnp.exp(used_score[at, :] - now).astype(BF16)
                values = jnp.concatenate([kv[0, o, used[2][turn], p] for o, p in where], axis=1)
                values = jnp.concatenate([values, ones], axis=0)
                mixed = mixed + jnp.dot(values, expo, preferred_element_type=F32)
        if used is not None:
            acc[slot] = mixed
            peak[slot] = jnp.broadcast_to(now, (8, 2 * piece))
        if made is not None:
            made_buffer[1][...] = top

    def att_copy(q_phase, plane):
        owner, part = owner_of(q_phase), q_phase % 2
        return remote(
            att_stage.at[q_phase * planes + plane], att_all.at[y * planes + z, part * half : (part + 1) * half],
            att_send, att_recv,
            {"sp": plane * 2 + x, "tp": owner * 2 + core},
        )

    def finish(q_phase, tile):
        whole = acc[q_phase * 2 + tile]
        ratio = whole[:LANES] / whole[LANES : LANES + 1]
        weight = jnp.where(core == lax.div(z, heads), lam_own[lax.rem(z, heads)], lam_pair[lax.rem(z, heads)])[0:1]
        values = ratio[:, :piece] - weight * ratio[:, piece:]
        scale = lax.rsqrt(jnp.mean(values * values, axis=0, keepdims=True) + EPS)
        rows = ((values * scale).T * att_gain[...]).astype(BF16)
        part = q_phase % 2
        for n in range(2):
            plane = 2 * tile + n
            att_stage[q_phase * planes + plane] = rows[n * half : (n + 1) * half]
            if q_phase < 2:

                @pl.when(plane == z)
                def _():
                    pltpu.make_async_copy(
                        att_stage.at[q_phase * planes + plane],
                        att_all.at[y * planes + z, part * half : (part + 1) * half],
                        att_recv,
                    ).start()

                @pl.when(plane != z)
                def _():
                    att_copy(q_phase, plane).start()
            else:
                att_copy(q_phase, plane).start()

    columns = min(512, out.shape[1])

    def rec_total():
        pltpu.make_async_copy(w_out, w_out, in_sem.at[12]).wait()
        remote(rec_all, rec_all, rec_send, rec_recv, partner).wait_recv()
        rec_rows = jnp.concatenate([rec_all[t] for t in range(tp)], axis=1)
        for n in range(0, out.shape[1], columns):
            total[:, n : n + columns] = jnp.dot(rec_rows, w_out[0, :, n : n + columns], preferred_element_type=F32)

    def run_units(units, before):
        for n in range(len(units) + 1):
            for action in before.get(n, ()):
                action()
            made = units[n] if n < len(units) else None
            used = units[n - 1] if n else None
            attend_step(made, buffers[n % 2], used, buffers[(n + 1) % 2])
            if used is not None and used[2][-1] == 3:
                finish(used[0], used[1])

    def tiles_of(q_phases, chunk):
        return [(q_phase, tile, chunk) for q_phase in q_phases for tile in range(2)]

    def call(f, *args):
        return functools.partial(f, *args)

    def all_of(f, phase, ks):
        return [call(f, phase, k) for k in ks]

    near, far = (0, 1), (2, 3)
    units = tiles_of(near, near) + tiles_of(far, near) + tiles_of(near, far) + tiles_of(far, far)
    before = {
        1: [call(relay_plane, 2, 0), call(relay_plane, 2, 1)],
        2: [call(relay_plane, 2, 2), call(relay_plane, 2, 3), pair_states],
        3: all_of(relay_side, 2, range(2)),
        4: all_of(relay_plane, 3, range(4)) + [call(settle_queries, 2), call(settle_queries, 3)],
        5: all_of(relay_side, 2, range(2, 4)) + [plane_states],
        6: all_of(relay_side, 3, range(2)),
        7: all_of(relay_side, 3, range(2, 4)),
        8: [call(settle, 2), call(settle, 3)],
        12: [second_pass],
    }

    for part in range(2):
        to_core(y, part, 1 - core, part).wait_recv()
    attention_inputs(near)
    for fetch in fetches[15:17]:
        fetch.start()
    recurrence_inputs(y, True)
    for fetch in (f_leak, f_decay, f_rec_gain, f_att_gain):
        fetch.wait()
    by_row = jnp.concatenate([decay[d] for d in range(2)] + [jnp.zeros((LANES - 2 * heads, length), F32)], axis=0)
    decay_rows[...] = by_row.T
    relay_plane(0, 0)
    relay_plane(1, 0)
    within_rows(y)
    relay_plane(0, 1)
    across(0, 1 - y).wait_recv()
    to_core(1 - y, 0, core, 2).start()
    relay_plane(0, 2)
    relay_plane(0, 3)
    relay_side(0, 0)
    across(1, 1 - y).wait_recv()
    to_core(1 - y, 1, core, 3).start()
    relay_plane(1, 1)
    for part in range(2):
        to_core(1 - y, part, 1 - core, 2 + part).wait_recv()
    attention_inputs(far)
    relay_plane(1, 2)
    relay_plane(1, 3)
    for k in range(1, 4):
        relay_side(0, k)
    recurrence_inputs(1 - y, False)
    relay_side(1, 0)
    relay_side(1, 1)
    within_rows(1 - y)
    local_states()
    pair_copy.start()
    relay_side(1, 2)
    relay_side(1, 3)
    lam_copy.wait_recv()
    for phase in near:
        settle(phase)
        settle_queries(phase)
    run_units(units, before)
    rec_total()

    remote(att_all, att_all, att_send, att_recv, partner).wait_recv()
    att_rows = jnp.concatenate([att_all[i] for i in range(2 * planes)], axis=1)
    for n in range(0, out.shape[1], columns):
        out[:, n : n + columns] = (
            total[:, n : n + columns]
            + jnp.dot(att_rows, w_out[1, :, n : n + columns], preferred_element_type=F32)
        ).astype(BF16)

    def sent(ref, sem, recv):
        remote(ref, ref, sem, recv, partner).wait_send()

    sent(held.at[:piece], across_send, core_recv.at[0])
    sent(held.at[: 2 * piece], core_send, core_recv.at[0])
    lam_copy.wait_send()
    is_local = core == lax.div(z, heads)

    @pl.when(is_local)
    def _():
        sent(stage_kv.at[:3], kv_send, near_recv.at[0])
        sent(stage_q.at[:3], q_send, near_recv.at[0])

    @pl.when(jnp.logical_not(is_local))
    def _():
        sent(stage_kv, kv_send, near_recv.at[0])
        sent(stage_q, q_send, near_recv.at[0])

    sent(kv.at[0, 0], side_send, near_recv.at[0])
    sent(kv.at[0], near_send, near_recv.at[0])
    pair_copy.wait_send()
    next_copy.wait_send()
    sent(plane_in.at[: planes - 1], plane_send, plane_recv)
    sent(rec_all.at[: tp - 1], rec_send, rec_recv)
    sent(att_stage.at[: 4 * planes - 2], att_send, att_recv)


def rotary_table(piece, pieces):
    frequency = THETA ** (-(np.arange(LANES) % (AK // 2)) * 2.0 / AK)
    inside = np.arange(piece)[:, None] * frequency[None, :]
    base = (np.arange(pieces) * piece)[:, None] * frequency[None, :]
    return np.concatenate([np.cos(inside), np.sin(inside), np.cos(base), np.sin(base)]).astype(np.float32)


def on_device(
    tokens, norm_gain, rec_query, fwd_gate, bwd_gate, rec_value, gate_leak, log_decay, rec_gain,
    att_query, att_key, att_value, lambdas, att_gain, out_rec, out_att,
):
    ranks = lax.axis_size("sp")
    tp = lax.axis_size("tp")
    heads = rec_query.shape[1] // HK
    planes = ranks // 2
    piece, model = tokens.shape
    if tp != 4 or planes != 2 * heads or planes != 4 or piece != LANES:
        return on_device_general(
            tokens, norm_gain, rec_query, fwd_gate, bwd_gate, rec_value, gate_leak, log_decay, rec_gain,
            att_query, att_key, att_value, lambdas, att_gain, out_rec, out_att,
        )
    length = piece * tp
    width = heads * LANES
    blocks = length // BLOCK
    keys = 4 * planes * piece
    anywhere = pl.BlockSpec(memory_space=pl.ANY)
    dma = pltpu.SemaphoreType.DMA
    vmem = pltpu.VMEM
    table = jnp.asarray(rotary_table(piece, ranks * tp))
    return pl.pallas_call(
        functools.partial(fused_kernel, ranks, tp, heads, planes),
        out_shape=jax.ShapeDtypeStruct((piece, model), BF16),
        in_specs=[anywhere] * 17,
        out_specs=pl.BlockSpec(memory_space=pltpu.VMEM),
        scratch_shapes=[
            vmem((piece, model), BF16),
            vmem((1, model), F32),
            vmem((7, model, width), BF16),
            vmem((2, width), F32),
            vmem((2, heads, length), F32),
            vmem((length, LANES), F32),
            vmem((1, LANES), F32),
            vmem((1, heads), F32),
            vmem((1, LANES), F32),
            vmem((2, *out_rec.shape), BF16),
            vmem(table.shape, F32),
            vmem((length, model), BF16),
            vmem((length, LANES), F32),
            vmem((length, LANES), F32),
            vmem((heads, 8, LANES), F32),
            vmem((heads, 8, LANES), F32),
            vmem((4, heads, 2, piece, LANES), BF16),
            vmem((4, heads, 2, piece // 2, LANES), BF16),
            vmem((2, 2, 4, planes, piece, LANES), BF16),
            vmem((4, planes * piece // 2, LANES), BF16),
            vmem((4, length, width), BF16),
            vmem((heads, length, 2 * LANES), BF16),
            vmem((blocks, 2, 8, width), F32),
            vmem((blocks, heads, LANES, 2 * LANES), F32),
            vmem((length, width), F32),
            vmem((2, heads, LANES, LANES), F32),
            vmem((2, heads, 8, LANES), F32),
            vmem((2, heads, LANES + PAD, LANES), BF16),
            vmem((2, heads, LANES + PAD, LANES), BF16),
            vmem((2, LANES + PAD, LANES), BF16),
            vmem((planes, LANES + PAD, LANES), BF16),
            vmem((2, LANES, LANES), F32),
            vmem((2, LANES, LANES), BF16),
            vmem((2, LANES, LANES), BF16),
            vmem((blocks, heads, LANES, 2 * LANES), BF16),
            vmem((length, width), BF16),
            vmem((tp, piece, width), BF16),
            vmem((keys, 2 * piece), F32),
            vmem((keys, 2 * piece), F32),
            vmem((8, 2 * piece), F32),
            vmem((8, 2 * piece), F32),
            vmem((2 * planes, LANES + PAD, 2 * piece), F32),
            vmem((2 * planes, 8, 2 * piece), F32),
            vmem((4 * planes, piece // 2, LANES), BF16),
            vmem((2 * planes, piece, LANES), BF16),
            vmem((piece, model), F32),
            pltpu.SemaphoreType.REGULAR, pltpu.SemaphoreType.REGULAR,
            dma((13,)), dma, dma((2,)), dma, dma((4,)), dma, dma,
            dma, dma((4, planes)), dma, dma((4,)),
            dma, dma((4, planes)), dma, dma((4,)),
            dma, dma, dma, dma, dma, dma,
            dma, dma, dma, dma,
        ],
        compiler_params=pltpu.CompilerParams(
            collective_id=2, has_side_effects=True, vmem_limit_bytes=60 * 1024 * 1024
        ),
        cost_estimate=pl.CostEstimate(flops=10**10, bytes_accessed=10**7, transcendentals=10**7),
    )(
        tokens, norm_gain.reshape(1, -1), att_key, att_value, att_query, rec_query, fwd_gate, bwd_gate, rec_value,
        gate_leak, log_decay.transpose(0, 2, 1), rec_gain.reshape(1, LANES), lambdas.reshape(1, heads), att_gain.reshape(1, LANES),
        out_rec, out_att, table,
    )


def solution(mesh):
    placed = (
        P(("sp", "tp"), None), P(), P(None, "tp"), P(None, "tp"), P(None, "tp"), P(None, "tp"),
        P(None, "tp"), P(None, "sp", "tp"), P(), P(None, "tp"), P(None, "tp"), P(None, "tp"),
        P("tp"), P(), P(), P(),
    )
    return jax.shard_map(
        on_device, mesh=mesh, in_specs=placed, out_specs=P(("sp", "tp"), None), check_vma=False
    )
```

```python
import functools

import jax
import jax.numpy as jnp
import numpy as np
from jax import lax
from jax.experimental import pallas as pl
from jax.experimental.pallas import tpu as pltpu
from jax.sharding import PartitionSpec as P

HK = 128
AK = 64
BLOCK = 64
LANES = 128
EPS = 1e-06
THETA = 500000.0
HIGHEST = lax.Precision.HIGHEST
F32 = jnp.float32
BF16 = jnp.bfloat16
PAD = 16


def rms_scale(values, gain):
    return values * lax.rsqrt(jnp.mean(values * values, axis=-1, keepdims=True) + EPS) * gain


def dot_t(a, b):
    return lax.dot_general(a, b, (((1,), (1,)), ((), ())), preferred_element_type=F32)


def dot_0(a, b):
    return lax.dot_general(a, b, (((0,), (0,)), ((), ())), preferred_element_type=F32)


def gather_kernel(tp, tokens, gain, *refs):
    weights, outs = refs[:7], refs[7:14]
    held, across, along, landed = refs[14:]
    me = lax.axis_index("tp")
    core = lax.rem(me, 2)
    pair = lax.div(me, 2)
    pairs = tp // 2
    count = tokens.shape[0]
    partner = pair * 2 + 1 - core
    others = [lax.rem(pair + k, pairs) for k in range(1, pairs)]
    barrier = pltpu.get_barrier_semaphore()
    pl.semaphore_signal(barrier, inc=1, device_id={"tp": partner})
    for q in others:
        pl.semaphore_signal(barrier, inc=1, device_id={"tp": q * 2 + core})

    def rows_at(block):
        return held.at[pl.ds(pl.multiple_of(block * count, count), count)]

    def to_partner(block):
        return pltpu.make_async_remote_copy(
            src_ref=rows_at(block),
            dst_ref=rows_at(block),
            send_sem=across.at[block],
            recv_sem=landed.at[block],
            device_id={"tp": partner},
        )

    def to_pair(q):
        return pltpu.make_async_remote_copy(
            src_ref=rows_at(me),
            dst_ref=rows_at(me),
            send_sem=along.at[q],
            recv_sem=landed.at[me],
            device_id={"tp": q * 2 + core},
        )

    normed = rms_scale(tokens[...].astype(F32), gain[...]).astype(BF16)
    held[pl.ds(pl.multiple_of(me * count, count), count), :] = normed
    pl.semaphore_wait(barrier, pairs)
    for q in others:
        to_pair(q).start()
    to_partner(me).start()

    def step(k, carry):
        q = lax.rem(pair + k, pairs)
        near = q * 2 + core

        @pl.when(k > 0)
        def _():
            to_partner(near).wait_recv()
            to_partner(near).start()

        to_partner(q * 2 + 1 - core).wait_recv()
        at = pl.ds(pl.multiple_of(q * 2 * count, 2 * count), 2 * count)
        for weight, result in zip(weights, outs):
            result[at, :] = jnp.dot(held[at, :], weight[...], preferred_element_type=F32).astype(BF16)
        return carry

    lax.fori_loop(0, pairs, step, 0)
    to_partner(me).wait_send()
    for q in others:
        to_pair(q).wait_send()
        to_partner(q * 2 + core).wait_send()


def mixer_kernel(
    ranks, tp, groups, heads, tile,
    proj_k, proj_v, proj_q, proj_rq, proj_fwd, proj_bwd, proj_rv, cosine, sine, leak, decay, lam, rec_gain, att_gain,
    out,
    kv, rest, swap, stage, state_out, state_in, cums, adds, states, rec_sum, peak, total, mixed,
    kv_send, kv_recv, swap_send, rest_recv, state_send, state_recv, out_send, out_recv,
):
    me = lax.axis_index("sp")
    slot = lax.rem(me, groups)
    mine = lax.div(me, groups)
    mesh_column = lax.axis_index("tp")
    length = proj_k.shape[0]
    piece = length // tp
    rows = groups * length
    width = heads * LANES
    block_count = rows // BLOCK
    partner_slot = groups - 1 - slot
    partner = mine * groups + partner_slot
    blocks = ranks // groups
    own_rows = pl.ds(pl.multiple_of(slot * length, length), length)
    other_rows = pl.ds(pl.multiple_of(partner_slot * length, length), length)

    barrier = pltpu.get_barrier_semaphore()
    peers = []
    for k in range(1, blocks):
        peers.append(lax.rem(mine + k, blocks))
    for peer in peers:
        pl.semaphore_signal(barrier, inc=1, device_id={"sp": peer * groups + slot})
    owners = []
    for dp in range(groups):
        for dt in range(tp):
            owners.append((dp, dt, lax.rem(slot + dp, groups), lax.rem(mesh_column + dt, tp)))
    for dp, dt, p, t in owners[1:]:
        pl.semaphore_signal(barrier, inc=1, device_id={"sp": mine * groups + p, "tp": t})

    lane = lax.broadcasted_iota(jnp.int32, (length, LANES), 1)
    low_half = lax.rem(lane, AK) < AK // 2

    def rotated(raw):
        wide = raw.astype(F32)
        turned = jnp.where(low_half, -pltpu.roll(wide, LANES - AK // 2, 1), pltpu.roll(wide, AK // 2, 1))
        return wide * cosine[...] + turned * sine[...]

    def prepare(head_group, key_value, others):
        def taken(ref, h):
            return ref[:, pl.ds(pl.multiple_of((head_group * heads + h) * LANES, LANES), LANES)]

        for h in range(heads):
            at = h * LANES
            key_value[:, at : at + LANES] = rotated(taken(proj_k, h)).astype(BF16)
            key_value[:, width + at : width + at + LANES] = taken(proj_v, h)
            others[:, at : at + LANES] = (rotated(taken(proj_q, h)) * AK ** (-0.5)).astype(BF16)
            for i, ref in enumerate((proj_rq, proj_fwd, proj_bwd, proj_rv)):
                others[:, (i + 1) * width + at : (i + 1) * width + at + LANES] = taken(ref, h)

    if groups > 1:
        prepare(partner_slot, swap.at[:, : 2 * width], swap.at[:, 2 * width :])
    prepare(slot, kv.at[mine, own_rows], rest.at[own_rows])
    pl.semaphore_wait(barrier, blocks - 1 + groups * tp - 1)

    def block_copy(source_rows, source_slot, peer):
        return pltpu.make_async_remote_copy(
            src_ref=kv.at[mine, source_rows],
            dst_ref=kv.at[mine, source_rows],
            send_sem=kv_send.at[peer, source_slot],
            recv_sem=kv_recv.at[mine, source_slot],
            device_id={"sp": peer * groups + slot},
        )

    def arrival(block, piece):
        piece_rows = pl.ds(pl.multiple_of(piece * length, length), length)
        return pltpu.make_async_remote_copy(
            src_ref=kv.at[block, piece_rows],
            dst_ref=kv.at[block, piece_rows],
            send_sem=kv_send.at[block, piece],
            recv_sem=kv_recv.at[block, piece],
            device_id={"sp": block * groups + slot},
        )

    if groups > 1:
        swap_kv = pltpu.make_async_remote_copy(
            src_ref=swap.at[:, : 2 * width],
            dst_ref=kv.at[mine, own_rows],
            send_sem=swap_send.at[0],
            recv_sem=kv_recv.at[mine, slot],
            device_id={"sp": partner},
        )
        swap_kv.start()
        swap_rest = pltpu.make_async_remote_copy(
            src_ref=swap.at[:, 2 * width :],
            dst_ref=rest.at[own_rows],
            send_sem=swap_send.at[1],
            recv_sem=rest_recv,
            device_id={"sp": partner},
        )
    own_copies = [block_copy(own_rows, slot, peer) for peer in peers]
    for copy in own_copies:
        copy.start()
    other_copies = []
    if groups > 1:
        swap_rest.start()
        arrival(mine, partner_slot).wait_recv()
        other_copies = [block_copy(other_rows, partner_slot, peer) for peer in peers]
        for copy in other_copies:
            copy.start()
        swap_rest.wait_recv()

    row_at = lax.broadcasted_iota(jnp.int32, (BLOCK, BLOCK), 0)
    col_at = lax.broadcasted_iota(jnp.int32, (BLOCK, BLOCK), 1)
    earlier = (row_at >= col_at, row_at <= col_at)
    triangles = tuple(mask.astype(F32) for mask in earlier)
    ends = (BLOCK - 1, 0)
    middles = (BLOCK // 2 - 1, BLOCK // 2)

    def rows_of(direction, step):
        index = step if direction == 0 else block_count - 1 - step
        return index, pl.ds(pl.multiple_of(index * BLOCK, BLOCK), BLOCK)

    def part(at, index, h):
        return rest[at, (index * heads + h) * LANES : (index * heads + h + 1) * LANES].astype(F32)

    def keys_of(at, direction, h):
        return leak[h, direction : direction + 1, :] * jax.nn.sigmoid(-part(at, 2 + direction, h))

    states[...] = jnp.zeros_like(states)
    rec_sum[...] = jnp.zeros_like(rec_sum)

    def first_pass(step, totals):
        after = []
        for h in range(heads):
            for d in range(2):
                index, at = rows_of(d, step)
                keys = keys_of(at, d, h)
                column = d * heads + h
                logs = jnp.log1p(-keys) + decay[at, column : column + 1]
                cum = jnp.dot(triangles[d], logs, precision=HIGHEST, preferred_element_type=F32)
                cums[h, d, at, :] = cum
                last = cum[ends[d] : ends[d] + 1, :]
                scaled = (keys * jnp.exp(last - cum)).astype(BF16)
                added = dot_0(part(at, 4, h).astype(BF16), scaled)
                adds[h, d, index] = added
                states[h, d] = states[h, d] * jnp.exp(last) + added
                after.append(totals[h * 2 + d] + last)
        return tuple(after)

    nothing = tuple(jnp.zeros((1, LANES), F32) for _ in range(2 * heads))
    sums = lax.fori_loop(0, block_count, first_pass, nothing, unroll=2)
    for h in range(heads):
        for d in range(2):
            state_out[d, h, :LANES, :] = states[h, d].astype(BF16)
            factor = jnp.broadcast_to(jnp.exp(sums[h * 2 + d]), (PAD, LANES))
            coarse = factor.astype(BF16)
            fine = (factor - coarse.astype(F32)).astype(BF16)
            first_row = lax.broadcasted_iota(jnp.int32, (PAD, LANES), 0) == 0
            state_out[d, h, LANES:, :] = jnp.where(first_row, coarse.astype(F32), fine.astype(F32)).astype(BF16)
    state_copies = []
    for peer in peers:
        copy = pltpu.make_async_remote_copy(
            src_ref=state_out.at[jnp.where(peer > mine, 0, 1)],
            dst_ref=state_in.at[mine],
            send_sem=state_send.at[peer],
            recv_sem=state_recv.at[mine],
            device_id={"sp": peer * groups + slot},
        )
        copy.start()
        state_copies.append(copy)

    lane_q = lax.broadcasted_iota(jnp.int32, (tile, LANES), 1)
    tiles = rows // tile
    peak[...] = jnp.full_like(peak, -jnp.inf)
    total[...] = jnp.zeros_like(total)
    mixed[...] = jnp.zeros_like(mixed)

    def attend(block):
        for h in range(heads):
            at = h * LANES

            def one_tile(index, carry):
                q_rows = pl.ds(pl.multiple_of(index * tile, tile), tile)
                queries = rest[q_rows, at : at + LANES]
                zero = jnp.zeros_like(queries)
                both = jnp.concatenate(
                    [jnp.where(lane_q < AK, queries, zero), jnp.where(lane_q < AK, zero, queries)], axis=0
                )
                scores = dot_t(both, kv[block, :, at : at + LANES])
                before = peak[h, index][:, :1]
                raised = jnp.maximum(before, jnp.max(scores, axis=-1, keepdims=True))
                shrink = jnp.exp(before - raised)
                expo = jnp.exp(scores - raised)
                sums_now = total[h, index][:, :1] * shrink + jnp.sum(expo, axis=-1, keepdims=True)
                product = jnp.dot(
                    expo.astype(BF16), kv[block, :, width + at : width + at + LANES], preferred_element_type=F32
                )
                mixed[h, index] = mixed[h, index] * shrink + product
                peak[h, index] = jnp.broadcast_to(raised, (2 * tile, LANES))
                total[h, index] = jnp.broadcast_to(sums_now, (2 * tile, LANES))
                return carry

            lax.fori_loop(0, tiles, one_tile, 0)

    attend(mine)

    def state_arrival(block):
        return pltpu.make_async_remote_copy(
            src_ref=state_out.at[0],
            dst_ref=state_in.at[block],
            send_sem=state_send.at[block],
            recv_sem=state_recv.at[block],
            device_id={"sp": block * groups + slot},
        )

    states[...] = jnp.zeros_like(states)

    def compose(d):
        def body(step, carry):
            block = step if d == 0 else blocks - 1 - step
            state_arrival(block).wait_recv()
            for h in range(heads):
                rows_last = state_in[block, h, LANES:, :].astype(F32)
                factor = rows_last[0:1] + rows_last[1:2]
                states[h, d] = states[h, d] * factor + state_in[block, h, :LANES, :].astype(F32)
            return carry

        return body

    lax.fori_loop(0, mine, compose(0), 0)
    lax.fori_loop(0, blocks - 1 - mine, compose(1), 0)

    def second_pass(step, carry):
        for h in range(heads):
            for d in range(2):
                index, at = rows_of(d, step)
                queries = jax.nn.silu(part(at, 1, h))
                keys = keys_of(at, d, h)
                cum = cums[h, d, at, :]
                middle = cum[middles[d] : middles[d] + 1, :]
                last = cum[ends[d] : ends[d] + 1, :]
                scores = dot_t(
                    (queries * jnp.exp(cum - middle)).astype(BF16), (keys * jnp.exp(middle - cum)).astype(BF16)
                )
                scores = jnp.where(earlier[d], scores, 0.0)
                within = jnp.dot(scores.astype(BF16), part(at, 4, h).astype(BF16), preferred_element_type=F32)
                before = states[h, d]
                carried = dot_t_state(queries * jnp.exp(cum), before)
                span = slice(h * LANES, (h + 1) * LANES)
                rec_sum[at, span] = rec_sum[at, span] + within + carried
                states[h, d] = before * jnp.exp(last) + adds[h, d, index]
        return carry

    def dot_t_state(reads, state):
        return dot_t(reads.astype(BF16), state.astype(BF16))

    lax.fori_loop(0, block_count, second_pass, 0, unroll=2)

    for h in range(heads):
        span = slice(h * LANES, (h + 1) * LANES)
        stage[:, span] = rms_scale(rec_sum[:, span], rec_gain[...]).astype(BF16)

    def hand_over(which, owner):
        dp, dt, p, t = owner
        columns = slice(which * width, (which + 1) * width)
        source = stage.at[pl.ds(pl.multiple_of(p * length + t * piece, piece), piece), columns]
        target = out.at[mesh_column, slot, :, columns]
        if dp == 0 and dt == 0:
            return pltpu.make_async_copy(source, target, out_send.at[which, dp, dt])
        return pltpu.make_async_remote_copy(
            src_ref=source,
            dst_ref=target,
            send_sem=out_send.at[which, dp, dt],
            recv_sem=out_recv.at[which, mesh_column, slot],
            device_id={"sp": mine * groups + p, "tp": t},
        )

    def taken_over(which, owner):
        dp, dt, p, t = owner
        columns = slice(which * width, (which + 1) * width)
        target = out.at[t, p, :, columns]
        return pltpu.make_async_remote_copy(
            src_ref=target,
            dst_ref=target,
            send_sem=out_send.at[which, dp, dt],
            recv_sem=out_recv.at[which, t, p],
            device_id={"sp": mine * groups + p, "tp": t},
        )

    for owner in owners:
        hand_over(0, owner).start()

    def next_block(turn, carry):
        near = lax.div(turn + 1, 2)
        away = jnp.where(lax.rem(turn, 2) == 1, near, blocks - near)
        block = lax.rem(mine + away, blocks)
        for piece in range(groups):
            arrival(block, piece).wait_recv()
        attend(block)
        return carry

    lax.fori_loop(1, blocks, next_block, 0)

    for h in range(heads):
        span = slice(width + h * LANES, width + (h + 1) * LANES)
        for index in range(tiles):
            ratio = mixed[h, index] / total[h, index][:, :1]
            values = ratio[:tile] - lam[h] * ratio[tile:]
            stage[index * tile : (index + 1) * tile, span] = rms_scale(values, att_gain[...]).astype(BF16)
    for owner in owners:
        hand_over(1, owner).start()

    for copy in own_copies + other_copies + state_copies:
        copy.wait_send()
    if groups > 1:
        swap_kv.wait_send()
        swap_rest.wait_send()
    for which in range(2):
        hand_over(which, owners[0]).wait()
        for owner in owners[1:]:
            hand_over(which, owner).wait_send()
            taken_over(which, owner).wait_recv()


def on_device_general(
    tokens, norm_gain, rec_query, fwd_gate, bwd_gate, rec_value, gate_leak, log_decay, rec_gain,
    att_query, att_key, att_value, lambdas, att_gain, out_rec, out_att,
):
    ranks = lax.axis_size("sp")
    tp = lax.axis_size("tp")
    local_heads = rec_query.shape[1] // HK
    groups = 2 if local_heads % 2 == 0 and ranks % 2 == 0 else 1
    heads = local_heads // groups
    width = heads * LANES
    slot = lax.axis_index("sp") % groups

    order = (att_key, att_value, att_query, rec_query, fwd_gate, bwd_gate, rec_value)
    length = tokens.shape[0] * tp
    vmem = pl.BlockSpec(memory_space=pltpu.VMEM)
    dma = pltpu.SemaphoreType.DMA
    projected = pl.pallas_call(
        functools.partial(gather_kernel, tp),
        out_shape=[jax.ShapeDtypeStruct((length, weight.shape[1]), BF16) for weight in order],
        in_specs=[vmem] * (2 + len(order)),
        out_specs=[vmem] * len(order),
        scratch_shapes=[
            pltpu.VMEM((length, tokens.shape[1]), BF16),
            dma((tp,)),
            dma((tp // 2,)),
            dma((tp,)),
        ],
        compiler_params=pltpu.CompilerParams(
            collective_id=1, has_side_effects=True, vmem_limit_bytes=40 * 1024 * 1024
        ),
        cost_estimate=pl.CostEstimate(flops=4 * 10**9, bytes_accessed=10**7, transcendentals=0),
    )(tokens, norm_gain.reshape(1, -1), *order)

    positions = (lax.axis_index("sp") * length + jnp.arange(length, dtype=jnp.int32)).astype(F32)
    frequency = THETA ** (-(jnp.arange(AK // 2, dtype=F32) * 2.0 / AK))
    angles = jnp.tile(positions[:, None] * frequency[None, :], (1, LANES // (AK // 2)))
    cosine, sine = jnp.cos(angles), jnp.sin(angles)

    by_head = log_decay.reshape(2, length, groups, heads).transpose(2, 1, 0, 3).reshape(groups, length, 2 * heads)
    own_decay = lax.dynamic_index_in_dim(by_head, slot, 0, keepdims=False)
    if groups > 1:
        swapped = lax.ppermute(
            lax.dynamic_index_in_dim(by_head, groups - 1 - slot, 0, keepdims=False),
            "sp",
            [(i, i + 1 - 2 * (i % 2)) for i in range(ranks)],
        )
        decay = jnp.where(
            slot == 0, jnp.concatenate([own_decay, swapped]), jnp.concatenate([swapped, own_decay])
        )
    else:
        decay = own_decay
    leak = lax.dynamic_index_in_dim(
        gate_leak.reshape(2, groups, heads, HK).transpose(1, 2, 0, 3), slot, 0, keepdims=False
    )
    lam = lax.dynamic_index_in_dim(lambdas.reshape(groups, heads), slot, 0, keepdims=False)
    lam = jnp.broadcast_to(lam[:, None, None], (heads, 1, LANES))

    blocks = ranks // groups
    rows = groups * length
    tile = min(256, length)
    mixers = pl.pallas_call(
        functools.partial(mixer_kernel, ranks, tp, groups, heads, tile),
        out_shape=jax.ShapeDtypeStruct((tp, groups, length // tp, 2 * width), BF16),
        in_specs=[vmem] * 14,
        out_specs=vmem,
        scratch_shapes=[
            pltpu.VMEM((blocks, rows, 2 * width), BF16),
            pltpu.VMEM((rows, 5 * width), BF16),
            pltpu.VMEM((length, 7 * width), BF16),
            pltpu.VMEM((rows, 2 * width), BF16),
            pltpu.VMEM((2, heads, LANES + PAD, LANES), BF16),
            pltpu.VMEM((blocks, heads, LANES + PAD, LANES), BF16),
            pltpu.VMEM((heads, 2, rows, LANES), F32),
            pltpu.VMEM((heads, 2, rows // BLOCK, LANES, LANES), F32),
            pltpu.VMEM((heads, 2, LANES, LANES), F32),
            pltpu.VMEM((rows, width), F32),
            pltpu.VMEM((heads, rows // tile, 2 * tile, LANES), F32),
            pltpu.VMEM((heads, rows // tile, 2 * tile, LANES), F32),
            pltpu.VMEM((heads, rows // tile, 2 * tile, LANES), F32),
            dma((blocks, groups)),
            dma((blocks, groups)),
            dma((2,)),
            dma,
            dma((blocks,)),
            dma((blocks,)),
            dma((2, groups, tp)),
            dma((2, tp, groups)),
        ],
        compiler_params=pltpu.CompilerParams(
            collective_id=0, has_side_effects=True, vmem_limit_bytes=56 * 1024 * 1024
        ),
        cost_estimate=pl.CostEstimate(flops=10**10, bytes_accessed=10**7, transcendentals=10**7),
    )(*projected, cosine, sine, leak, decay, lam, rec_gain.reshape(1, LANES), att_gain.reshape(1, LANES))

    shares = mixers.reshape(tp, groups, length // tp, 2, heads, LANES)
    both = shares.transpose(2, 3, 0, 1, 4, 5).reshape(length // tp, 2, -1)
    result = jnp.dot(both[:, 0], out_rec, preferred_element_type=F32) + jnp.dot(
        both[:, 1], out_att, preferred_element_type=F32
    )
    return result.astype(BF16)


def fused_kernel(
    ranks, tp, heads, planes,
    tokens_in, norm_in, w_key, w_value, w_query, w_rq, w_fwd, w_bwd, w_rv, leak_in, decay_in, rec_gain_in,
    lam_in, att_gain_in, out_rec_in, out_att_in, rotary_in,
    out,
    tokens, gain, weights, leak, decay, decay_rows, rec_gain, lam, att_gain, w_out, rotary,
    held, cosine, sine, lam_own, lam_pair, stage_kv, stage_q, kv, query, recp, cum_reads, facts, adds, rec_sum,
    state, fade, pair_out, pair_in, plane_out, plane_in, plane_sum, next_out, next_in, before_block,
    rec_stage, rec_all, score_a, score_b, top_a, top_b, acc, peak, att_stage, att_all, total,
    up, down, in_sem, across_send, across_recv, core_send, core_recv, lam_send, lam_recv,
    kv_send, kv_recv, q_send, q_recv, side_send, side_recv, near_send, near_recv,
    pair_send, pair_recv, plane_send, plane_recv, next_send, next_recv,
    rec_send, rec_recv, att_send, att_recv,
):
    sp = lax.axis_index("sp")
    me = lax.axis_index("tp")
    x = lax.rem(sp, 2)
    z = lax.div(sp, 2)
    core = lax.rem(me, 2)
    y = lax.div(me, 2)
    piece = tokens.shape[0]
    half = piece // 2
    length = piece * tp
    width = heads * LANES
    partner = {"tp": y * 2 + 1 - core}
    opposite = {"tp": (1 - y) * 2 + core}
    beside = {"sp": z * 2 + 1 - x}

    small = (
        (rotary_in, rotary), (lam_in, lam), (leak_in, leak), (decay_in, decay),
        (rec_gain_in, rec_gain), (att_gain_in, att_gain),
    )
    inputs = (w_key, w_value, w_query, w_rq, w_fwd, w_bwd, w_rv)
    moves = (
        [(tokens_in, tokens), (norm_in, gain)]
        + [(a, weights.at[i]) for i, a in enumerate(inputs)]
        + list(small) + [(out_rec_in, w_out.at[0]), (out_att_in, w_out.at[1])]
    )
    slots = (0, 1, 2, 3, 4, 5, 5, 5, 5, 6, 7, 8, 9, 10, 11, 12, 12)
    fetches = [pltpu.make_async_copy(a, b, in_sem.at[i]) for i, (a, b) in zip(slots, moves)]
    f_rotary, f_lam, f_leak, f_decay, f_rec_gain, f_att_gain = fetches[9:15]
    for fetch in fetches[:2] + fetches[9:11]:
        fetch.start()

    barrier = pltpu.get_barrier_semaphore()
    above = {"sp": sp + 2}
    below = {"sp": sp - 2}
    for to in (partner, opposite, {"tp": (1 - y) * 2 + 1 - core}, beside):
        pl.semaphore_signal(barrier, inc=1, device_id=to)

    @pl.when(z > 0)
    def _():
        pl.semaphore_signal(barrier, inc=1, device_id=below)

    @pl.when(z < planes - 1)
    def _():
        pl.semaphore_signal(barrier, inc=1, device_id=above)

    neighbours = 4 + lax.div(z + planes - 2, planes - 1) + lax.div(2 * planes - 3 - z, planes - 1)

    def hop(turn):
        for toward, signal, source in ((above, up, 0), (below, down, planes - 1)):

            @pl.when(z == (turn if source == 0 else source - turn))
            def _():
                if turn:
                    pl.semaphore_wait(signal, 1)
                if turn < planes - 1:
                    pl.semaphore_signal(signal, inc=1, device_id=toward)

    def remote(source, target, send, recv, to):
        return pltpu.make_async_remote_copy(
            src_ref=source, dst_ref=target, send_sem=send, recv_sem=recv, device_id=to
        )

    def held_at(owner, part, side):
        return owner * 2 * piece + part * piece + side * half

    def held_rows(owner, part, side):
        return held.at[pl.ds(pl.multiple_of(held_at(owner, part, side), half), half)]

    def across(part, owner):
        rows = held_rows(owner, part, core)
        return remote(rows, rows, across_send, across_recv.at[part], opposite)

    def to_core(owner, part, side, slot):
        rows = held_rows(owner, part, side)
        return remote(rows, rows, core_send, core_recv.at[slot], partner)

    fetches[0].wait()
    fetches[1].wait()
    for fetch in fetches[2:9] + fetches[11:15]:
        fetch.start()
    for part in range(2):
        rows = tokens[part * half : (part + 1) * half, :].astype(F32)
        at = pl.ds(pl.multiple_of(held_at(y, part, core), half), half)
        held[at, :] = rms_scale(rows, gain[...]).astype(BF16)
        if part == 0:
            pl.semaphore_wait(barrier, neighbours)
            hop(0)
        across(part, y).start()
        to_core(y, part, core, part).start()
    f_lam.wait()
    for i in range(heads):
        lam_own[i] = jnp.broadcast_to(lam[:, i : i + 1], (8, LANES))
    lam_copy = remote(lam_own, lam_pair, lam_send, lam_recv, partner)
    lam_copy.start()

    f_rotary.wait()
    lane = lax.broadcasted_iota(jnp.int32, (piece, LANES), 1)
    low_half = lax.rem(lane, AK) < AK // 2
    for t in range(tp):
        begin = 2 * piece + sp * tp + t
        cos_base = rotary[pl.ds(begin, 1), :]
        sin_base = rotary[pl.ds(begin + ranks * tp, 1), :]
        cos_row, sin_row = rotary[:piece, :], rotary[piece : 2 * piece, :]
        turned = sin_base * cos_row + cos_base * sin_row
        cos_here = cos_base * cos_row - sin_base * sin_row
        sin_here = jnp.where(low_half, -turned, turned)
        for part in range(2):
            to = held_at(t // 2, part, t % 2)
            cosine[to : to + half, :] = cos_here[part * half : (part + 1) * half]
            sine[to : to + half, :] = sin_here[part * half : (part + 1) * half]

    hop(1)

    def rotated(wide, cos_at, sin_at):
        rows = wide.shape[0]
        low = jnp.concatenate([low_half] * (rows // piece), axis=0)
        turned = jnp.where(low, pltpu.roll(wide, LANES - AK // 2, 1), pltpu.roll(wide, AK // 2, 1))
        return wide * cos_at + turned * sin_at

    def owner_of(phase):
        return y if phase < 2 else 1 - y

    def plane_copy(phase, i, kind):
        return remote(
            stage_kv.at[phase, i, kind], kv.at[kind, 0, phase, z], kv_send, kv_recv.at[phase, z],
            {"sp": (core * heads + i) * 2 + x, "tp": y * 2 + kind},
        )

    def query_rows(phase, plane):
        return query.at[phase, pl.ds(pl.multiple_of(plane * half, half), half)]

    def query_copy(phase, i, c):
        return remote(
            stage_q.at[phase, i, c], query_rows(phase, z), q_send, q_recv.at[phase],
            {"sp": (core * heads + i) * 2 + x, "tp": y * 2 + c},
        )

    def is_own(i, c):
        return jnp.logical_and(core * heads + i == z, core == c)

    def project(at, index):
        return jnp.dot(held[at, :], weights[index], preferred_element_type=F32)

    def attention_inputs(phases):
        count = len(phases) * piece
        owner = owner_of(phases[0])
        at = pl.ds(pl.multiple_of(held_at(owner, phases[0] % 2, 0), piece), count)
        cos_at, sin_at = cosine[at, :], sine[at, :]
        if phases[0] == 0:
            fetches[2].wait()
        keys = project(at, 0).astype(BF16).astype(F32)
        if phases[0] == 0:
            fetches[3].wait()
        values = project(at, 1).astype(BF16).astype(F32)
        if phases[0] == 0:
            hop(2)
        for i in range(heads):
            span = slice(i * LANES, (i + 1) * LANES)
            value = values[:, span].T.astype(BF16)
            key = rotated(keys[:, span], cos_at, sin_at).astype(BF16)
            for n, phase in enumerate(phases):
                part = slice(n * piece, (n + 1) * piece)
                stage_kv[phase, i, 0] = value[:, part]
                stage_kv[phase, i, 1] = key[part]
        if phases[0] == 0:
            hop(3)
        for phase in phases:
            send_each(phase, plane_copy, kv_recv.at[phase, z], lambda i, c: (stage_kv.at[phase, i, c], kv.at[c, 0, phase, z]))
        if phases[0] == 0:
            fetches[4].wait()
        queries = project(at, 2).astype(BF16).astype(F32)
        for i in range(heads):
            span = slice(i * LANES, (i + 1) * LANES)
            turned = (rotated(queries[:, span], cos_at, sin_at) * AK ** (-0.5)).astype(BF16)
            for n, phase in enumerate(phases):
                for c in range(2):
                    stage_q[phase, i, c] = turned[n * piece + c * half : n * piece + (c + 1) * half]
        for phase in phases:
            send_each(phase, query_copy, q_recv.at[phase], lambda i, c: (stage_q.at[phase, i, c], query_rows(phase, z)))

    def send_each(phase, copy, recv, local):
        for i in range(heads):
            for c in range(2):
                own = is_own(i, c)

                @pl.when(own)
                def _():
                    source, target = local(i, c)
                    pltpu.make_async_copy(source, target, recv).start()

                @pl.when(jnp.logical_not(own))
                def _():
                    copy(phase, i, c).start()

    def recurrence_inputs(owner, wait):
        at = pl.ds(pl.multiple_of(held_at(owner, 0, 0), 2 * piece), 2 * piece)
        if wait:
            pltpu.make_async_copy(weights.at[3:7], weights.at[3:7], in_sem.at[5]).wait()
        for i in range(4):
            recp[i, at, :] = project(at, 3 + i).astype(BF16)

    def plane_at(k):
        return (z, z + 1 - 2 * lax.rem(z, 2), lax.rem(z + 2, planes), planes - 1 - z)[k]

    def mine_of(origin, phase, plane):
        return kv.at[core, origin, phase, plane]

    def to_side(phase, plane):
        return remote(
            mine_of(0, phase, plane), mine_of(1, phase, plane),
            side_send, side_recv.at[phase, plane], beside,
        )

    def to_near(origin, phase, plane):
        block = mine_of(origin, phase, plane)
        return remote(
            block, block, near_send, near_recv.at[phase, origin], partner
        )

    def relay_plane(phase, k):
        plane = plane_at(k)
        block = mine_of(0, phase, plane)
        remote(block, block, near_send, kv_recv.at[phase, plane], partner).wait_recv()
        to_side(phase, plane).start()
        to_near(0, phase, plane).start()

    def relay_side(phase, k):
        plane = plane_at(k)
        block = mine_of(1, phase, plane)
        remote(block, block, side_send, side_recv.at[phase, plane], beside).wait_recv()
        to_near(1, phase, plane).start()

    def settle(phase, origin):
        blocks_in = kv.at[1 - core, origin, phase]
        remote(blocks_in, blocks_in, near_send, near_recv.at[phase, origin], partner).wait_recv()

    def settle_queries(phase):
        rows = query.at[phase]
        remote(rows, rows, q_send, q_recv.at[phase], partner).wait_recv()

    row_at = lax.broadcasted_iota(jnp.int32, (BLOCK, 3 * BLOCK), 0)
    col_at = lax.rem(lax.broadcasted_iota(jnp.int32, (BLOCK, 3 * BLOCK), 1), BLOCK)
    triangles = (jnp.where(row_at >= col_at, 1.0, 0.0).astype(BF16), jnp.where(row_at <= col_at, 1.0, 0.0).astype(BF16))
    row_in = lax.broadcasted_iota(jnp.int32, (BLOCK, BLOCK), 0)
    col_in = lax.broadcasted_iota(jnp.int32, (BLOCK, BLOCK), 1)
    earlier = (row_in >= col_in, row_in <= col_in)
    ends = (BLOCK - 1, 0)
    middles = (BLOCK // 2 - 1, BLOCK // 2)
    blocks = length // BLOCK
    spans = [slice(h * LANES, (h + 1) * LANES) for h in range(heads)]

    def within_block(b):
        at = pl.ds(pl.multiple_of(b * BLOCK, BLOCK), BLOCK)
        t = lax.div(b, 2)
        stored = held_at(lax.div(t, 2), lax.rem(b, 2), lax.rem(t, 2))
        held_block = pl.ds(pl.multiple_of(stored, BLOCK), BLOCK)
        queries = jax.nn.silu(recp[0, held_block, :].astype(F32))
        values = recp[3, held_block, :]
        scores, tails = [], []
        for d in range(2):
            keys = leak[d : d + 1, :] * jax.nn.sigmoid(-recp[1 + d, held_block, :].astype(F32))
            added = jnp.concatenate(
                [jnp.broadcast_to(decay_rows[at, d * heads + h : d * heads + h + 1], (BLOCK, LANES)) for h in range(heads)],
                axis=1,
            )
            logs = jnp.log1p(-keys) + added
            coarse = logs.astype(BF16)
            rest = logs - coarse.astype(F32)
            fine = rest.astype(BF16)
            finest = (rest - fine.astype(F32)).astype(BF16)
            cum = jnp.dot(
                triangles[d], jnp.concatenate([coarse, fine, finest], axis=0), preferred_element_type=F32
            )
            middle = cum[middles[d] : middles[d] + 1, :]
            last = cum[ends[d] : ends[d] + 1, :]
            reads = (queries * jnp.exp(cum - middle)).astype(BF16)
            writes = (keys * jnp.exp(middle - cum)).astype(BF16)
            tails.append((keys * jnp.exp(last - cum)).astype(BF16))
            carried = (queries * jnp.exp(cum)).astype(BF16)
            facts[b, d] = jnp.broadcast_to(jnp.exp(last), (8, width))
            scores.append([jnp.where(earlier[d], dot_t(reads[:, s], writes[:, s]), 0.0) for s in spans])
            for h in range(heads):
                cum_reads[h, at, d * LANES : (d + 1) * LANES] = carried[:, spans[h]]
        for h in range(heads):
            both = (scores[0][h] + scores[1][h]).astype(BF16)
            rec_sum[at, spans[h]] = jnp.dot(both, values[:, spans[h]], preferred_element_type=F32)
            adds[b, h] = dot_0(
                values[:, spans[h]], jnp.concatenate([tails[0][:, spans[h]], tails[1][:, spans[h]]], axis=1)
            )

    def within_rows(owner, turns):
        count = blocks // 2

        def some(j, carry):
            within_block(owner * count + 2 * j)
            within_block(owner * count + 2 * j + 1)
            return carry

        lax.fori_loop(turns[0], turns[-1] + 1, some, 0)

    def order(d):
        return range(blocks) if d == 0 else range(blocks - 1, -1, -1)

    def half_of(d):
        return slice(d * LANES, (d + 1) * LANES)

    first_row = lax.broadcasted_iota(jnp.int32, (PAD, LANES), 0) == 0

    def pack(target, moved, factor):
        target[:LANES, :] = moved.astype(BF16)
        wide = jnp.broadcast_to(factor, (PAD, LANES))
        coarse = wide.astype(BF16).astype(F32)
        target[LANES:, :] = jnp.where(first_row, coarse, wide - coarse).astype(BF16)

    def unpack(source):
        last = source[LANES:, :].astype(F32)
        return source[:LANES, :].astype(F32), last[0:1] + last[1:2]

    def local_states():
        for h in range(heads):
            for d in range(2):
                moved = jnp.zeros((LANES, LANES), F32)
                factor = jnp.ones((1, LANES), F32)
                for b in order(d):
                    step = facts[b, d, 0:1, spans[h]]
                    moved = moved * step + adds[b, h, :, half_of(d)]
                    factor = factor * step
                state[d, h] = moved
                fade[d, h] = jnp.broadcast_to(factor, (8, LANES))
                pack(pair_out.at[d, h], moved, factor)

    def pair_copies():
        return [
            remote(pair_out.at[d, h], pair_in.at[d, h], pair_send, pair_recv, beside)
            for d, h in ((0, 1 - x), (1, 1 - x), (x, x))
        ]

    def pair_done():
        three = plane_in.at[:3]
        return remote(three, three, pair_send, pair_recv, beside)

    def send_pair():
        for copy in pair_copies():
            copy.start()

    def pair_states():
        pair_done().wait_recv()
        for d in range(2):
            mine, factor = state[d, x], fade[d, x][0:1]
            other, other_factor = unpack(pair_in.at[d, x])
            joined = jnp.where(x == d, mine * other_factor + other, other * factor + mine)
            pack(plane_out.at[d], joined, factor * other_factor)
        for dz in range(1, planes):
            to_plane(lax.rem(z + dz, planes)).start()

    def to_plane(target):
        return remote(
            plane_out.at[jnp.where(target > z, 0, 1)], plane_in.at[z],
            plane_send, plane_recv, {"sp": target * 2 + x},
        )

    def other_planes():
        blocks_in = plane_in.at[: planes - 1]
        return remote(blocks_in, blocks_in, plane_send, plane_recv, partner)

    next_copy = remote(next_out, next_in, next_send, next_recv, beside)

    def plane_states():
        other_planes().wait_recv()
        plane_sum[...] = jnp.zeros_like(plane_sum)

        def fold(d):
            def one(step, carry):
                plane = step if d == 0 else planes - 1 - step
                moved, factor = unpack(plane_in.at[plane])
                plane_sum[d] = plane_sum[d] * factor + moved
                return carry

            return one

        lax.fori_loop(0, z, fold(0), 0)
        lax.fori_loop(0, planes - 1 - z, fold(1), 0)
        next_out[...] = plane_sum[...].astype(BF16)
        next_copy.start()

    def second_pass():
        next_copy.wait_recv()
        for h in range(heads):
            for d in range(2):
                entering = jnp.where(x == h, plane_sum[d], next_in[d].astype(F32))
                other, other_factor = unpack(pair_in.at[d, jnp.where(x == d, x, h)])
                running = jnp.where(x == d, entering, entering * other_factor + other)
                for b in order(d):
                    before_block[b, h, :, half_of(d)] = running.astype(BF16)
                    running = running * facts[b, d, 0:1, spans[h]] + adds[b, h, :, half_of(d)]
            for b in range(blocks):
                at = slice(b * BLOCK, (b + 1) * BLOCK)
                whole = rec_sum[at, spans[h]] + dot_t(cum_reads[h, at, :], before_block[b, h])
                rec_stage[at, spans[h]] = rms_scale(whole, rec_gain[...]).astype(BF16)
        for dt in range(tp):
            rec_copy(dt).start()

    def rec_copy(dt):
        t = lax.rem(me + dt, tp)
        source = rec_stage.at[pl.ds(pl.multiple_of(t * piece, piece), piece)]
        if dt == 0:
            return pltpu.make_async_copy(source, rec_all.at[me], rec_recv)
        return remote(source, rec_all.at[me], rec_send, rec_recv, {"tp": t})

    acc[...] = jnp.zeros_like(acc)
    peak[...] = jnp.full_like(peak, -jnp.inf)
    sub = 2 * piece
    ones = jnp.ones((PAD, sub), BF16)
    low_map = lane < AK
    buffers = ((score_a, top_a), (score_b, top_b))

    def attend_step(made, made_buffer, used, used_buffer):
        if made is not None:
            q_phase, tile, chunk = made
            made_blocks = [(o, f, p) for f, o in chunk for p in range(planes)]
            rows = query[q_phase, tile * piece : (tile + 1) * piece, :]
            none = jnp.zeros_like(rows)
            both = jnp.concatenate([jnp.where(low_map, rows, none), jnp.where(low_map, none, rows)], axis=0)
            top = None
        if used is not None:
            slot = used[0] * 2 + used[1]
            used_blocks = [(o, f, p) for f, o in used[2] for p in range(planes)]
            used_score, used_top = used_buffer
            before = peak[slot][0:1]
            now = jnp.maximum(before, jnp.max(used_top[...], axis=0, keepdims=True))
            mixed = acc[slot] * jnp.exp(before - now)
        made_pairs = len(made_blocks) // 2 if made is not None else 0
        used_pairs = len(used_blocks) // 2 if used is not None else 0
        for u in range(max(made_pairs, used_pairs)):
            at = slice(u * sub, (u + 1) * sub)
            if u < made_pairs:
                keys = jnp.concatenate([kv[(1, *block)] for block in made_blocks[2 * u : 2 * u + 2]], axis=0)
                scores = dot_t(keys, both)
                made_buffer[0][at, :] = scores
                high = jnp.max(scores.reshape(sub // 8, 8, 2 * piece), axis=0)
                top = high if top is None else jnp.maximum(top, high)
            if u < used_pairs:
                expo = jnp.exp(used_score[at, :] - now).astype(BF16)
                values = jnp.concatenate([kv[(0, *block)] for block in used_blocks[2 * u : 2 * u + 2]], axis=1)
                values = jnp.concatenate([values, ones], axis=0)
                mixed = mixed + jnp.dot(values, expo, preferred_element_type=F32)
        if used is not None:
            acc[slot] = mixed
            peak[slot] = jnp.broadcast_to(now, (8, 2 * piece))
        if made is not None:
            made_buffer[1][...] = top

    def att_copy(q_phase, plane):
        owner, part = owner_of(q_phase), q_phase % 2
        return remote(
            att_stage.at[q_phase * planes + plane], att_all.at[y * planes + z, part * half : (part + 1) * half],
            att_send, att_recv,
            {"sp": plane * 2 + x, "tp": owner * 2 + core},
        )

    def finish(q_phase, tile):
        whole = acc[q_phase * 2 + tile]
        ratio = whole[:LANES] / whole[LANES : LANES + 1]
        weight = jnp.where(core == lax.div(z, heads), lam_own[lax.rem(z, heads)], lam_pair[lax.rem(z, heads)])[0:1]
        values = ratio[:, :piece] - weight * ratio[:, piece:]
        scale = lax.rsqrt(jnp.mean(values * values, axis=0, keepdims=True) + EPS)
        rows = ((values * scale).T * att_gain[...]).astype(BF16)
        part = q_phase % 2
        for n in range(2):
            plane = 2 * tile + n
            att_stage[q_phase * planes + plane] = rows[n * half : (n + 1) * half]
            if q_phase < 2:

                @pl.when(plane == z)
                def _():
                    pltpu.make_async_copy(
                        att_stage.at[q_phase * planes + plane],
                        att_all.at[y * planes + z, part * half : (part + 1) * half],
                        att_recv,
                    ).start()

                @pl.when(plane != z)
                def _():
                    att_copy(q_phase, plane).start()
            else:
                att_copy(q_phase, plane).start()

    columns = min(512, out.shape[1])

    def rec_total():
        pltpu.make_async_copy(w_out, w_out, in_sem.at[12]).wait()
        remote(rec_all, rec_all, rec_send, rec_recv, partner).wait_recv()
        rec_rows = jnp.concatenate([rec_all[t] for t in range(tp)], axis=1)
        for n in range(0, out.shape[1], columns):
            total[:, n : n + columns] = jnp.dot(rec_rows, w_out[0, :, n : n + columns], preferred_element_type=F32)

    def run_units(units, before):
        for n in range(len(units) + 1):
            for action in before.get(n, ()):
                action()
            made = units[n] if n < len(units) else None
            used = units[n - 1] if n else None
            attend_step(made, buffers[n % 2], used, buffers[(n + 1) % 2])
            if used is not None and used[2][-1] == (3, 1):
                finish(used[0], used[1])

    def tiles_of(q_phases, chunk):
        return [(q_phase, tile, chunk) for q_phase in q_phases for tile in range(2)]

    def call(f, *args):
        return functools.partial(f, *args)

    def all_of(f, phase, ks):
        return [call(f, phase, k) for k in ks]

    near, far = (0, 1), (2, 3)
    near_keys = [(f, o) for f in near for o in range(2)]
    far_keys = [(f, o) for f in far for o in range(2)]
    every = near + far
    units = tiles_of(every, near_keys) + tiles_of(every, far_keys)
    before = {
        1: [call(relay_plane, 3, 0)],
        2: [call(relay_plane, 3, 1)] + all_of(relay_side, 2, range(1)),
        3: [call(relay_plane, 3, 2)] + all_of(relay_side, 2, range(1, 2)),
        4: [call(settle_queries, 2), call(settle_queries, 3), call(relay_plane, 3, 3)],
        5: all_of(relay_side, 2, range(2, 4)),
        6: all_of(relay_side, 3, range(1)),
        7: all_of(relay_side, 3, range(1, 3)),
        8: all_of(relay_side, 3, range(3, 4)) + [call(settle, f, o) for f, o in far_keys],
        9: [plane_states],
        12: [second_pass],
    }
    before[4].append(pair_states)

    for part in range(2):
        to_core(y, part, 1 - core, part).wait_recv()
    attention_inputs(near)
    for fetch in fetches[15:17]:
        fetch.start()
    recurrence_inputs(y, True)
    for fetch in (f_leak, f_decay, f_rec_gain, f_att_gain):
        fetch.wait()
    by_row = jnp.concatenate([decay[d] for d in range(2)] + [jnp.zeros((LANES - 2 * heads, length), F32)], axis=0)
    decay_rows[...] = by_row.T
    relay_plane(0, 0)
    relay_plane(1, 0)
    within_rows(y, (0, 1))
    relay_plane(0, 1)
    across(0, 1 - y).wait_recv()
    to_core(1 - y, 0, core, 2).start()
    relay_plane(0, 2)
    to_core(1 - y, 0, 1 - core, 2).wait_recv()
    attention_inputs((2,))
    relay_plane(0, 3)
    relay_side(0, 0)
    relay_plane(1, 1)
    across(1, 1 - y).wait_recv()
    to_core(1 - y, 1, core, 3).start()
    to_core(1 - y, 1, 1 - core, 3).wait_recv()
    attention_inputs((3,))
    relay_plane(1, 2)
    relay_plane(1, 3)
    for k in range(1, 4):
        relay_side(0, k)
    relay_plane(2, 0)
    recurrence_inputs(1 - y, False)
    relay_side(1, 0)
    relay_side(1, 1)
    relay_plane(2, 1)
    within_rows(1 - y, (0,))
    relay_side(1, 2)
    relay_side(1, 3)
    relay_plane(2, 2)
    within_rows(1 - y, (1,))
    relay_plane(2, 3)
    local_states()
    send_pair()
    lam_copy.wait_recv()
    for phase in near:
        for origin in range(2):
            settle(phase, origin)
        settle_queries(phase)
    run_units(units, before)
    rec_total()

    remote(att_all, att_all, att_send, att_recv, partner).wait_recv()
    att_rows = jnp.concatenate([att_all[i] for i in range(2 * planes)], axis=1)
    for n in range(0, out.shape[1], columns):
        out[:, n : n + columns] = (
            total[:, n : n + columns]
            + jnp.dot(att_rows, w_out[1, :, n : n + columns], preferred_element_type=F32)
        ).astype(BF16)

    def sent(ref, sem, recv):
        remote(ref, ref, sem, recv, partner).wait_send()

    sent(held.at[:piece], across_send, core_recv.at[0])
    sent(held.at[: 2 * piece], core_send, core_recv.at[0])
    lam_copy.wait_send()
    is_local = core == lax.div(z, heads)

    @pl.when(is_local)
    def _():
        sent(stage_kv.at[:3], kv_send, near_recv.at[0, 0])
        sent(stage_q.at[:3], q_send, near_recv.at[0, 0])

    @pl.when(jnp.logical_not(is_local))
    def _():
        sent(stage_kv, kv_send, near_recv.at[0, 0])
        sent(stage_q, q_send, near_recv.at[0, 0])

    sent(kv.at[0, 0], side_send, near_recv.at[0, 0])
    sent(kv.at[0], near_send, near_recv.at[0, 0])
    pair_done().wait_send()
    next_copy.wait_send()
    sent(plane_in.at[: planes - 1], plane_send, plane_recv)
    sent(rec_all.at[: tp - 1], rec_send, rec_recv)
    sent(att_stage.at[: 4 * planes - 2], att_send, att_recv)


def rotary_table(piece, pieces):
    frequency = THETA ** (-(np.arange(LANES) % (AK // 2)) * 2.0 / AK)
    inside = np.arange(piece)[:, None] * frequency[None, :]
    base = (np.arange(pieces) * piece)[:, None] * frequency[None, :]
    return np.concatenate([np.cos(inside), np.sin(inside), np.cos(base), np.sin(base)]).astype(np.float32)


def on_device(
    tokens, norm_gain, rec_query, fwd_gate, bwd_gate, rec_value, gate_leak, log_decay, rec_gain,
    att_query, att_key, att_value, lambdas, att_gain, out_rec, out_att,
):
    ranks = lax.axis_size("sp")
    tp = lax.axis_size("tp")
    heads = rec_query.shape[1] // HK
    planes = ranks // 2
    piece, model = tokens.shape
    if tp != 4 or planes != 2 * heads or planes != 4 or piece != LANES:
        return on_device_general(
            tokens, norm_gain, rec_query, fwd_gate, bwd_gate, rec_value, gate_leak, log_decay, rec_gain,
            att_query, att_key, att_value, lambdas, att_gain, out_rec, out_att,
        )
    length = piece * tp
    width = heads * LANES
    blocks = length // BLOCK
    keys = 4 * planes * piece
    anywhere = pl.BlockSpec(memory_space=pl.ANY)
    dma = pltpu.SemaphoreType.DMA
    vmem = pltpu.VMEM
    table = jnp.asarray(rotary_table(piece, ranks * tp))
    return pl.pallas_call(
        functools.partial(fused_kernel, ranks, tp, heads, planes),
        out_shape=jax.ShapeDtypeStruct((piece, model), BF16),
        in_specs=[anywhere] * 17,
        out_specs=pl.BlockSpec(memory_space=pltpu.VMEM),
        scratch_shapes=[
            vmem((piece, model), BF16),
            vmem((1, model), F32),
            vmem((7, model, width), BF16),
            vmem((2, width), F32),
            vmem((2, heads, length), F32),
            vmem((length, LANES), F32),
            vmem((1, LANES), F32),
            vmem((1, heads), F32),
            vmem((1, LANES), F32),
            vmem((2, *out_rec.shape), BF16),
            vmem(table.shape, F32),
            vmem((length, model), BF16),
            vmem((length, LANES), F32),
            vmem((length, LANES), F32),
            vmem((heads, 8, LANES), F32),
            vmem((heads, 8, LANES), F32),
            vmem((4, heads, 2, piece, LANES), BF16),
            vmem((4, heads, 2, piece // 2, LANES), BF16),
            vmem((2, 2, 4, planes, piece, LANES), BF16),
            vmem((4, planes * piece // 2, LANES), BF16),
            vmem((4, length, width), BF16),
            vmem((heads, length, 2 * LANES), BF16),
            vmem((blocks, 2, 8, width), F32),
            vmem((blocks, heads, LANES, 2 * LANES), F32),
            vmem((length, width), F32),
            vmem((2, heads, LANES, LANES), F32),
            vmem((2, heads, 8, LANES), F32),
            vmem((2, heads, LANES + PAD, LANES), BF16),
            vmem((2, heads, LANES + PAD, LANES), BF16),
            vmem((2, LANES + PAD, LANES), BF16),
            vmem((planes, LANES + PAD, LANES), BF16),
            vmem((2, LANES, LANES), F32),
            vmem((2, LANES, LANES), BF16),
            vmem((2, LANES, LANES), BF16),
            vmem((blocks, heads, LANES, 2 * LANES), BF16),
            vmem((length, width), BF16),
            vmem((tp, piece, width), BF16),
            vmem((keys, 2 * piece), F32),
            vmem((keys, 2 * piece), F32),
            vmem((8, 2 * piece), F32),
            vmem((8, 2 * piece), F32),
            vmem((2 * planes, LANES + PAD, 2 * piece), F32),
            vmem((2 * planes, 8, 2 * piece), F32),
            vmem((4 * planes, piece // 2, LANES), BF16),
            vmem((2 * planes, piece, LANES), BF16),
            vmem((piece, model), F32),
            pltpu.SemaphoreType.REGULAR, pltpu.SemaphoreType.REGULAR,
            dma((13,)), dma, dma((2,)), dma, dma((4,)), dma, dma,
            dma, dma((4, planes)), dma, dma((4,)),
            dma, dma((4, planes)), dma, dma((4, 2)),
            dma, dma, dma, dma, dma, dma,
            dma, dma, dma, dma,
        ],
        compiler_params=pltpu.CompilerParams(
            collective_id=2, has_side_effects=True, vmem_limit_bytes=60 * 1024 * 1024
        ),
        cost_estimate=pl.CostEstimate(flops=10**10, bytes_accessed=10**7, transcendentals=10**7),
    )(
        tokens, norm_gain.reshape(1, -1), att_key, att_value, att_query, rec_query, fwd_gate, bwd_gate, rec_value,
        gate_leak, log_decay.transpose(0, 2, 1), rec_gain.reshape(1, LANES), lambdas.reshape(1, heads), att_gain.reshape(1, LANES),
        out_rec, out_att, table,
    )


def solution(mesh):
    placed = (
        P(("sp", "tp"), None), P(), P(None, "tp"), P(None, "tp"), P(None, "tp"), P(None, "tp"),
        P(None, "tp"), P(None, "sp", "tp"), P(), P(None, "tp"), P(None, "tp"), P(None, "tp"),
        P("tp"), P(), P(), P(),
    )
    return jax.shard_map(
        on_device, mesh=mesh, in_specs=placed, out_specs=P(("sp", "tp"), None), check_vma=False
    )
```

```python
import functools

import jax
import jax.numpy as jnp
import numpy as np
from jax import lax
from jax.experimental import pallas as pl
from jax.experimental.pallas import tpu as pltpu
from jax.sharding import PartitionSpec as P

HK = 128
AK = 64
BLOCK = 64
LANES = 128
EPS = 1e-06
THETA = 500000.0
HIGHEST = lax.Precision.HIGHEST
F32 = jnp.float32
BF16 = jnp.bfloat16
PAD = 16


def rms_scale(values, gain):
    return values * lax.rsqrt(jnp.mean(values * values, axis=-1, keepdims=True) + EPS) * gain


def dot_t(a, b):
    return lax.dot_general(a, b, (((1,), (1,)), ((), ())), preferred_element_type=F32)


def dot_0(a, b):
    return lax.dot_general(a, b, (((0,), (0,)), ((), ())), preferred_element_type=F32)


def gather_kernel(tp, tokens, gain, *refs):
    weights, outs = refs[:7], refs[7:14]
    held, across, along, landed = refs[14:]
    me = lax.axis_index("tp")
    core = lax.rem(me, 2)
    pair = lax.div(me, 2)
    pairs = tp // 2
    count = tokens.shape[0]
    partner = pair * 2 + 1 - core
    others = [lax.rem(pair + k, pairs) for k in range(1, pairs)]
    barrier = pltpu.get_barrier_semaphore()
    pl.semaphore_signal(barrier, inc=1, device_id={"tp": partner})
    for q in others:
        pl.semaphore_signal(barrier, inc=1, device_id={"tp": q * 2 + core})

    def rows_at(block):
        return held.at[pl.ds(pl.multiple_of(block * count, count), count)]

    def to_partner(block):
        return pltpu.make_async_remote_copy(
            src_ref=rows_at(block),
            dst_ref=rows_at(block),
            send_sem=across.at[block],
            recv_sem=landed.at[block],
            device_id={"tp": partner},
        )

    def to_pair(q):
        return pltpu.make_async_remote_copy(
            src_ref=rows_at(me),
            dst_ref=rows_at(me),
            send_sem=along.at[q],
            recv_sem=landed.at[me],
            device_id={"tp": q * 2 + core},
        )

    normed = rms_scale(tokens[...].astype(F32), gain[...]).astype(BF16)
    held[pl.ds(pl.multiple_of(me * count, count), count), :] = normed
    pl.semaphore_wait(barrier, pairs)
    for q in others:
        to_pair(q).start()
    to_partner(me).start()

    def step(k, carry):
        q = lax.rem(pair + k, pairs)
        near = q * 2 + core

        @pl.when(k > 0)
        def _():
            to_partner(near).wait_recv()
            to_partner(near).start()

        to_partner(q * 2 + 1 - core).wait_recv()
        at = pl.ds(pl.multiple_of(q * 2 * count, 2 * count), 2 * count)
        for weight, result in zip(weights, outs):
            result[at, :] = jnp.dot(held[at, :], weight[...], preferred_element_type=F32).astype(BF16)
        return carry

    lax.fori_loop(0, pairs, step, 0)
    to_partner(me).wait_send()
    for q in others:
        to_pair(q).wait_send()
        to_partner(q * 2 + core).wait_send()


def mixer_kernel(
    ranks, tp, groups, heads, tile,
    proj_k, proj_v, proj_q, proj_rq, proj_fwd, proj_bwd, proj_rv, cosine, sine, leak, decay, lam, rec_gain, att_gain,
    out,
    kv, rest, swap, stage, state_out, state_in, cums, adds, states, rec_sum, peak, total, mixed,
    kv_send, kv_recv, swap_send, rest_recv, state_send, state_recv, out_send, out_recv,
):
    me = lax.axis_index("sp")
    slot = lax.rem(me, groups)
    mine = lax.div(me, groups)
    mesh_column = lax.axis_index("tp")
    length = proj_k.shape[0]
    piece = length // tp
    rows = groups * length
    width = heads * LANES
    block_count = rows // BLOCK
    partner_slot = groups - 1 - slot
    partner = mine * groups + partner_slot
    blocks = ranks // groups
    own_rows = pl.ds(pl.multiple_of(slot * length, length), length)
    other_rows = pl.ds(pl.multiple_of(partner_slot * length, length), length)

    barrier = pltpu.get_barrier_semaphore()
    peers = []
    for k in range(1, blocks):
        peers.append(lax.rem(mine + k, blocks))
    for peer in peers:
        pl.semaphore_signal(barrier, inc=1, device_id={"sp": peer * groups + slot})
    owners = []
    for dp in range(groups):
        for dt in range(tp):
            owners.append((dp, dt, lax.rem(slot + dp, groups), lax.rem(mesh_column + dt, tp)))
    for dp, dt, p, t in owners[1:]:
        pl.semaphore_signal(barrier, inc=1, device_id={"sp": mine * groups + p, "tp": t})

    lane = lax.broadcasted_iota(jnp.int32, (length, LANES), 1)
    low_half = lax.rem(lane, AK) < AK // 2

    def rotated(raw):
        wide = raw.astype(F32)
        turned = jnp.where(low_half, -pltpu.roll(wide, LANES - AK // 2, 1), pltpu.roll(wide, AK // 2, 1))
        return wide * cosine[...] + turned * sine[...]

    def prepare(head_group, key_value, others):
        def taken(ref, h):
            return ref[:, pl.ds(pl.multiple_of((head_group * heads + h) * LANES, LANES), LANES)]

        for h in range(heads):
            at = h * LANES
            key_value[:, at : at + LANES] = rotated(taken(proj_k, h)).astype(BF16)
            key_value[:, width + at : width + at + LANES] = taken(proj_v, h)
            others[:, at : at + LANES] = (rotated(taken(proj_q, h)) * AK ** (-0.5)).astype(BF16)
            for i, ref in enumerate((proj_rq, proj_fwd, proj_bwd, proj_rv)):
                others[:, (i + 1) * width + at : (i + 1) * width + at + LANES] = taken(ref, h)

    if groups > 1:
        prepare(partner_slot, swap.at[:, : 2 * width], swap.at[:, 2 * width :])
    prepare(slot, kv.at[mine, own_rows], rest.at[own_rows])
    pl.semaphore_wait(barrier, blocks - 1 + groups * tp - 1)

    def block_copy(source_rows, source_slot, peer):
        return pltpu.make_async_remote_copy(
            src_ref=kv.at[mine, source_rows],
            dst_ref=kv.at[mine, source_rows],
            send_sem=kv_send.at[peer, source_slot],
            recv_sem=kv_recv.at[mine, source_slot],
            device_id={"sp": peer * groups + slot},
        )

    def arrival(block, piece):
        piece_rows = pl.ds(pl.multiple_of(piece * length, length), length)
        return pltpu.make_async_remote_copy(
            src_ref=kv.at[block, piece_rows],
            dst_ref=kv.at[block, piece_rows],
            send_sem=kv_send.at[block, piece],
            recv_sem=kv_recv.at[block, piece],
            device_id={"sp": block * groups + slot},
        )

    if groups > 1:
        swap_kv = pltpu.make_async_remote_copy(
            src_ref=swap.at[:, : 2 * width],
            dst_ref=kv.at[mine, own_rows],
            send_sem=swap_send.at[0],
            recv_sem=kv_recv.at[mine, slot],
            device_id={"sp": partner},
        )
        swap_kv.start()
        swap_rest = pltpu.make_async_remote_copy(
            src_ref=swap.at[:, 2 * width :],
            dst_ref=rest.at[own_rows],
            send_sem=swap_send.at[1],
            recv_sem=rest_recv,
            device_id={"sp": partner},
        )
    own_copies = [block_copy(own_rows, slot, peer) for peer in peers]
    for copy in own_copies:
        copy.start()
    other_copies = []
    if groups > 1:
        swap_rest.start()
        arrival(mine, partner_slot).wait_recv()
        other_copies = [block_copy(other_rows, partner_slot, peer) for peer in peers]
        for copy in other_copies:
            copy.start()
        swap_rest.wait_recv()

    row_at = lax.broadcasted_iota(jnp.int32, (BLOCK, BLOCK), 0)
    col_at = lax.broadcasted_iota(jnp.int32, (BLOCK, BLOCK), 1)
    earlier = (row_at >= col_at, row_at <= col_at)
    triangles = tuple(mask.astype(F32) for mask in earlier)
    ends = (BLOCK - 1, 0)
    middles = (BLOCK // 2 - 1, BLOCK // 2)

    def rows_of(direction, step):
        index = step if direction == 0 else block_count - 1 - step
        return index, pl.ds(pl.multiple_of(index * BLOCK, BLOCK), BLOCK)

    def part(at, index, h):
        return rest[at, (index * heads + h) * LANES : (index * heads + h + 1) * LANES].astype(F32)

    def keys_of(at, direction, h):
        return leak[h, direction : direction + 1, :] * jax.nn.sigmoid(-part(at, 2 + direction, h))

    states[...] = jnp.zeros_like(states)
    rec_sum[...] = jnp.zeros_like(rec_sum)

    def first_pass(step, totals):
        after = []
        for h in range(heads):
            for d in range(2):
                index, at = rows_of(d, step)
                keys = keys_of(at, d, h)
                column = d * heads + h
                logs = jnp.log1p(-keys) + decay[at, column : column + 1]
                cum = jnp.dot(triangles[d], logs, precision=HIGHEST, preferred_element_type=F32)
                cums[h, d, at, :] = cum
                last = cum[ends[d] : ends[d] + 1, :]
                scaled = (keys * jnp.exp(last - cum)).astype(BF16)
                added = dot_0(part(at, 4, h).astype(BF16), scaled)
                adds[h, d, index] = added
                states[h, d] = states[h, d] * jnp.exp(last) + added
                after.append(totals[h * 2 + d] + last)
        return tuple(after)

    nothing = tuple(jnp.zeros((1, LANES), F32) for _ in range(2 * heads))
    sums = lax.fori_loop(0, block_count, first_pass, nothing, unroll=2)
    for h in range(heads):
        for d in range(2):
            state_out[d, h, :LANES, :] = states[h, d].astype(BF16)
            factor = jnp.broadcast_to(jnp.exp(sums[h * 2 + d]), (PAD, LANES))
            coarse = factor.astype(BF16)
            fine = (factor - coarse.astype(F32)).astype(BF16)
            first_row = lax.broadcasted_iota(jnp.int32, (PAD, LANES), 0) == 0
            state_out[d, h, LANES:, :] = jnp.where(first_row, coarse.astype(F32), fine.astype(F32)).astype(BF16)
    state_copies = []
    for peer in peers:
        copy = pltpu.make_async_remote_copy(
            src_ref=state_out.at[jnp.where(peer > mine, 0, 1)],
            dst_ref=state_in.at[mine],
            send_sem=state_send.at[peer],
            recv_sem=state_recv.at[mine],
            device_id={"sp": peer * groups + slot},
        )
        copy.start()
        state_copies.append(copy)

    lane_q = lax.broadcasted_iota(jnp.int32, (tile, LANES), 1)
    tiles = rows // tile
    peak[...] = jnp.full_like(peak, -jnp.inf)
    total[...] = jnp.zeros_like(total)
    mixed[...] = jnp.zeros_like(mixed)

    def attend(block):
        for h in range(heads):
            at = h * LANES

            def one_tile(index, carry):
                q_rows = pl.ds(pl.multiple_of(index * tile, tile), tile)
                queries = rest[q_rows, at : at + LANES]
                zero = jnp.zeros_like(queries)
                both = jnp.concatenate(
                    [jnp.where(lane_q < AK, queries, zero), jnp.where(lane_q < AK, zero, queries)], axis=0
                )
                scores = dot_t(both, kv[block, :, at : at + LANES])
                before = peak[h, index][:, :1]
                raised = jnp.maximum(before, jnp.max(scores, axis=-1, keepdims=True))
                shrink = jnp.exp(before - raised)
                expo = jnp.exp(scores - raised)
                sums_now = total[h, index][:, :1] * shrink + jnp.sum(expo, axis=-1, keepdims=True)
                product = jnp.dot(
                    expo.astype(BF16), kv[block, :, width + at : width + at + LANES], preferred_element_type=F32
                )
                mixed[h, index] = mixed[h, index] * shrink + product
                peak[h, index] = jnp.broadcast_to(raised, (2 * tile, LANES))
                total[h, index] = jnp.broadcast_to(sums_now, (2 * tile, LANES))
                return carry

            lax.fori_loop(0, tiles, one_tile, 0)

    attend(mine)

    def state_arrival(block):
        return pltpu.make_async_remote_copy(
            src_ref=state_out.at[0],
            dst_ref=state_in.at[block],
            send_sem=state_send.at[block],
            recv_sem=state_recv.at[block],
            device_id={"sp": block * groups + slot},
        )

    states[...] = jnp.zeros_like(states)

    def compose(d):
        def body(step, carry):
            block = step if d == 0 else blocks - 1 - step
            state_arrival(block).wait_recv()
            for h in range(heads):
                rows_last = state_in[block, h, LANES:, :].astype(F32)
                factor = rows_last[0:1] + rows_last[1:2]
                states[h, d] = states[h, d] * factor + state_in[block, h, :LANES, :].astype(F32)
            return carry

        return body

    lax.fori_loop(0, mine, compose(0), 0)
    lax.fori_loop(0, blocks - 1 - mine, compose(1), 0)

    def second_pass(step, carry):
        for h in range(heads):
            for d in range(2):
                index, at = rows_of(d, step)
                queries = jax.nn.silu(part(at, 1, h))
                keys = keys_of(at, d, h)
                cum = cums[h, d, at, :]
                middle = cum[middles[d] : middles[d] + 1, :]
                last = cum[ends[d] : ends[d] + 1, :]
                scores = dot_t(
                    (queries * jnp.exp(cum - middle)).astype(BF16), (keys * jnp.exp(middle - cum)).astype(BF16)
                )
                scores = jnp.where(earlier[d], scores, 0.0)
                within = jnp.dot(scores.astype(BF16), part(at, 4, h).astype(BF16), preferred_element_type=F32)
                before = states[h, d]
                carried = dot_t_state(queries * jnp.exp(cum), before)
                span = slice(h * LANES, (h + 1) * LANES)
                rec_sum[at, span] = rec_sum[at, span] + within + carried
                states[h, d] = before * jnp.exp(last) + adds[h, d, index]
        return carry

    def dot_t_state(reads, state):
        return dot_t(reads.astype(BF16), state.astype(BF16))

    lax.fori_loop(0, block_count, second_pass, 0, unroll=2)

    for h in range(heads):
        span = slice(h * LANES, (h + 1) * LANES)
        stage[:, span] = rms_scale(rec_sum[:, span], rec_gain[...]).astype(BF16)

    def hand_over(which, owner):
        dp, dt, p, t = owner
        columns = slice(which * width, (which + 1) * width)
        source = stage.at[pl.ds(pl.multiple_of(p * length + t * piece, piece), piece), columns]
        target = out.at[mesh_column, slot, :, columns]
        if dp == 0 and dt == 0:
            return pltpu.make_async_copy(source, target, out_send.at[which, dp, dt])
        return pltpu.make_async_remote_copy(
            src_ref=source,
            dst_ref=target,
            send_sem=out_send.at[which, dp, dt],
            recv_sem=out_recv.at[which, mesh_column, slot],
            device_id={"sp": mine * groups + p, "tp": t},
        )

    def taken_over(which, owner):
        dp, dt, p, t = owner
        columns = slice(which * width, (which + 1) * width)
        target = out.at[t, p, :, columns]
        return pltpu.make_async_remote_copy(
            src_ref=target,
            dst_ref=target,
            send_sem=out_send.at[which, dp, dt],
            recv_sem=out_recv.at[which, t, p],
            device_id={"sp": mine * groups + p, "tp": t},
        )

    for owner in owners:
        hand_over(0, owner).start()

    def next_block(turn, carry):
        near = lax.div(turn + 1, 2)
        away = jnp.where(lax.rem(turn, 2) == 1, near, blocks - near)
        block = lax.rem(mine + away, blocks)
        for piece in range(groups):
            arrival(block, piece).wait_recv()
        attend(block)
        return carry

    lax.fori_loop(1, blocks, next_block, 0)

    for h in range(heads):
        span = slice(width + h * LANES, width + (h + 1) * LANES)
        for index in range(tiles):
            ratio = mixed[h, index] / total[h, index][:, :1]
            values = ratio[:tile] - lam[h] * ratio[tile:]
            stage[index * tile : (index + 1) * tile, span] = rms_scale(values, att_gain[...]).astype(BF16)
    for owner in owners:
        hand_over(1, owner).start()

    for copy in own_copies + other_copies + state_copies:
        copy.wait_send()
    if groups > 1:
        swap_kv.wait_send()
        swap_rest.wait_send()
    for which in range(2):
        hand_over(which, owners[0]).wait()
        for owner in owners[1:]:
            hand_over(which, owner).wait_send()
            taken_over(which, owner).wait_recv()


def on_device_general(
    tokens, norm_gain, rec_query, fwd_gate, bwd_gate, rec_value, gate_leak, log_decay, rec_gain,
    att_query, att_key, att_value, lambdas, att_gain, out_rec, out_att,
):
    ranks = lax.axis_size("sp")
    tp = lax.axis_size("tp")
    local_heads = rec_query.shape[1] // HK
    groups = 2 if local_heads % 2 == 0 and ranks % 2 == 0 else 1
    heads = local_heads // groups
    width = heads * LANES
    slot = lax.axis_index("sp") % groups

    order = (att_key, att_value, att_query, rec_query, fwd_gate, bwd_gate, rec_value)
    length = tokens.shape[0] * tp
    vmem = pl.BlockSpec(memory_space=pltpu.VMEM)
    dma = pltpu.SemaphoreType.DMA
    projected = pl.pallas_call(
        functools.partial(gather_kernel, tp),
        out_shape=[jax.ShapeDtypeStruct((length, weight.shape[1]), BF16) for weight in order],
        in_specs=[vmem] * (2 + len(order)),
        out_specs=[vmem] * len(order),
        scratch_shapes=[
            pltpu.VMEM((length, tokens.shape[1]), BF16),
            dma((tp,)),
            dma((tp // 2,)),
            dma((tp,)),
        ],
        compiler_params=pltpu.CompilerParams(
            collective_id=1, has_side_effects=True, vmem_limit_bytes=40 * 1024 * 1024
        ),
        cost_estimate=pl.CostEstimate(flops=4 * 10**9, bytes_accessed=10**7, transcendentals=0),
    )(tokens, norm_gain.reshape(1, -1), *order)

    positions = (lax.axis_index("sp") * length + jnp.arange(length, dtype=jnp.int32)).astype(F32)
    frequency = THETA ** (-(jnp.arange(AK // 2, dtype=F32) * 2.0 / AK))
    angles = jnp.tile(positions[:, None] * frequency[None, :], (1, LANES // (AK // 2)))
    cosine, sine = jnp.cos(angles), jnp.sin(angles)

    by_head = log_decay.reshape(2, length, groups, heads).transpose(2, 1, 0, 3).reshape(groups, length, 2 * heads)
    own_decay = lax.dynamic_index_in_dim(by_head, slot, 0, keepdims=False)
    if groups > 1:
        swapped = lax.ppermute(
            lax.dynamic_index_in_dim(by_head, groups - 1 - slot, 0, keepdims=False),
            "sp",
            [(i, i + 1 - 2 * (i % 2)) for i in range(ranks)],
        )
        decay = jnp.where(
            slot == 0, jnp.concatenate([own_decay, swapped]), jnp.concatenate([swapped, own_decay])
        )
    else:
        decay = own_decay
    leak = lax.dynamic_index_in_dim(
        gate_leak.reshape(2, groups, heads, HK).transpose(1, 2, 0, 3), slot, 0, keepdims=False
    )
    lam = lax.dynamic_index_in_dim(lambdas.reshape(groups, heads), slot, 0, keepdims=False)
    lam = jnp.broadcast_to(lam[:, None, None], (heads, 1, LANES))

    blocks = ranks // groups
    rows = groups * length
    tile = min(256, length)
    mixers = pl.pallas_call(
        functools.partial(mixer_kernel, ranks, tp, groups, heads, tile),
        out_shape=jax.ShapeDtypeStruct((tp, groups, length // tp, 2 * width), BF16),
        in_specs=[vmem] * 14,
        out_specs=vmem,
        scratch_shapes=[
            pltpu.VMEM((blocks, rows, 2 * width), BF16),
            pltpu.VMEM((rows, 5 * width), BF16),
            pltpu.VMEM((length, 7 * width), BF16),
            pltpu.VMEM((rows, 2 * width), BF16),
            pltpu.VMEM((2, heads, LANES + PAD, LANES), BF16),
            pltpu.VMEM((blocks, heads, LANES + PAD, LANES), BF16),
            pltpu.VMEM((heads, 2, rows, LANES), F32),
            pltpu.VMEM((heads, 2, rows // BLOCK, LANES, LANES), F32),
            pltpu.VMEM((heads, 2, LANES, LANES), F32),
            pltpu.VMEM((rows, width), F32),
            pltpu.VMEM((heads, rows // tile, 2 * tile, LANES), F32),
            pltpu.VMEM((heads, rows // tile, 2 * tile, LANES), F32),
            pltpu.VMEM((heads, rows // tile, 2 * tile, LANES), F32),
            dma((blocks, groups)),
            dma((blocks, groups)),
            dma((2,)),
            dma,
            dma((blocks,)),
            dma((blocks,)),
            dma((2, groups, tp)),
            dma((2, tp, groups)),
        ],
        compiler_params=pltpu.CompilerParams(
            collective_id=0, has_side_effects=True, vmem_limit_bytes=56 * 1024 * 1024
        ),
        cost_estimate=pl.CostEstimate(flops=10**10, bytes_accessed=10**7, transcendentals=10**7),
    )(*projected, cosine, sine, leak, decay, lam, rec_gain.reshape(1, LANES), att_gain.reshape(1, LANES))

    shares = mixers.reshape(tp, groups, length // tp, 2, heads, LANES)
    both = shares.transpose(2, 3, 0, 1, 4, 5).reshape(length // tp, 2, -1)
    result = jnp.dot(both[:, 0], out_rec, preferred_element_type=F32) + jnp.dot(
        both[:, 1], out_att, preferred_element_type=F32
    )
    return result.astype(BF16)


def fused_kernel(
    ranks, tp, heads, planes,
    tokens_in, norm_in, w_key, w_value, w_query, w_rq, w_fwd, w_bwd, w_rv, leak_in, decay_in, rec_gain_in,
    lam_in, att_gain_in, out_rec_in, out_att_in, rotary_in,
    out,
    tokens, gain, weights, leak, decay, decay_rows, rec_gain, lam, att_gain, w_out, rotary,
    held, cosine, sine, lam_own, lam_pair, stage_kv, stage_q, kv, query, recp, cum_reads, facts, adds, rec_sum,
    state, fade, pair_out, pair_in, plane_out, plane_in, plane_sum, next_out, next_in, before_block,
    rec_stage, rec_all, score_a, score_b, top_a, top_b, acc, peak, att_stage, att_all, total,
    up, down, in_sem, across_send, across_recv, core_send, core_recv, lam_send, lam_recv,
    kv_send, kv_recv, q_send, q_recv, side_send, side_recv, near_send, near_recv,
    pair_send, pair_recv, plane_send, plane_recv, next_send, next_recv,
    rec_send, rec_recv, att_send, att_recv,
):
    sp = lax.axis_index("sp")
    me = lax.axis_index("tp")
    x = lax.rem(sp, 2)
    z = lax.div(sp, 2)
    core = lax.rem(me, 2)
    y = lax.div(me, 2)
    piece = tokens.shape[0]
    half = piece // 2
    length = piece * tp
    width = heads * LANES
    partner = {"tp": y * 2 + 1 - core}
    opposite = {"tp": (1 - y) * 2 + core}
    beside = {"sp": z * 2 + 1 - x}

    small = (
        (rotary_in, rotary), (lam_in, lam), (leak_in, leak), (decay_in, decay),
        (rec_gain_in, rec_gain), (att_gain_in, att_gain),
    )
    inputs = (w_key, w_value, w_query, w_rq, w_fwd, w_bwd, w_rv)
    moves = (
        [(tokens_in, tokens), (norm_in, gain)]
        + [(a, weights.at[i]) for i, a in enumerate(inputs)]
        + list(small) + [(out_rec_in, w_out.at[0]), (out_att_in, w_out.at[1])]
    )
    slots = (0, 1, 2, 3, 4, 5, 5, 5, 5, 6, 7, 8, 9, 10, 11, 12, 12)
    fetches = [pltpu.make_async_copy(a, b, in_sem.at[i]) for i, (a, b) in zip(slots, moves)]
    f_rotary, f_lam, f_leak, f_decay, f_rec_gain, f_att_gain = fetches[9:15]
    for fetch in fetches[:2] + fetches[9:11]:
        fetch.start()

    barrier = pltpu.get_barrier_semaphore()
    above = {"sp": sp + 2}
    below = {"sp": sp - 2}
    for to in (partner, opposite, {"tp": (1 - y) * 2 + 1 - core}, beside):
        pl.semaphore_signal(barrier, inc=1, device_id=to)

    @pl.when(z > 0)
    def _():
        pl.semaphore_signal(barrier, inc=1, device_id=below)

    @pl.when(z < planes - 1)
    def _():
        pl.semaphore_signal(barrier, inc=1, device_id=above)

    neighbours = 4 + lax.div(z + planes - 2, planes - 1) + lax.div(2 * planes - 3 - z, planes - 1)

    def hop(turn):
        for toward, signal, source in ((above, up, 0), (below, down, planes - 1)):

            @pl.when(z == (turn if source == 0 else source - turn))
            def _():
                if turn:
                    pl.semaphore_wait(signal, 1)
                if turn < planes - 1:
                    pl.semaphore_signal(signal, inc=1, device_id=toward)

    def remote(source, target, send, recv, to):
        return pltpu.make_async_remote_copy(
            src_ref=source, dst_ref=target, send_sem=send, recv_sem=recv, device_id=to
        )

    def held_at(owner, part, side):
        return owner * 2 * piece + part * piece + side * half

    def held_rows(owner, part, side):
        return held.at[pl.ds(pl.multiple_of(held_at(owner, part, side), half), half)]

    def across(part, owner):
        rows = held_rows(owner, part, core)
        return remote(rows, rows, across_send, across_recv.at[part], opposite)

    def to_core(owner, part, side, slot):
        rows = held_rows(owner, part, side)
        return remote(rows, rows, core_send, core_recv.at[slot], partner)

    fetches[0].wait()
    fetches[1].wait()
    for fetch in fetches[2:9] + fetches[11:15]:
        fetch.start()
    for part in range(2):
        rows = tokens[part * half : (part + 1) * half, :].astype(F32)
        at = pl.ds(pl.multiple_of(held_at(y, part, core), half), half)
        held[at, :] = rms_scale(rows, gain[...]).astype(BF16)
        if part == 0:
            pl.semaphore_wait(barrier, neighbours)
            hop(0)
        across(part, y).start()
        to_core(y, part, core, part).start()
    f_lam.wait()
    for i in range(heads):
        lam_own[i] = jnp.broadcast_to(lam[:, i : i + 1], (8, LANES))
    lam_copy = remote(lam_own, lam_pair, lam_send, lam_recv, partner)
    lam_copy.start()

    f_rotary.wait()
    lane = lax.broadcasted_iota(jnp.int32, (piece, LANES), 1)
    low_half = lax.rem(lane, AK) < AK // 2
    for t in range(tp):
        begin = 2 * piece + sp * tp + t
        cos_base = rotary[pl.ds(begin, 1), :]
        sin_base = rotary[pl.ds(begin + ranks * tp, 1), :]
        cos_row, sin_row = rotary[:piece, :], rotary[piece : 2 * piece, :]
        turned = sin_base * cos_row + cos_base * sin_row
        cos_here = cos_base * cos_row - sin_base * sin_row
        sin_here = jnp.where(low_half, -turned, turned)
        for part in range(2):
            to = held_at(t // 2, part, t % 2)
            cosine[to : to + half, :] = cos_here[part * half : (part + 1) * half]
            sine[to : to + half, :] = sin_here[part * half : (part + 1) * half]

    hop(1)

    def rotated(wide, cos_at, sin_at):
        rows = wide.shape[0]
        low = jnp.concatenate([low_half] * (rows // piece), axis=0)
        turned = jnp.where(low, pltpu.roll(wide, LANES - AK // 2, 1), pltpu.roll(wide, AK // 2, 1))
        return wide * cos_at + turned * sin_at

    def owner_of(phase):
        return y if phase < 2 else 1 - y

    def plane_copy(phase, i, kind):
        return remote(
            stage_kv.at[phase, i, kind], kv.at[kind, 0, phase, z], kv_send, kv_recv.at[phase, z],
            {"sp": (core * heads + i) * 2 + x, "tp": y * 2 + kind},
        )

    def query_rows(phase, plane):
        return query.at[phase, pl.ds(pl.multiple_of(plane * half, half), half)]

    def query_copy(phase, i, c):
        return remote(
            stage_q.at[phase, i, c], query_rows(phase, z), q_send, q_recv.at[phase],
            {"sp": (core * heads + i) * 2 + x, "tp": y * 2 + c},
        )

    def is_own(i, c):
        return jnp.logical_and(core * heads + i == z, core == c)

    def project(at, index):
        return jnp.dot(held[at, :], weights[index], preferred_element_type=F32)

    def attention_inputs(phases):
        count = len(phases) * piece
        owner = owner_of(phases[0])
        at = pl.ds(pl.multiple_of(held_at(owner, phases[0] % 2, 0), piece), count)
        cos_at, sin_at = cosine[at, :], sine[at, :]
        if phases[0] == 0:
            fetches[2].wait()
        keys = project(at, 0).astype(BF16).astype(F32)
        if phases[0] == 0:
            fetches[3].wait()
        values = project(at, 1).astype(BF16).astype(F32)
        if phases[0] == 0:
            hop(2)
        for i in range(heads):
            span = slice(i * LANES, (i + 1) * LANES)
            value = values[:, span].T.astype(BF16)
            key = rotated(keys[:, span], cos_at, sin_at).astype(BF16)
            for n, phase in enumerate(phases):
                part = slice(n * piece, (n + 1) * piece)
                stage_kv[phase, i, 0] = value[:, part]
                stage_kv[phase, i, 1] = key[part]
        if phases[0] == 0:
            hop(3)
        for phase in phases:
            send_each(phase, plane_copy, kv_recv.at[phase, z], lambda i, c: (stage_kv.at[phase, i, c], kv.at[c, 0, phase, z]))
        if phases[0] == 0:
            fetches[4].wait()
        queries = project(at, 2).astype(BF16).astype(F32)
        for i in range(heads):
            span = slice(i * LANES, (i + 1) * LANES)
            turned = (rotated(queries[:, span], cos_at, sin_at) * AK ** (-0.5)).astype(BF16)
            for n, phase in enumerate(phases):
                for c in range(2):
                    stage_q[phase, i, c] = turned[n * piece + c * half : n * piece + (c + 1) * half]
        for phase in phases:
            send_each(phase, query_copy, q_recv.at[phase], lambda i, c: (stage_q.at[phase, i, c], query_rows(phase, z)))

    def send_each(phase, copy, recv, local):
        for i in range(heads):
            for c in range(2):
                own = is_own(i, c)

                @pl.when(own)
                def _():
                    source, target = local(i, c)
                    pltpu.make_async_copy(source, target, recv).start()

                @pl.when(jnp.logical_not(own))
                def _():
                    copy(phase, i, c).start()

    def recurrence_inputs(owner, parts, wait):
        at = pl.ds(pl.multiple_of(held_at(owner, parts[0], 0), piece), len(parts) * piece)
        if wait:
            pltpu.make_async_copy(weights.at[3:7], weights.at[3:7], in_sem.at[5]).wait()
        for i in range(4):
            recp[i, at, :] = project(at, 3 + i).astype(BF16)

    def plane_at(k):
        return (z, z + 1 - 2 * lax.rem(z, 2), lax.rem(z + 2, planes), planes - 1 - z)[k]

    def mine_of(origin, phase, plane):
        return kv.at[core, origin, phase, plane]

    def to_side(phase, plane):
        return remote(
            mine_of(0, phase, plane), mine_of(1, phase, plane),
            side_send, side_recv.at[phase, plane], beside,
        )

    def to_near(origin, phase, plane):
        block = mine_of(origin, phase, plane)
        return remote(
            block, block, near_send, near_recv.at[phase, origin], partner
        )

    def relay_plane(phase, k):
        plane = plane_at(k)
        block = mine_of(0, phase, plane)
        remote(block, block, near_send, kv_recv.at[phase, plane], partner).wait_recv()
        to_side(phase, plane).start()
        to_near(0, phase, plane).start()

    def relay_side(phase, k):
        plane = plane_at(k)
        block = mine_of(1, phase, plane)
        remote(block, block, side_send, side_recv.at[phase, plane], beside).wait_recv()
        to_near(1, phase, plane).start()

    def settle(phase, origin):
        blocks_in = kv.at[1 - core, origin, phase]
        remote(blocks_in, blocks_in, near_send, near_recv.at[phase, origin], partner).wait_recv()

    def settle_queries(phase):
        rows = query.at[phase]
        remote(rows, rows, q_send, q_recv.at[phase], partner).wait_recv()

    row_at = lax.broadcasted_iota(jnp.int32, (BLOCK, 3 * BLOCK), 0)
    col_at = lax.rem(lax.broadcasted_iota(jnp.int32, (BLOCK, 3 * BLOCK), 1), BLOCK)
    triangles = (jnp.where(row_at >= col_at, 1.0, 0.0).astype(BF16), jnp.where(row_at <= col_at, 1.0, 0.0).astype(BF16))
    row_in = lax.broadcasted_iota(jnp.int32, (BLOCK, BLOCK), 0)
    col_in = lax.broadcasted_iota(jnp.int32, (BLOCK, BLOCK), 1)
    earlier = (row_in >= col_in, row_in <= col_in)
    ends = (BLOCK - 1, 0)
    middles = (BLOCK // 2 - 1, BLOCK // 2)
    blocks = length // BLOCK
    spans = [slice(h * LANES, (h + 1) * LANES) for h in range(heads)]

    def within_block(b):
        at = pl.ds(pl.multiple_of(b * BLOCK, BLOCK), BLOCK)
        t = lax.div(b, 2)
        stored = held_at(lax.div(t, 2), lax.rem(b, 2), lax.rem(t, 2))
        held_block = pl.ds(pl.multiple_of(stored, BLOCK), BLOCK)
        queries = jax.nn.silu(recp[0, held_block, :].astype(F32))
        values = recp[3, held_block, :]
        scores, tails = [], []
        for d in range(2):
            keys = leak[d : d + 1, :] * jax.nn.sigmoid(-recp[1 + d, held_block, :].astype(F32))
            added = jnp.concatenate(
                [jnp.broadcast_to(decay_rows[at, d * heads + h : d * heads + h + 1], (BLOCK, LANES)) for h in range(heads)],
                axis=1,
            )
            logs = jnp.log1p(-keys) + added
            coarse = logs.astype(BF16)
            rest = logs - coarse.astype(F32)
            fine = rest.astype(BF16)
            finest = (rest - fine.astype(F32)).astype(BF16)
            cum = jnp.dot(
                triangles[d], jnp.concatenate([coarse, fine, finest], axis=0), preferred_element_type=F32
            )
            middle = cum[middles[d] : middles[d] + 1, :]
            last = cum[ends[d] : ends[d] + 1, :]
            reads = (queries * jnp.exp(cum - middle)).astype(BF16)
            writes = (keys * jnp.exp(middle - cum)).astype(BF16)
            tails.append((keys * jnp.exp(last - cum)).astype(BF16))
            carried = (queries * jnp.exp(cum)).astype(BF16)
            facts[b, d] = jnp.broadcast_to(jnp.exp(last), (8, width))
            scores.append([jnp.where(earlier[d], dot_t(reads[:, s], writes[:, s]), 0.0) for s in spans])
            for h in range(heads):
                cum_reads[h, at, d * LANES : (d + 1) * LANES] = carried[:, spans[h]]
        for h in range(heads):
            both = (scores[0][h] + scores[1][h]).astype(BF16)
            rec_sum[at, spans[h]] = jnp.dot(both, values[:, spans[h]], preferred_element_type=F32)
            adds[b, h] = dot_0(
                values[:, spans[h]], jnp.concatenate([tails[0][:, spans[h]], tails[1][:, spans[h]]], axis=1)
            )

    def within_rows(owner, parts):
        def some(part, carry):
            within_block(owner * 4 + part)
            within_block(owner * 4 + 2 + part)
            return carry

        lax.fori_loop(parts[0], parts[-1] + 1, some, 0)

    def order(d):
        return range(blocks) if d == 0 else range(blocks - 1, -1, -1)

    def half_of(d):
        return slice(d * LANES, (d + 1) * LANES)

    first_row = lax.broadcasted_iota(jnp.int32, (PAD, LANES), 0) == 0

    def pack(target, moved, factor):
        target[:LANES, :] = moved.astype(BF16)
        wide = jnp.broadcast_to(factor, (PAD, LANES))
        coarse = wide.astype(BF16).astype(F32)
        target[LANES:, :] = jnp.where(first_row, coarse, wide - coarse).astype(BF16)

    def unpack(source):
        last = source[LANES:, :].astype(F32)
        return source[:LANES, :].astype(F32), last[0:1] + last[1:2]

    def local_states():
        for h in range(heads):
            for d in range(2):
                moved = jnp.zeros((LANES, LANES), F32)
                factor = jnp.ones((1, LANES), F32)
                for b in order(d):
                    step = facts[b, d, 0:1, spans[h]]
                    moved = moved * step + adds[b, h, :, half_of(d)]
                    factor = factor * step
                state[d, h] = moved
                fade[d, h] = jnp.broadcast_to(factor, (8, LANES))
                pack(pair_out.at[d, h], moved, factor)

    def pair_copies():
        return [
            remote(pair_out.at[d, h], pair_in.at[d, h], pair_send, pair_recv, beside)
            for d, h in ((0, 1 - x), (1, 1 - x), (x, x))
        ]

    def pair_done():
        three = plane_in.at[:3]
        return remote(three, three, pair_send, pair_recv, beside)

    def send_pair():
        for copy in pair_copies():
            copy.start()

    def pair_states():
        pair_done().wait_recv()
        for d in range(2):
            mine, factor = state[d, x], fade[d, x][0:1]
            other, other_factor = unpack(pair_in.at[d, x])
            joined = jnp.where(x == d, mine * other_factor + other, other * factor + mine)
            pack(plane_out.at[d], joined, factor * other_factor)
        for dz in range(1, planes):
            to_plane(lax.rem(z + dz, planes)).start()

    def to_plane(target):
        return remote(
            plane_out.at[jnp.where(target > z, 0, 1)], plane_in.at[z],
            plane_send, plane_recv, {"sp": target * 2 + x},
        )

    def other_planes():
        blocks_in = plane_in.at[: planes - 1]
        return remote(blocks_in, blocks_in, plane_send, plane_recv, partner)

    next_copy = remote(next_out, next_in, next_send, next_recv, beside)

    def plane_states():
        other_planes().wait_recv()
        plane_sum[...] = jnp.zeros_like(plane_sum)

        def fold(d):
            def one(step, carry):
                plane = step if d == 0 else planes - 1 - step
                moved, factor = unpack(plane_in.at[plane])
                plane_sum[d] = plane_sum[d] * factor + moved
                return carry

            return one

        lax.fori_loop(0, z, fold(0), 0)
        lax.fori_loop(0, planes - 1 - z, fold(1), 0)
        next_out[...] = plane_sum[...].astype(BF16)
        next_copy.start()

    def second_pass():
        next_copy.wait_recv()
        for h in range(heads):
            for d in range(2):
                entering = jnp.where(x == h, plane_sum[d], next_in[d].astype(F32))
                other, other_factor = unpack(pair_in.at[d, jnp.where(x == d, x, h)])
                running = jnp.where(x == d, entering, entering * other_factor + other)
                for b in order(d):
                    before_block[b, h, :, half_of(d)] = running.astype(BF16)
                    running = running * facts[b, d, 0:1, spans[h]] + adds[b, h, :, half_of(d)]
            for b in range(blocks):
                at = slice(b * BLOCK, (b + 1) * BLOCK)
                whole = rec_sum[at, spans[h]] + dot_t(cum_reads[h, at, :], before_block[b, h])
                rec_stage[at, spans[h]] = rms_scale(whole, rec_gain[...]).astype(BF16)
        for dt in range(tp):
            rec_copy(dt).start()

    def rec_copy(dt):
        t = lax.rem(me + dt, tp)
        source = rec_stage.at[pl.ds(pl.multiple_of(t * piece, piece), piece)]
        if dt == 0:
            return pltpu.make_async_copy(source, rec_all.at[me], rec_recv)
        return remote(source, rec_all.at[me], rec_send, rec_recv, {"tp": t})

    acc[...] = jnp.zeros_like(acc)
    peak[...] = jnp.full_like(peak, -jnp.inf)
    sub = 2 * piece
    ones = jnp.ones((PAD, sub), BF16)
    low_map = lane < AK
    buffers = ((score_a, top_a), (score_b, top_b))

    def attend_step(made, made_buffer, used, used_buffer):
        if made is not None:
            q_phase, tile, chunk = made
            made_blocks = [(o, f, p) for f, o in chunk for p in range(planes)]
            rows = query[q_phase, pl.ds(tile * piece if isinstance(tile, int) else pl.multiple_of(tile * piece, piece), piece), :]
            none = jnp.zeros_like(rows)
            both = jnp.concatenate([jnp.where(low_map, rows, none), jnp.where(low_map, none, rows)], axis=0)
            top = None
        if used is not None:
            slot = used[0] * 2 + used[1]
            used_blocks = [(o, f, p) for f, o in used[2] for p in range(planes)]
            used_score, used_top = used_buffer
            before = peak[slot][0:1]
            now = jnp.maximum(before, jnp.max(used_top[...], axis=0, keepdims=True))
            mixed = acc[slot] * jnp.exp(before - now)
        made_pairs = len(made_blocks) // 2 if made is not None else 0
        used_pairs = len(used_blocks) // 2 if used is not None else 0
        for u in range(max(made_pairs, used_pairs)):
            at = slice(u * sub, (u + 1) * sub)
            if u < made_pairs:
                keys = jnp.concatenate([kv[(1, *block)] for block in made_blocks[2 * u : 2 * u + 2]], axis=0)
                scores = dot_t(keys, both)
                made_buffer[0][at, :] = scores
                high = jnp.max(scores.reshape(sub // 8, 8, 2 * piece), axis=0)
                top = high if top is None else jnp.maximum(top, high)
            if u < used_pairs:
                expo = jnp.exp(used_score[at, :] - now).astype(BF16)
                values = jnp.concatenate([kv[(0, *block)] for block in used_blocks[2 * u : 2 * u + 2]], axis=1)
                values = jnp.concatenate([values, ones], axis=0)
                mixed = mixed + jnp.dot(values, expo, preferred_element_type=F32)
        if used is not None:
            acc[slot] = mixed
            peak[slot] = jnp.broadcast_to(now, (8, 2 * piece))
        if made is not None:
            made_buffer[1][...] = top

    def att_copy(q_phase, plane):
        owner, part = owner_of(q_phase), q_phase % 2
        return remote(
            att_stage.at[q_phase * planes + plane], att_all.at[y * planes + z, part * half : (part + 1) * half],
            att_send, att_recv,
            {"sp": plane * 2 + x, "tp": owner * 2 + core},
        )

    def finish(q_phase, tile):
        whole = acc[q_phase * 2 + tile]
        ratio = whole[:LANES] / whole[LANES : LANES + 1]
        weight = jnp.where(core == lax.div(z, heads), lam_own[lax.rem(z, heads)], lam_pair[lax.rem(z, heads)])[0:1]
        values = ratio[:, :piece] - weight * ratio[:, piece:]
        scale = lax.rsqrt(jnp.mean(values * values, axis=0, keepdims=True) + EPS)
        rows = ((values * scale).T * att_gain[...]).astype(BF16)
        part = q_phase % 2
        for n in range(2):
            plane = 2 * tile + n
            att_stage[q_phase * planes + plane] = rows[n * half : (n + 1) * half]
            if q_phase < 2:

                @pl.when(plane == z)
                def _():
                    pltpu.make_async_copy(
                        att_stage.at[q_phase * planes + plane],
                        att_all.at[y * planes + z, part * half : (part + 1) * half],
                        att_recv,
                    ).start()

                @pl.when(plane != z)
                def _():
                    att_copy(q_phase, plane).start()
            else:
                att_copy(q_phase, plane).start()

    columns = min(512, out.shape[1])

    def rec_total():
        pltpu.make_async_copy(w_out, w_out, in_sem.at[12]).wait()
        remote(rec_all, rec_all, rec_send, rec_recv, partner).wait_recv()
        rec_rows = jnp.concatenate([rec_all[t] for t in range(tp)], axis=1)
        for n in range(0, out.shape[1], columns):
            total[:, n : n + columns] = jnp.dot(rec_rows, w_out[0, :, n : n + columns], preferred_element_type=F32)

    def run_units(units, before):
        for n in range(len(units) + 1):
            for action in before.get(n, ()):
                action()
            made = units[n] if n < len(units) else None
            used = units[n - 1] if n else None
            attend_step(made, buffers[n % 2], used, buffers[(n + 1) % 2])
            if used is not None and used[2][-1] == (3, 1):
                finish(used[0], used[1])

    def tiles_of(q_phases, chunk):
        return [(q_phase, tile, chunk) for q_phase in q_phases for tile in range(2)]

    def call(f, *args):
        return functools.partial(f, *args)

    def all_of(f, phase, ks):
        return [call(f, phase, k) for k in ks]

    near, far = (0, 1), (2, 3)
    near_keys = [(f, o) for f in near for o in range(2)]
    far_keys = [(f, o) for f in far for o in range(2)]
    every = near + far
    units = tiles_of(every, near_keys)
    side_tile = 1 - lax.div(2 * z, planes)
    for tile in (side_tile, 1 - side_tile):
        units += [(q_phase, tile, far_keys) for q_phase in every]
    before = {
        1: [call(relay_plane, 3, 0)],
        2: [call(relay_plane, 3, 1)] + all_of(relay_side, 2, range(1)),
        3: [call(relay_plane, 3, 2)] + all_of(relay_side, 2, range(1, 2)),
        4: [call(settle_queries, 2), call(settle_queries, 3), call(relay_plane, 3, 3)],
        5: all_of(relay_side, 2, range(2, 4)),
        6: all_of(relay_side, 3, range(1)),
        7: all_of(relay_side, 3, range(1, 3)),
        8: all_of(relay_side, 3, range(3, 4)) + [call(settle, f, o) for f, o in far_keys],
        9: [plane_states],
        12: [second_pass],
    }
    before[4].append(pair_states)

    for part in range(2):
        to_core(y, part, 1 - core, part).wait_recv()
    attention_inputs(near)
    for fetch in fetches[15:17]:
        fetch.start()
    recurrence_inputs(y, (0, 1), True)
    for fetch in (f_leak, f_decay, f_rec_gain, f_att_gain):
        fetch.wait()
    by_row = jnp.concatenate([decay[d] for d in range(2)] + [jnp.zeros((LANES - 2 * heads, length), F32)], axis=0)
    decay_rows[...] = by_row.T
    relay_plane(0, 0)
    relay_plane(1, 0)
    within_rows(y, (0, 1))
    relay_plane(0, 1)
    across(0, 1 - y).wait_recv()
    to_core(1 - y, 0, core, 2).start()
    relay_plane(0, 2)
    to_core(1 - y, 0, 1 - core, 2).wait_recv()
    attention_inputs((2,))
    relay_plane(0, 3)
    relay_side(0, 0)
    relay_plane(1, 1)
    recurrence_inputs(1 - y, (0,), False)
    across(1, 1 - y).wait_recv()
    to_core(1 - y, 1, core, 3).start()
    within_rows(1 - y, (0,))
    relay_plane(1, 2)
    to_core(1 - y, 1, 1 - core, 3).wait_recv()
    attention_inputs((3,))
    relay_plane(1, 3)
    for k in range(1, 4):
        relay_side(0, k)
    relay_plane(2, 0)
    recurrence_inputs(1 - y, (1,), False)
    relay_side(1, 0)
    relay_side(1, 1)
    relay_plane(2, 1)
    within_rows(1 - y, (1,))
    local_states()
    send_pair()
    relay_plane(2, 2)
    relay_plane(2, 3)
    relay_side(1, 2)
    relay_side(1, 3)
    lam_copy.wait_recv()
    for phase in near:
        for origin in range(2):
            settle(phase, origin)
        settle_queries(phase)
    run_units(units, before)
    rec_total()

    remote(att_all, att_all, att_send, att_recv, partner).wait_recv()
    att_rows = jnp.concatenate([att_all[i] for i in range(2 * planes)], axis=1)
    for n in range(0, out.shape[1], columns):
        out[:, n : n + columns] = (
            total[:, n : n + columns]
            + jnp.dot(att_rows, w_out[1, :, n : n + columns], preferred_element_type=F32)
        ).astype(BF16)

    def sent(ref, sem, recv):
        remote(ref, ref, sem, recv, partner).wait_send()

    sent(held.at[:piece], across_send, core_recv.at[0])
    sent(held.at[: 2 * piece], core_send, core_recv.at[0])
    lam_copy.wait_send()
    is_local = core == lax.div(z, heads)

    @pl.when(is_local)
    def _():
        sent(stage_kv.at[:3], kv_send, near_recv.at[0, 0])
        sent(stage_q.at[:3], q_send, near_recv.at[0, 0])

    @pl.when(jnp.logical_not(is_local))
    def _():
        sent(stage_kv, kv_send, near_recv.at[0, 0])
        sent(stage_q, q_send, near_recv.at[0, 0])

    sent(kv.at[0, 0], side_send, near_recv.at[0, 0])
    sent(kv.at[0], near_send, near_recv.at[0, 0])
    pair_done().wait_send()
    next_copy.wait_send()
    sent(plane_in.at[: planes - 1], plane_send, plane_recv)
    sent(rec_all.at[: tp - 1], rec_send, rec_recv)
    sent(att_stage.at[: 4 * planes - 2], att_send, att_recv)


def rotary_table(piece, pieces):
    frequency = THETA ** (-(np.arange(LANES) % (AK // 2)) * 2.0 / AK)
    inside = np.arange(piece)[:, None] * frequency[None, :]
    base = (np.arange(pieces) * piece)[:, None] * frequency[None, :]
    return np.concatenate([np.cos(inside), np.sin(inside), np.cos(base), np.sin(base)]).astype(np.float32)


def on_device(
    tokens, norm_gain, rec_query, fwd_gate, bwd_gate, rec_value, gate_leak, log_decay, rec_gain,
    att_query, att_key, att_value, lambdas, att_gain, out_rec, out_att,
):
    ranks = lax.axis_size("sp")
    tp = lax.axis_size("tp")
    heads = rec_query.shape[1] // HK
    planes = ranks // 2
    piece, model = tokens.shape
    if tp != 4 or planes != 2 * heads or planes != 4 or piece != LANES:
        return on_device_general(
            tokens, norm_gain, rec_query, fwd_gate, bwd_gate, rec_value, gate_leak, log_decay, rec_gain,
            att_query, att_key, att_value, lambdas, att_gain, out_rec, out_att,
        )
    length = piece * tp
    width = heads * LANES
    blocks = length // BLOCK
    keys = 4 * planes * piece
    anywhere = pl.BlockSpec(memory_space=pl.ANY)
    dma = pltpu.SemaphoreType.DMA
    vmem = pltpu.VMEM
    table = jnp.asarray(rotary_table(piece, ranks * tp))
    return pl.pallas_call(
        functools.partial(fused_kernel, ranks, tp, heads, planes),
        out_shape=jax.ShapeDtypeStruct((piece, model), BF16),
        in_specs=[anywhere] * 17,
        out_specs=pl.BlockSpec(memory_space=pltpu.VMEM),
        scratch_shapes=[
            vmem((piece, model), BF16),
            vmem((1, model), F32),
            vmem((7, model, width), BF16),
            vmem((2, width), F32),
            vmem((2, heads, length), F32),
            vmem((length, LANES), F32),
            vmem((1, LANES), F32),
            vmem((1, heads), F32),
            vmem((1, LANES), F32),
            vmem((2, *out_rec.shape), BF16),
            vmem(table.shape, F32),
            vmem((length, model), BF16),
            vmem((length, LANES), F32),
            vmem((length, LANES), F32),
            vmem((heads, 8, LANES), F32),
            vmem((heads, 8, LANES), F32),
            vmem((4, heads, 2, piece, LANES), BF16),
            vmem((4, heads, 2, piece // 2, LANES), BF16),
            vmem((2, 2, 4, planes, piece, LANES), BF16),
            vmem((4, planes * piece // 2, LANES), BF16),
            vmem((4, length, width), BF16),
            vmem((heads, length, 2 * LANES), BF16),
            vmem((blocks, 2, 8, width), F32),
            vmem((blocks, heads, LANES, 2 * LANES), F32),
            vmem((length, width), F32),
            vmem((2, heads, LANES, LANES), F32),
            vmem((2, heads, 8, LANES), F32),
            vmem((2, heads, LANES + PAD, LANES), BF16),
            vmem((2, heads, LANES + PAD, LANES), BF16),
            vmem((2, LANES + PAD, LANES), BF16),
            vmem((planes, LANES + PAD, LANES), BF16),
            vmem((2, LANES, LANES), F32),
            vmem((2, LANES, LANES), BF16),
            vmem((2, LANES, LANES), BF16),
            vmem((blocks, heads, LANES, 2 * LANES), BF16),
            vmem((length, width), BF16),
            vmem((tp, piece, width), BF16),
            vmem((keys, 2 * piece), F32),
            vmem((keys, 2 * piece), F32),
            vmem((8, 2 * piece), F32),
            vmem((8, 2 * piece), F32),
            vmem((2 * planes, LANES + PAD, 2 * piece), F32),
            vmem((2 * planes, 8, 2 * piece), F32),
            vmem((4 * planes, piece // 2, LANES), BF16),
            vmem((2 * planes, piece, LANES), BF16),
            vmem((piece, model), F32),
            pltpu.SemaphoreType.REGULAR, pltpu.SemaphoreType.REGULAR,
            dma((13,)), dma, dma((2,)), dma, dma((4,)), dma, dma,
            dma, dma((4, planes)), dma, dma((4,)),
            dma, dma((4, planes)), dma, dma((4, 2)),
            dma, dma, dma, dma, dma, dma,
            dma, dma, dma, dma,
        ],
        compiler_params=pltpu.CompilerParams(
            collective_id=2, has_side_effects=True, vmem_limit_bytes=60 * 1024 * 1024
        ),
        cost_estimate=pl.CostEstimate(flops=10**10, bytes_accessed=10**7, transcendentals=10**7),
    )(
        tokens, norm_gain.reshape(1, -1), att_key, att_value, att_query, rec_query, fwd_gate, bwd_gate, rec_value,
        gate_leak, log_decay.transpose(0, 2, 1), rec_gain.reshape(1, LANES), lambdas.reshape(1, heads), att_gain.reshape(1, LANES),
        out_rec, out_att, table,
    )


def solution(mesh):
    placed = (
        P(("sp", "tp"), None), P(), P(None, "tp"), P(None, "tp"), P(None, "tp"), P(None, "tp"),
        P(None, "tp"), P(None, "sp", "tp"), P(), P(None, "tp"), P(None, "tp"), P(None, "tp"),
        P("tp"), P(), P(), P(),
    )
    return jax.shard_map(
        on_device, mesh=mesh, in_specs=placed, out_specs=P(("sp", "tp"), None), check_vma=False
    )
```

```python
import functools

import jax
import jax.numpy as jnp
import numpy as np
from jax import lax
from jax.experimental import pallas as pl
from jax.experimental.pallas import tpu as pltpu
from jax.sharding import PartitionSpec as P

HK = 128
AK = 64
BLOCK = 64
LANES = 128
EPS = 1e-06
THETA = 500000.0
HIGHEST = lax.Precision.HIGHEST
F32 = jnp.float32
BF16 = jnp.bfloat16
PAD = 16


def rms_scale(values, gain):
    return values * lax.rsqrt(jnp.mean(values * values, axis=-1, keepdims=True) + EPS) * gain


def dot_t(a, b):
    return lax.dot_general(a, b, (((1,), (1,)), ((), ())), preferred_element_type=F32)


def dot_0(a, b):
    return lax.dot_general(a, b, (((0,), (0,)), ((), ())), preferred_element_type=F32)


def gather_kernel(tp, tokens, gain, *refs):
    weights, outs = refs[:7], refs[7:14]
    held, across, along, landed = refs[14:]
    me = lax.axis_index("tp")
    core = lax.rem(me, 2)
    pair = lax.div(me, 2)
    pairs = tp // 2
    count = tokens.shape[0]
    partner = pair * 2 + 1 - core
    others = [lax.rem(pair + k, pairs) for k in range(1, pairs)]
    barrier = pltpu.get_barrier_semaphore()
    pl.semaphore_signal(barrier, inc=1, device_id={"tp": partner})
    for q in others:
        pl.semaphore_signal(barrier, inc=1, device_id={"tp": q * 2 + core})

    def rows_at(block):
        return held.at[pl.ds(pl.multiple_of(block * count, count), count)]

    def to_partner(block):
        return pltpu.make_async_remote_copy(
            src_ref=rows_at(block),
            dst_ref=rows_at(block),
            send_sem=across.at[block],
            recv_sem=landed.at[block],
            device_id={"tp": partner},
        )

    def to_pair(q):
        return pltpu.make_async_remote_copy(
            src_ref=rows_at(me),
            dst_ref=rows_at(me),
            send_sem=along.at[q],
            recv_sem=landed.at[me],
            device_id={"tp": q * 2 + core},
        )

    normed = rms_scale(tokens[...].astype(F32), gain[...]).astype(BF16)
    held[pl.ds(pl.multiple_of(me * count, count), count), :] = normed
    pl.semaphore_wait(barrier, pairs)
    for q in others:
        to_pair(q).start()
    to_partner(me).start()

    def step(k, carry):
        q = lax.rem(pair + k, pairs)
        near = q * 2 + core

        @pl.when(k > 0)
        def _():
            to_partner(near).wait_recv()
            to_partner(near).start()

        to_partner(q * 2 + 1 - core).wait_recv()
        at = pl.ds(pl.multiple_of(q * 2 * count, 2 * count), 2 * count)
        for weight, result in zip(weights, outs):
            result[at, :] = jnp.dot(held[at, :], weight[...], preferred_element_type=F32).astype(BF16)
        return carry

    lax.fori_loop(0, pairs, step, 0)
    to_partner(me).wait_send()
    for q in others:
        to_pair(q).wait_send()
        to_partner(q * 2 + core).wait_send()


def mixer_kernel(
    ranks, tp, groups, heads, tile,
    proj_k, proj_v, proj_q, proj_rq, proj_fwd, proj_bwd, proj_rv, cosine, sine, leak, decay, lam, rec_gain, att_gain,
    out,
    kv, rest, swap, stage, state_out, state_in, cums, adds, states, rec_sum, peak, total, mixed,
    kv_send, kv_recv, swap_send, rest_recv, state_send, state_recv, out_send, out_recv,
):
    me = lax.axis_index("sp")
    slot = lax.rem(me, groups)
    mine = lax.div(me, groups)
    mesh_column = lax.axis_index("tp")
    length = proj_k.shape[0]
    piece = length // tp
    rows = groups * length
    width = heads * LANES
    block_count = rows // BLOCK
    partner_slot = groups - 1 - slot
    partner = mine * groups + partner_slot
    blocks = ranks // groups
    own_rows = pl.ds(pl.multiple_of(slot * length, length), length)
    other_rows = pl.ds(pl.multiple_of(partner_slot * length, length), length)

    barrier = pltpu.get_barrier_semaphore()
    peers = []
    for k in range(1, blocks):
        peers.append(lax.rem(mine + k, blocks))
    for peer in peers:
        pl.semaphore_signal(barrier, inc=1, device_id={"sp": peer * groups + slot})
    owners = []
    for dp in range(groups):
        for dt in range(tp):
            owners.append((dp, dt, lax.rem(slot + dp, groups), lax.rem(mesh_column + dt, tp)))
    for dp, dt, p, t in owners[1:]:
        pl.semaphore_signal(barrier, inc=1, device_id={"sp": mine * groups + p, "tp": t})

    lane = lax.broadcasted_iota(jnp.int32, (length, LANES), 1)
    low_half = lax.rem(lane, AK) < AK // 2

    def rotated(raw):
        wide = raw.astype(F32)
        turned = jnp.where(low_half, -pltpu.roll(wide, LANES - AK // 2, 1), pltpu.roll(wide, AK // 2, 1))
        return wide * cosine[...] + turned * sine[...]

    def prepare(head_group, key_value, others):
        def taken(ref, h):
            return ref[:, pl.ds(pl.multiple_of((head_group * heads + h) * LANES, LANES), LANES)]

        for h in range(heads):
            at = h * LANES
            key_value[:, at : at + LANES] = rotated(taken(proj_k, h)).astype(BF16)
            key_value[:, width + at : width + at + LANES] = taken(proj_v, h)
            others[:, at : at + LANES] = (rotated(taken(proj_q, h)) * AK ** (-0.5)).astype(BF16)
            for i, ref in enumerate((proj_rq, proj_fwd, proj_bwd, proj_rv)):
                others[:, (i + 1) * width + at : (i + 1) * width + at + LANES] = taken(ref, h)

    if groups > 1:
        prepare(partner_slot, swap.at[:, : 2 * width], swap.at[:, 2 * width :])
    prepare(slot, kv.at[mine, own_rows], rest.at[own_rows])
    pl.semaphore_wait(barrier, blocks - 1 + groups * tp - 1)

    def block_copy(source_rows, source_slot, peer):
        return pltpu.make_async_remote_copy(
            src_ref=kv.at[mine, source_rows],
            dst_ref=kv.at[mine, source_rows],
            send_sem=kv_send.at[peer, source_slot],
            recv_sem=kv_recv.at[mine, source_slot],
            device_id={"sp": peer * groups + slot},
        )

    def arrival(block, piece):
        piece_rows = pl.ds(pl.multiple_of(piece * length, length), length)
        return pltpu.make_async_remote_copy(
            src_ref=kv.at[block, piece_rows],
            dst_ref=kv.at[block, piece_rows],
            send_sem=kv_send.at[block, piece],
            recv_sem=kv_recv.at[block, piece],
            device_id={"sp": block * groups + slot},
        )

    if groups > 1:
        swap_kv = pltpu.make_async_remote_copy(
            src_ref=swap.at[:, : 2 * width],
            dst_ref=kv.at[mine, own_rows],
            send_sem=swap_send.at[0],
            recv_sem=kv_recv.at[mine, slot],
            device_id={"sp": partner},
        )
        swap_kv.start()
        swap_rest = pltpu.make_async_remote_copy(
            src_ref=swap.at[:, 2 * width :],
            dst_ref=rest.at[own_rows],
            send_sem=swap_send.at[1],
            recv_sem=rest_recv,
            device_id={"sp": partner},
        )
    own_copies = [block_copy(own_rows, slot, peer) for peer in peers]
    for copy in own_copies:
        copy.start()
    other_copies = []
    if groups > 1:
        swap_rest.start()
        arrival(mine, partner_slot).wait_recv()
        other_copies = [block_copy(other_rows, partner_slot, peer) for peer in peers]
        for copy in other_copies:
            copy.start()
        swap_rest.wait_recv()

    row_at = lax.broadcasted_iota(jnp.int32, (BLOCK, BLOCK), 0)
    col_at = lax.broadcasted_iota(jnp.int32, (BLOCK, BLOCK), 1)
    earlier = (row_at >= col_at, row_at <= col_at)
    triangles = tuple(mask.astype(F32) for mask in earlier)
    ends = (BLOCK - 1, 0)
    middles = (BLOCK // 2 - 1, BLOCK // 2)

    def rows_of(direction, step):
        index = step if direction == 0 else block_count - 1 - step
        return index, pl.ds(pl.multiple_of(index * BLOCK, BLOCK), BLOCK)

    def part(at, index, h):
        return rest[at, (index * heads + h) * LANES : (index * heads + h + 1) * LANES].astype(F32)

    def keys_of(at, direction, h):
        return leak[h, direction : direction + 1, :] * jax.nn.sigmoid(-part(at, 2 + direction, h))

    states[...] = jnp.zeros_like(states)
    rec_sum[...] = jnp.zeros_like(rec_sum)

    def first_pass(step, totals):
        after = []
        for h in range(heads):
            for d in range(2):
                index, at = rows_of(d, step)
                keys = keys_of(at, d, h)
                column = d * heads + h
                logs = jnp.log1p(-keys) + decay[at, column : column + 1]
                cum = jnp.dot(triangles[d], logs, precision=HIGHEST, preferred_element_type=F32)
                cums[h, d, at, :] = cum
                last = cum[ends[d] : ends[d] + 1, :]
                scaled = (keys * jnp.exp(last - cum)).astype(BF16)
                added = dot_0(part(at, 4, h).astype(BF16), scaled)
                adds[h, d, index] = added
                states[h, d] = states[h, d] * jnp.exp(last) + added
                after.append(totals[h * 2 + d] + last)
        return tuple(after)

    nothing = tuple(jnp.zeros((1, LANES), F32) for _ in range(2 * heads))
    sums = lax.fori_loop(0, block_count, first_pass, nothing, unroll=2)
    for h in range(heads):
        for d in range(2):
            state_out[d, h, :LANES, :] = states[h, d].astype(BF16)
            factor = jnp.broadcast_to(jnp.exp(sums[h * 2 + d]), (PAD, LANES))
            coarse = factor.astype(BF16)
            fine = (factor - coarse.astype(F32)).astype(BF16)
            first_row = lax.broadcasted_iota(jnp.int32, (PAD, LANES), 0) == 0
            state_out[d, h, LANES:, :] = jnp.where(first_row, coarse.astype(F32), fine.astype(F32)).astype(BF16)
    state_copies = []
    for peer in peers:
        copy = pltpu.make_async_remote_copy(
            src_ref=state_out.at[jnp.where(peer > mine, 0, 1)],
            dst_ref=state_in.at[mine],
            send_sem=state_send.at[peer],
            recv_sem=state_recv.at[mine],
            device_id={"sp": peer * groups + slot},
        )
        copy.start()
        state_copies.append(copy)

    lane_q = lax.broadcasted_iota(jnp.int32, (tile, LANES), 1)
    tiles = rows // tile
    peak[...] = jnp.full_like(peak, -jnp.inf)
    total[...] = jnp.zeros_like(total)
    mixed[...] = jnp.zeros_like(mixed)

    def attend(block):
        for h in range(heads):
            at = h * LANES

            def one_tile(index, carry):
                q_rows = pl.ds(pl.multiple_of(index * tile, tile), tile)
                queries = rest[q_rows, at : at + LANES]
                zero = jnp.zeros_like(queries)
                both = jnp.concatenate(
                    [jnp.where(lane_q < AK, queries, zero), jnp.where(lane_q < AK, zero, queries)], axis=0
                )
                scores = dot_t(both, kv[block, :, at : at + LANES])
                before = peak[h, index][:, :1]
                raised = jnp.maximum(before, jnp.max(scores, axis=-1, keepdims=True))
                shrink = jnp.exp(before - raised)
                expo = jnp.exp(scores - raised)
                sums_now = total[h, index][:, :1] * shrink + jnp.sum(expo, axis=-1, keepdims=True)
                product = jnp.dot(
                    expo.astype(BF16), kv[block, :, width + at : width + at + LANES], preferred_element_type=F32
                )
                mixed[h, index] = mixed[h, index] * shrink + product
                peak[h, index] = jnp.broadcast_to(raised, (2 * tile, LANES))
                total[h, index] = jnp.broadcast_to(sums_now, (2 * tile, LANES))
                return carry

            lax.fori_loop(0, tiles, one_tile, 0)

    attend(mine)

    def state_arrival(block):
        return pltpu.make_async_remote_copy(
            src_ref=state_out.at[0],
            dst_ref=state_in.at[block],
            send_sem=state_send.at[block],
            recv_sem=state_recv.at[block],
            device_id={"sp": block * groups + slot},
        )

    states[...] = jnp.zeros_like(states)

    def compose(d):
        def body(step, carry):
            block = step if d == 0 else blocks - 1 - step
            state_arrival(block).wait_recv()
            for h in range(heads):
                rows_last = state_in[block, h, LANES:, :].astype(F32)
                factor = rows_last[0:1] + rows_last[1:2]
                states[h, d] = states[h, d] * factor + state_in[block, h, :LANES, :].astype(F32)
            return carry

        return body

    lax.fori_loop(0, mine, compose(0), 0)
    lax.fori_loop(0, blocks - 1 - mine, compose(1), 0)

    def second_pass(step, carry):
        for h in range(heads):
            for d in range(2):
                index, at = rows_of(d, step)
                queries = jax.nn.silu(part(at, 1, h))
                keys = keys_of(at, d, h)
                cum = cums[h, d, at, :]
                middle = cum[middles[d] : middles[d] + 1, :]
                last = cum[ends[d] : ends[d] + 1, :]
                scores = dot_t(
                    (queries * jnp.exp(cum - middle)).astype(BF16), (keys * jnp.exp(middle - cum)).astype(BF16)
                )
                scores = jnp.where(earlier[d], scores, 0.0)
                within = jnp.dot(scores.astype(BF16), part(at, 4, h).astype(BF16), preferred_element_type=F32)
                before = states[h, d]
                carried = dot_t_state(queries * jnp.exp(cum), before)
                span = slice(h * LANES, (h + 1) * LANES)
                rec_sum[at, span] = rec_sum[at, span] + within + carried
                states[h, d] = before * jnp.exp(last) + adds[h, d, index]
        return carry

    def dot_t_state(reads, state):
        return dot_t(reads.astype(BF16), state.astype(BF16))

    lax.fori_loop(0, block_count, second_pass, 0, unroll=2)

    for h in range(heads):
        span = slice(h * LANES, (h + 1) * LANES)
        stage[:, span] = rms_scale(rec_sum[:, span], rec_gain[...]).astype(BF16)

    def hand_over(which, owner):
        dp, dt, p, t = owner
        columns = slice(which * width, (which + 1) * width)
        source = stage.at[pl.ds(pl.multiple_of(p * length + t * piece, piece), piece), columns]
        target = out.at[mesh_column, slot, :, columns]
        if dp == 0 and dt == 0:
            return pltpu.make_async_copy(source, target, out_send.at[which, dp, dt])
        return pltpu.make_async_remote_copy(
            src_ref=source,
            dst_ref=target,
            send_sem=out_send.at[which, dp, dt],
            recv_sem=out_recv.at[which, mesh_column, slot],
            device_id={"sp": mine * groups + p, "tp": t},
        )

    def taken_over(which, owner):
        dp, dt, p, t = owner
        columns = slice(which * width, (which + 1) * width)
        target = out.at[t, p, :, columns]
        return pltpu.make_async_remote_copy(
            src_ref=target,
            dst_ref=target,
            send_sem=out_send.at[which, dp, dt],
            recv_sem=out_recv.at[which, t, p],
            device_id={"sp": mine * groups + p, "tp": t},
        )

    for owner in owners:
        hand_over(0, owner).start()

    def next_block(turn, carry):
        near = lax.div(turn + 1, 2)
        away = jnp.where(lax.rem(turn, 2) == 1, near, blocks - near)
        block = lax.rem(mine + away, blocks)
        for piece in range(groups):
            arrival(block, piece).wait_recv()
        attend(block)
        return carry

    lax.fori_loop(1, blocks, next_block, 0)

    for h in range(heads):
        span = slice(width + h * LANES, width + (h + 1) * LANES)
        for index in range(tiles):
            ratio = mixed[h, index] / total[h, index][:, :1]
            values = ratio[:tile] - lam[h] * ratio[tile:]
            stage[index * tile : (index + 1) * tile, span] = rms_scale(values, att_gain[...]).astype(BF16)
    for owner in owners:
        hand_over(1, owner).start()

    for copy in own_copies + other_copies + state_copies:
        copy.wait_send()
    if groups > 1:
        swap_kv.wait_send()
        swap_rest.wait_send()
    for which in range(2):
        hand_over(which, owners[0]).wait()
        for owner in owners[1:]:
            hand_over(which, owner).wait_send()
            taken_over(which, owner).wait_recv()


def on_device_general(
    tokens, norm_gain, rec_query, fwd_gate, bwd_gate, rec_value, gate_leak, log_decay, rec_gain,
    att_query, att_key, att_value, lambdas, att_gain, out_rec, out_att,
):
    ranks = lax.axis_size("sp")
    tp = lax.axis_size("tp")
    local_heads = rec_query.shape[1] // HK
    groups = 2 if local_heads % 2 == 0 and ranks % 2 == 0 else 1
    heads = local_heads // groups
    width = heads * LANES
    slot = lax.axis_index("sp") % groups

    order = (att_key, att_value, att_query, rec_query, fwd_gate, bwd_gate, rec_value)
    length = tokens.shape[0] * tp
    vmem = pl.BlockSpec(memory_space=pltpu.VMEM)
    dma = pltpu.SemaphoreType.DMA
    projected = pl.pallas_call(
        functools.partial(gather_kernel, tp),
        out_shape=[jax.ShapeDtypeStruct((length, weight.shape[1]), BF16) for weight in order],
        in_specs=[vmem] * (2 + len(order)),
        out_specs=[vmem] * len(order),
        scratch_shapes=[
            pltpu.VMEM((length, tokens.shape[1]), BF16),
            dma((tp,)),
            dma((tp // 2,)),
            dma((tp,)),
        ],
        compiler_params=pltpu.CompilerParams(
            collective_id=1, has_side_effects=True, vmem_limit_bytes=40 * 1024 * 1024
        ),
        cost_estimate=pl.CostEstimate(flops=4 * 10**9, bytes_accessed=10**7, transcendentals=0),
    )(tokens, norm_gain.reshape(1, -1), *order)

    positions = (lax.axis_index("sp") * length + jnp.arange(length, dtype=jnp.int32)).astype(F32)
    frequency = THETA ** (-(jnp.arange(AK // 2, dtype=F32) * 2.0 / AK))
    angles = jnp.tile(positions[:, None] * frequency[None, :], (1, LANES // (AK // 2)))
    cosine, sine = jnp.cos(angles), jnp.sin(angles)

    by_head = log_decay.reshape(2, length, groups, heads).transpose(2, 1, 0, 3).reshape(groups, length, 2 * heads)
    own_decay = lax.dynamic_index_in_dim(by_head, slot, 0, keepdims=False)
    if groups > 1:
        swapped = lax.ppermute(
            lax.dynamic_index_in_dim(by_head, groups - 1 - slot, 0, keepdims=False),
            "sp",
            [(i, i + 1 - 2 * (i % 2)) for i in range(ranks)],
        )
        decay = jnp.where(
            slot == 0, jnp.concatenate([own_decay, swapped]), jnp.concatenate([swapped, own_decay])
        )
    else:
        decay = own_decay
    leak = lax.dynamic_index_in_dim(
        gate_leak.reshape(2, groups, heads, HK).transpose(1, 2, 0, 3), slot, 0, keepdims=False
    )
    lam = lax.dynamic_index_in_dim(lambdas.reshape(groups, heads), slot, 0, keepdims=False)
    lam = jnp.broadcast_to(lam[:, None, None], (heads, 1, LANES))

    blocks = ranks // groups
    rows = groups * length
    tile = min(256, length)
    mixers = pl.pallas_call(
        functools.partial(mixer_kernel, ranks, tp, groups, heads, tile),
        out_shape=jax.ShapeDtypeStruct((tp, groups, length // tp, 2 * width), BF16),
        in_specs=[vmem] * 14,
        out_specs=vmem,
        scratch_shapes=[
            pltpu.VMEM((blocks, rows, 2 * width), BF16),
            pltpu.VMEM((rows, 5 * width), BF16),
            pltpu.VMEM((length, 7 * width), BF16),
            pltpu.VMEM((rows, 2 * width), BF16),
            pltpu.VMEM((2, heads, LANES + PAD, LANES), BF16),
            pltpu.VMEM((blocks, heads, LANES + PAD, LANES), BF16),
            pltpu.VMEM((heads, 2, rows, LANES), F32),
            pltpu.VMEM((heads, 2, rows // BLOCK, LANES, LANES), F32),
            pltpu.VMEM((heads, 2, LANES, LANES), F32),
            pltpu.VMEM((rows, width), F32),
            pltpu.VMEM((heads, rows // tile, 2 * tile, LANES), F32),
            pltpu.VMEM((heads, rows // tile, 2 * tile, LANES), F32),
            pltpu.VMEM((heads, rows // tile, 2 * tile, LANES), F32),
            dma((blocks, groups)),
            dma((blocks, groups)),
            dma((2,)),
            dma,
            dma((blocks,)),
            dma((blocks,)),
            dma((2, groups, tp)),
            dma((2, tp, groups)),
        ],
        compiler_params=pltpu.CompilerParams(
            collective_id=0, has_side_effects=True, vmem_limit_bytes=56 * 1024 * 1024
        ),
        cost_estimate=pl.CostEstimate(flops=10**10, bytes_accessed=10**7, transcendentals=10**7),
    )(*projected, cosine, sine, leak, decay, lam, rec_gain.reshape(1, LANES), att_gain.reshape(1, LANES))

    shares = mixers.reshape(tp, groups, length // tp, 2, heads, LANES)
    both = shares.transpose(2, 3, 0, 1, 4, 5).reshape(length // tp, 2, -1)
    result = jnp.dot(both[:, 0], out_rec, preferred_element_type=F32) + jnp.dot(
        both[:, 1], out_att, preferred_element_type=F32
    )
    return result.astype(BF16)


def fused_kernel(
    ranks, tp, heads, planes,
    tokens_in, norm_in, w_key, w_value, w_query, w_rq, w_fwd, w_bwd, w_rv, leak_in, decay_in, rec_gain_in,
    lam_in, att_gain_in, out_rec_in, out_att_in, rotary_in,
    out,
    tokens, gain, weights, leak, decay, decay_rows, rec_gain, lam, att_gain, w_out, rotary,
    held, cosine, sine, lam_own, lam_pair, stage_kv, stage_q, kv, query, recp, cum_reads, facts, adds, rec_sum,
    state, fade, pair_out, pair_in, plane_out, plane_in, plane_sum, next_out, next_in, before_block,
    rec_stage, rec_all, score_a, score_b, top_a, top_b, acc, peak, att_stage, att_all, total,
    up, down, in_sem, across_send, across_recv, core_send, core_recv, lam_send, lam_recv,
    kv_send, kv_recv, q_send, q_recv, side_send, side_recv, near_send, near_recv,
    pair_send, pair_recv, plane_send, plane_recv, next_send, next_recv,
    rec_send, rec_recv, att_send, att_recv,
):
    sp = lax.axis_index("sp")
    me = lax.axis_index("tp")
    x = lax.rem(sp, 2)
    z = lax.div(sp, 2)
    core = lax.rem(me, 2)
    y = lax.div(me, 2)
    piece = tokens.shape[0]
    half = piece // 2
    length = piece * tp
    width = heads * LANES
    partner = {"tp": y * 2 + 1 - core}
    opposite = {"tp": (1 - y) * 2 + core}
    beside = {"sp": z * 2 + 1 - x}

    small = (
        (rotary_in, rotary), (lam_in, lam), (leak_in, leak), (decay_in, decay),
        (rec_gain_in, rec_gain), (att_gain_in, att_gain),
    )
    inputs = (w_key, w_value, w_query, w_rq, w_fwd, w_bwd, w_rv)
    moves = (
        [(tokens_in, tokens), (norm_in, gain)]
        + [(a, weights.at[i]) for i, a in enumerate(inputs)]
        + list(small) + [(out_rec_in, w_out.at[0]), (out_att_in, w_out.at[1])]
    )
    slots = (0, 1, 2, 3, 4, 5, 5, 5, 5, 6, 7, 8, 9, 10, 11, 12, 12)
    fetches = [pltpu.make_async_copy(a, b, in_sem.at[i]) for i, (a, b) in zip(slots, moves)]
    f_rotary, f_lam, f_leak, f_decay, f_rec_gain, f_att_gain = fetches[9:15]
    for fetch in fetches[:2] + fetches[9:11]:
        fetch.start()

    barrier = pltpu.get_barrier_semaphore()
    above = {"sp": sp + 2}
    below = {"sp": sp - 2}
    for to in (partner, opposite, {"tp": (1 - y) * 2 + 1 - core}, beside):
        pl.semaphore_signal(barrier, inc=1, device_id=to)

    @pl.when(z > 0)
    def _():
        pl.semaphore_signal(barrier, inc=1, device_id=below)

    @pl.when(z < planes - 1)
    def _():
        pl.semaphore_signal(barrier, inc=1, device_id=above)

    neighbours = 4 + lax.div(z + planes - 2, planes - 1) + lax.div(2 * planes - 3 - z, planes - 1)

    def hop(turn):
        for toward, signal, source in ((above, up, 0), (below, down, planes - 1)):

            @pl.when(z == (turn if source == 0 else source - turn))
            def _():
                if turn:
                    pl.semaphore_wait(signal, 1)
                if turn < planes - 1:
                    pl.semaphore_signal(signal, inc=1, device_id=toward)

    def remote(source, target, send, recv, to):
        return pltpu.make_async_remote_copy(
            src_ref=source, dst_ref=target, send_sem=send, recv_sem=recv, device_id=to
        )

    def held_at(owner, part, side):
        return owner * 2 * piece + part * piece + side * half

    def held_rows(owner, part, side):
        return held.at[pl.ds(pl.multiple_of(held_at(owner, part, side), half), half)]

    def across(part, owner):
        rows = held_rows(owner, part, core)
        return remote(rows, rows, across_send, across_recv.at[part], opposite)

    def to_core(owner, part, side, slot):
        rows = held_rows(owner, part, side)
        return remote(rows, rows, core_send, core_recv.at[slot], partner)

    fetches[0].wait()
    fetches[1].wait()
    for fetch in fetches[2:9] + fetches[11:15]:
        fetch.start()
    for part in range(2):
        rows = tokens[part * half : (part + 1) * half, :].astype(F32)
        at = pl.ds(pl.multiple_of(held_at(y, part, core), half), half)
        held[at, :] = rms_scale(rows, gain[...]).astype(BF16)
        if part == 0:
            pl.semaphore_wait(barrier, neighbours)
            hop(0)
        across(part, y).start()
        to_core(y, part, core, part).start()
    f_lam.wait()
    for i in range(heads):
        lam_own[i] = jnp.broadcast_to(lam[:, i : i + 1], (8, LANES))
    lam_copy = remote(lam_own, lam_pair, lam_send, lam_recv, partner)
    lam_copy.start()

    f_rotary.wait()
    lane = lax.broadcasted_iota(jnp.int32, (piece, LANES), 1)
    low_half = lax.rem(lane, AK) < AK // 2
    for t in range(tp):
        begin = 2 * piece + sp * tp + t
        cos_base = rotary[pl.ds(begin, 1), :]
        sin_base = rotary[pl.ds(begin + ranks * tp, 1), :]
        cos_row, sin_row = rotary[:piece, :], rotary[piece : 2 * piece, :]
        turned = sin_base * cos_row + cos_base * sin_row
        cos_here = cos_base * cos_row - sin_base * sin_row
        sin_here = jnp.where(low_half, -turned, turned)
        for part in range(2):
            to = held_at(t // 2, part, t % 2)
            cosine[to : to + half, :] = cos_here[part * half : (part + 1) * half]
            sine[to : to + half, :] = sin_here[part * half : (part + 1) * half]

    hop(1)

    def rotated(wide, cos_at, sin_at):
        rows = wide.shape[0]
        low = jnp.concatenate([low_half] * (rows // piece), axis=0)
        turned = jnp.where(low, pltpu.roll(wide, LANES - AK // 2, 1), pltpu.roll(wide, AK // 2, 1))
        return wide * cos_at + turned * sin_at

    def owner_of(phase):
        return y if phase < 2 else 1 - y

    def plane_copy(phase, i, kind):
        return remote(
            stage_kv.at[phase, i, kind], kv.at[kind, 0, phase, z], kv_send, kv_recv.at[phase, z],
            {"sp": (core * heads + i) * 2 + x, "tp": y * 2 + kind},
        )

    def query_rows(phase, plane):
        return query.at[phase, pl.ds(pl.multiple_of(plane * half, half), half)]

    def query_copy(phase, i, c):
        return remote(
            stage_q.at[phase, i, c], query_rows(phase, z), q_send, q_recv.at[phase],
            {"sp": (core * heads + i) * 2 + x, "tp": y * 2 + c},
        )

    def is_own(i, c):
        return jnp.logical_and(core * heads + i == z, core == c)

    def project(at, index):
        return jnp.dot(held[at, :], weights[index], preferred_element_type=F32)

    def attention_inputs(phases):
        count = len(phases) * piece
        owner = owner_of(phases[0])
        at = pl.ds(pl.multiple_of(held_at(owner, phases[0] % 2, 0), piece), count)
        cos_at, sin_at = cosine[at, :], sine[at, :]
        if phases[0] == 0:
            fetches[2].wait()
        keys = project(at, 0).astype(BF16).astype(F32)
        if phases[0] == 0:
            fetches[3].wait()
        values = project(at, 1).astype(BF16).astype(F32)
        if phases[0] == 0:
            hop(2)
        for i in range(heads):
            span = slice(i * LANES, (i + 1) * LANES)
            value = values[:, span].T.astype(BF16)
            key = rotated(keys[:, span], cos_at, sin_at).astype(BF16)
            for n, phase in enumerate(phases):
                part = slice(n * piece, (n + 1) * piece)
                stage_kv[phase, i, 0] = value[:, part]
                stage_kv[phase, i, 1] = key[part]
        if phases[0] == 0:
            hop(3)
        for phase in phases:
            send_each(phase, plane_copy, kv_recv.at[phase, z], lambda i, c: (stage_kv.at[phase, i, c], kv.at[c, 0, phase, z]))
        if phases[0] == 0:
            fetches[4].wait()
        queries = project(at, 2).astype(BF16).astype(F32)
        for i in range(heads):
            span = slice(i * LANES, (i + 1) * LANES)
            turned = (rotated(queries[:, span], cos_at, sin_at) * AK ** (-0.5)).astype(BF16)
            for n, phase in enumerate(phases):
                for c in range(2):
                    stage_q[phase, i, c] = turned[n * piece + c * half : n * piece + (c + 1) * half]
        for phase in phases:
            send_each(phase, query_copy, q_recv.at[phase], lambda i, c: (stage_q.at[phase, i, c], query_rows(phase, z)))

    def send_each(phase, copy, recv, local):
        for i in range(heads):
            for c in range(2):
                own = is_own(i, c)

                @pl.when(own)
                def _():
                    source, target = local(i, c)
                    pltpu.make_async_copy(source, target, recv).start()

                @pl.when(jnp.logical_not(own))
                def _():
                    copy(phase, i, c).start()

    def recurrence_inputs(owner, parts, wait):
        at = pl.ds(pl.multiple_of(held_at(owner, parts[0], 0), piece), len(parts) * piece)
        if wait:
            pltpu.make_async_copy(weights.at[3:7], weights.at[3:7], in_sem.at[5]).wait()
        for i in range(4):
            recp[i, at, :] = project(at, 3 + i).astype(BF16)

    def plane_at(k):
        return (z, z + 1 - 2 * lax.rem(z, 2), lax.rem(z + 2, planes), planes - 1 - z)[k]

    def mine_of(origin, phase, plane):
        return kv.at[core, origin, phase, plane]

    def to_side(phase, plane):
        return remote(
            mine_of(0, phase, plane), mine_of(1, phase, plane),
            side_send, side_recv.at[phase, plane], beside,
        )

    def to_near(origin, phase, plane):
        block = mine_of(origin, phase, plane)
        return remote(
            block, block, near_send, near_recv.at[phase, origin], partner
        )

    def relay_plane(phase, k):
        plane = plane_at(k)
        block = mine_of(0, phase, plane)
        remote(block, block, near_send, kv_recv.at[phase, plane], partner).wait_recv()
        to_side(phase, plane).start()
        to_near(0, phase, plane).start()

    def relay_side(phase, k):
        plane = plane_at(k)
        block = mine_of(1, phase, plane)
        remote(block, block, side_send, side_recv.at[phase, plane], beside).wait_recv()
        to_near(1, phase, plane).start()

    def settle(phase, origin):
        blocks_in = kv.at[1 - core, origin, phase]
        remote(blocks_in, blocks_in, near_send, near_recv.at[phase, origin], partner).wait_recv()

    def settle_queries(phase):
        rows = query.at[phase]
        remote(rows, rows, q_send, q_recv.at[phase], partner).wait_recv()

    row_at = lax.broadcasted_iota(jnp.int32, (BLOCK, 3 * BLOCK), 0)
    col_at = lax.rem(lax.broadcasted_iota(jnp.int32, (BLOCK, 3 * BLOCK), 1), BLOCK)
    triangles = (jnp.where(row_at >= col_at, 1.0, 0.0).astype(BF16), jnp.where(row_at <= col_at, 1.0, 0.0).astype(BF16))
    row_in = lax.broadcasted_iota(jnp.int32, (BLOCK, BLOCK), 0)
    col_in = lax.broadcasted_iota(jnp.int32, (BLOCK, BLOCK), 1)
    earlier = (row_in >= col_in, row_in <= col_in)
    ends = (BLOCK - 1, 0)
    middles = (BLOCK // 2 - 1, BLOCK // 2)
    blocks = length // BLOCK
    spans = [slice(h * LANES, (h + 1) * LANES) for h in range(heads)]

    def within_block(b):
        at = pl.ds(pl.multiple_of(b * BLOCK, BLOCK), BLOCK)
        t = lax.div(b, 2)
        stored = held_at(lax.div(t, 2), lax.rem(b, 2), lax.rem(t, 2))
        held_block = pl.ds(pl.multiple_of(stored, BLOCK), BLOCK)
        queries = jax.nn.silu(recp[0, held_block, :].astype(F32))
        values = recp[3, held_block, :]
        scores, tails = [], []
        for d in range(2):
            keys = leak[d : d + 1, :] * jax.nn.sigmoid(-recp[1 + d, held_block, :].astype(F32))
            added = jnp.concatenate(
                [jnp.broadcast_to(decay_rows[at, d * heads + h : d * heads + h + 1], (BLOCK, LANES)) for h in range(heads)],
                axis=1,
            )
            logs = jnp.log1p(-keys) + added
            coarse = logs.astype(BF16)
            rest = logs - coarse.astype(F32)
            fine = rest.astype(BF16)
            finest = (rest - fine.astype(F32)).astype(BF16)
            cum = jnp.dot(
                triangles[d], jnp.concatenate([coarse, fine, finest], axis=0), preferred_element_type=F32
            )
            middle = cum[middles[d] : middles[d] + 1, :]
            last = cum[ends[d] : ends[d] + 1, :]
            reads = (queries * jnp.exp(cum - middle)).astype(BF16)
            writes = (keys * jnp.exp(middle - cum)).astype(BF16)
            tails.append((keys * jnp.exp(last - cum)).astype(BF16))
            carried = (queries * jnp.exp(cum)).astype(BF16)
            facts[b, d] = jnp.broadcast_to(jnp.exp(last), (8, width))
            scores.append([jnp.where(earlier[d], dot_t(reads[:, s], writes[:, s]), 0.0) for s in spans])
            for h in range(heads):
                cum_reads[h, at, d * LANES : (d + 1) * LANES] = carried[:, spans[h]]
        for h in range(heads):
            both = (scores[0][h] + scores[1][h]).astype(BF16)
            rec_sum[at, spans[h]] = jnp.dot(both, values[:, spans[h]], preferred_element_type=F32)
            adds[b, h] = dot_0(
                values[:, spans[h]], jnp.concatenate([tails[0][:, spans[h]], tails[1][:, spans[h]]], axis=1)
            )

    def within_rows(owner, parts):
        def some(part, carry):
            within_block(owner * 4 + part)
            within_block(owner * 4 + 2 + part)
            return carry

        lax.fori_loop(parts[0], parts[-1] + 1, some, 0)

    def order(d):
        return range(blocks) if d == 0 else range(blocks - 1, -1, -1)

    def half_of(d):
        return slice(d * LANES, (d + 1) * LANES)

    first_row = lax.broadcasted_iota(jnp.int32, (PAD, LANES), 0) == 0

    def pack(target, moved, factor):
        target[:LANES, :] = moved.astype(BF16)
        wide = jnp.broadcast_to(factor, (PAD, LANES))
        coarse = wide.astype(BF16).astype(F32)
        target[LANES:, :] = jnp.where(first_row, coarse, wide - coarse).astype(BF16)

    def unpack(source):
        last = source[LANES:, :].astype(F32)
        return source[:LANES, :].astype(F32), last[0:1] + last[1:2]

    def local_states():
        for h in range(heads):
            for d in range(2):
                moved = jnp.zeros((LANES, LANES), F32)
                factor = jnp.ones((1, LANES), F32)
                for b in order(d):
                    step = facts[b, d, 0:1, spans[h]]
                    moved = moved * step + adds[b, h, :, half_of(d)]
                    factor = factor * step
                state[d, h] = moved
                fade[d, h] = jnp.broadcast_to(factor, (8, LANES))
                pack(pair_out.at[d, h], moved, factor)

    def pair_copies():
        return [
            remote(pair_out.at[d, h], pair_in.at[d, h], pair_send, pair_recv, beside)
            for d, h in ((0, 1 - x), (1, 1 - x), (x, x))
        ]

    def pair_done():
        three = plane_in.at[:3]
        return remote(three, three, pair_send, pair_recv, beside)

    def send_pair():
        for copy in pair_copies():
            copy.start()

    def pair_states():
        pair_done().wait_recv()
        for d in range(2):
            mine, factor = state[d, x], fade[d, x][0:1]
            other, other_factor = unpack(pair_in.at[d, x])
            joined = jnp.where(x == d, mine * other_factor + other, other * factor + mine)
            pack(plane_out.at[d], joined, factor * other_factor)
        for dz in range(1, planes):
            to_plane(lax.rem(z + dz, planes)).start()

    def to_plane(target):
        return remote(
            plane_out.at[jnp.where(target > z, 0, 1)], plane_in.at[z],
            plane_send, plane_recv, {"sp": target * 2 + x},
        )

    def other_planes():
        blocks_in = plane_in.at[: planes - 1]
        return remote(blocks_in, blocks_in, plane_send, plane_recv, partner)

    next_copy = remote(next_out, next_in, next_send, next_recv, beside)

    def plane_states():
        other_planes().wait_recv()
        plane_sum[...] = jnp.zeros_like(plane_sum)

        def fold(d):
            def one(step, carry):
                plane = step if d == 0 else planes - 1 - step
                moved, factor = unpack(plane_in.at[plane])
                plane_sum[d] = plane_sum[d] * factor + moved
                return carry

            return one

        lax.fori_loop(0, z, fold(0), 0)
        lax.fori_loop(0, planes - 1 - z, fold(1), 0)
        next_out[...] = plane_sum[...].astype(BF16)
        next_copy.start()

    def second_pass():
        next_copy.wait_recv()
        for h in range(heads):
            for d in range(2):
                entering = jnp.where(x == h, plane_sum[d], next_in[d].astype(F32))
                other, other_factor = unpack(pair_in.at[d, jnp.where(x == d, x, h)])
                running = jnp.where(x == d, entering, entering * other_factor + other)
                for b in order(d):
                    before_block[b, h, :, half_of(d)] = running.astype(BF16)
                    running = running * facts[b, d, 0:1, spans[h]] + adds[b, h, :, half_of(d)]
            for b in range(blocks):
                at = slice(b * BLOCK, (b + 1) * BLOCK)
                whole = rec_sum[at, spans[h]] + dot_t(cum_reads[h, at, :], before_block[b, h])
                rec_stage[at, spans[h]] = rms_scale(whole, rec_gain[...]).astype(BF16)
        for dt in range(tp):
            rec_copy(dt).start()

    def rec_copy(dt):
        t = lax.rem(me + dt, tp)
        source = rec_stage.at[pl.ds(pl.multiple_of(t * piece, piece), piece)]
        if dt == 0:
            return pltpu.make_async_copy(source, rec_all.at[me], rec_recv)
        return remote(source, rec_all.at[me], rec_send, rec_recv, {"tp": t})

    acc[...] = jnp.zeros_like(acc)
    peak[...] = jnp.full_like(peak, -jnp.inf)
    sub = 2 * piece
    ones = jnp.ones((PAD, sub), BF16)
    low_map = lane < AK
    buffers = ((score_a, top_a), (score_b, top_b))

    def attend_step(made, made_buffer, used, used_buffer):
        if made is not None:
            q_phase, tile, chunk = made
            made_blocks = [(o, f, p) for f, o in chunk for p in range(planes)]
            rows = query[q_phase, pl.ds(tile * piece if isinstance(tile, int) else pl.multiple_of(tile * piece, piece), piece), :]
            none = jnp.zeros_like(rows)
            both = jnp.concatenate([jnp.where(low_map, rows, none), jnp.where(low_map, none, rows)], axis=0)
            top = None
        if used is not None:
            slot = used[0] * 2 + used[1]
            used_blocks = [(o, f, p) for f, o in used[2] for p in range(planes)]
            used_score, used_top = used_buffer
            before = peak[slot][0:1]
            now = jnp.maximum(before, jnp.max(used_top[...], axis=0, keepdims=True))
            mixed = acc[slot] * jnp.exp(before - now)
        made_pairs = len(made_blocks) // 2 if made is not None else 0
        used_pairs = len(used_blocks) // 2 if used is not None else 0
        for u in range(max(made_pairs, used_pairs)):
            at = slice(u * sub, (u + 1) * sub)
            if u < made_pairs:
                keys = jnp.concatenate([kv[(1, *block)] for block in made_blocks[2 * u : 2 * u + 2]], axis=0)
                scores = dot_t(keys, both)
                made_buffer[0][at, :] = scores
                high = jnp.max(scores.reshape(sub // 8, 8, 2 * piece), axis=0)
                top = high if top is None else jnp.maximum(top, high)
            if u < used_pairs:
                expo = jnp.exp(used_score[at, :] - now).astype(BF16)
                values = jnp.concatenate([kv[(0, *block)] for block in used_blocks[2 * u : 2 * u + 2]], axis=1)
                values = jnp.concatenate([values, ones], axis=0)
                mixed = mixed + jnp.dot(values, expo, preferred_element_type=F32)
        if used is not None:
            acc[slot] = mixed
            peak[slot] = jnp.broadcast_to(now, (8, 2 * piece))
        if made is not None:
            made_buffer[1][...] = top

    def att_copy(q_phase, plane):
        owner, part = owner_of(q_phase), q_phase % 2
        return remote(
            att_stage.at[q_phase * planes + plane], att_all.at[y * planes + z, part * half : (part + 1) * half],
            att_send, att_recv,
            {"sp": plane * 2 + x, "tp": owner * 2 + core},
        )

    def finish(q_phase, tile):
        whole = acc[q_phase * 2 + tile]
        ratio = whole[:LANES] / whole[LANES : LANES + 1]
        weight = jnp.where(core == lax.div(z, heads), lam_own[lax.rem(z, heads)], lam_pair[lax.rem(z, heads)])[0:1]
        values = ratio[:, :piece] - weight * ratio[:, piece:]
        scale = lax.rsqrt(jnp.mean(values * values, axis=0, keepdims=True) + EPS)
        rows = ((values * scale).T * att_gain[...]).astype(BF16)
        part = q_phase % 2
        for n in range(2):
            plane = 2 * tile + n
            att_stage[q_phase * planes + plane] = rows[n * half : (n + 1) * half]
            if q_phase < 2:

                @pl.when(plane == z)
                def _():
                    pltpu.make_async_copy(
                        att_stage.at[q_phase * planes + plane],
                        att_all.at[y * planes + z, part * half : (part + 1) * half],
                        att_recv,
                    ).start()

                @pl.when(plane != z)
                def _():
                    att_copy(q_phase, plane).start()
            else:
                att_copy(q_phase, plane).start()

    columns = min(512, out.shape[1])

    def rec_total():
        pltpu.make_async_copy(w_out, w_out, in_sem.at[12]).wait()
        remote(rec_all, rec_all, rec_send, rec_recv, partner).wait_recv()
        rec_rows = jnp.concatenate([rec_all[t] for t in range(tp)], axis=1)
        for n in range(0, out.shape[1], columns):
            total[:, n : n + columns] = jnp.dot(rec_rows, w_out[0, :, n : n + columns], preferred_element_type=F32)

    def run_units(units, before):
        for n in range(len(units) + 1):
            for action in before.get(n, ()):
                action()
            made = units[n] if n < len(units) else None
            used = units[n - 1] if n else None
            attend_step(made, buffers[n % 2], used, buffers[(n + 1) % 2])
            if used is not None and used[2][-1] == (3, 1):
                finish(used[0], used[1])

    def tiles_of(q_phases, chunk):
        return [(q_phase, tile, chunk) for q_phase in q_phases for tile in range(2)]

    def call(f, *args):
        return functools.partial(f, *args)

    def all_of(f, phase, ks):
        return [call(f, phase, k) for k in ks]

    near, far = (0, 1), (2, 3)
    near_keys = [(f, o) for f in near for o in range(2)]
    far_keys = [(f, o) for f in far for o in range(2)]
    every = near + far
    units = tiles_of(every, near_keys)
    side_tile = 1 - lax.div(2 * z, planes)
    for tile in (side_tile, 1 - side_tile):
        units += [(q_phase, tile, far_keys) for q_phase in far + near]
    before = {
        1: [call(relay_plane, 3, 0)],
        2: [call(relay_plane, 3, 1)] + all_of(relay_side, 2, range(1)),
        3: [call(relay_plane, 3, 2)] + all_of(relay_side, 2, range(1, 2)),
        4: [call(settle_queries, 2), call(settle_queries, 3), call(relay_plane, 3, 3)],
        5: all_of(relay_side, 2, range(2, 4)),
        6: all_of(relay_side, 3, range(1)),
        7: all_of(relay_side, 3, range(1, 3)),
        8: all_of(relay_side, 3, range(3, 4)) + [call(settle, f, o) for f, o in far_keys],
        9: [plane_states],
        12: [second_pass],
    }
    before[4].append(pair_states)

    for part in range(2):
        to_core(y, part, 1 - core, part).wait_recv()
    attention_inputs(near)
    for fetch in fetches[15:17]:
        fetch.start()
    recurrence_inputs(y, (0, 1), True)
    for fetch in (f_leak, f_decay, f_rec_gain, f_att_gain):
        fetch.wait()
    by_row = jnp.concatenate([decay[d] for d in range(2)] + [jnp.zeros((LANES - 2 * heads, length), F32)], axis=0)
    decay_rows[...] = by_row.T
    relay_plane(0, 0)
    relay_plane(1, 0)
    within_rows(y, (0, 1))
    relay_plane(0, 1)
    across(0, 1 - y).wait_recv()
    to_core(1 - y, 0, core, 2).start()
    relay_plane(0, 2)
    to_core(1 - y, 0, 1 - core, 2).wait_recv()
    attention_inputs((2,))
    relay_plane(0, 3)
    relay_side(0, 0)
    relay_plane(1, 1)
    recurrence_inputs(1 - y, (0,), False)
    across(1, 1 - y).wait_recv()
    to_core(1 - y, 1, core, 3).start()
    within_rows(1 - y, (0,))
    relay_plane(1, 2)
    to_core(1 - y, 1, 1 - core, 3).wait_recv()
    attention_inputs((3,))
    relay_plane(1, 3)
    for k in range(1, 4):
        relay_side(0, k)
    relay_plane(2, 0)
    recurrence_inputs(1 - y, (1,), False)
    relay_side(1, 0)
    relay_side(1, 1)
    relay_plane(2, 1)
    within_rows(1 - y, (1,))
    local_states()
    send_pair()
    relay_plane(2, 2)
    relay_plane(2, 3)
    relay_side(1, 2)
    relay_side(1, 3)
    lam_copy.wait_recv()
    for phase in near:
        for origin in range(2):
            settle(phase, origin)
        settle_queries(phase)
    run_units(units, before)
    rec_total()

    remote(att_all, att_all, att_send, att_recv, partner).wait_recv()
    att_rows = jnp.concatenate([att_all[i] for i in range(2 * planes)], axis=1)
    for n in range(0, out.shape[1], columns):
        out[:, n : n + columns] = (
            total[:, n : n + columns]
            + jnp.dot(att_rows, w_out[1, :, n : n + columns], preferred_element_type=F32)
        ).astype(BF16)

    def sent(ref, sem, recv):
        remote(ref, ref, sem, recv, partner).wait_send()

    sent(held.at[:piece], across_send, core_recv.at[0])
    sent(held.at[: 2 * piece], core_send, core_recv.at[0])
    lam_copy.wait_send()
    is_local = core == lax.div(z, heads)

    @pl.when(is_local)
    def _():
        sent(stage_kv.at[:3], kv_send, near_recv.at[0, 0])
        sent(stage_q.at[:3], q_send, near_recv.at[0, 0])

    @pl.when(jnp.logical_not(is_local))
    def _():
        sent(stage_kv, kv_send, near_recv.at[0, 0])
        sent(stage_q, q_send, near_recv.at[0, 0])

    sent(kv.at[0, 0], side_send, near_recv.at[0, 0])
    sent(kv.at[0], near_send, near_recv.at[0, 0])
    pair_done().wait_send()
    next_copy.wait_send()
    sent(plane_in.at[: planes - 1], plane_send, plane_recv)
    sent(rec_all.at[: tp - 1], rec_send, rec_recv)
    sent(att_stage.at[: 4 * planes - 2], att_send, att_recv)


def rotary_table(piece, pieces):
    frequency = THETA ** (-(np.arange(LANES) % (AK // 2)) * 2.0 / AK)
    inside = np.arange(piece)[:, None] * frequency[None, :]
    base = (np.arange(pieces) * piece)[:, None] * frequency[None, :]
    return np.concatenate([np.cos(inside), np.sin(inside), np.cos(base), np.sin(base)]).astype(np.float32)


def on_device(
    tokens, norm_gain, rec_query, fwd_gate, bwd_gate, rec_value, gate_leak, log_decay, rec_gain,
    att_query, att_key, att_value, lambdas, att_gain, out_rec, out_att,
):
    ranks = lax.axis_size("sp")
    tp = lax.axis_size("tp")
    heads = rec_query.shape[1] // HK
    planes = ranks // 2
    piece, model = tokens.shape
    if tp != 4 or planes != 2 * heads or planes != 4 or piece != LANES:
        return on_device_general(
            tokens, norm_gain, rec_query, fwd_gate, bwd_gate, rec_value, gate_leak, log_decay, rec_gain,
            att_query, att_key, att_value, lambdas, att_gain, out_rec, out_att,
        )
    length = piece * tp
    width = heads * LANES
    blocks = length // BLOCK
    keys = 4 * planes * piece
    anywhere = pl.BlockSpec(memory_space=pl.ANY)
    dma = pltpu.SemaphoreType.DMA
    vmem = pltpu.VMEM
    table = jnp.asarray(rotary_table(piece, ranks * tp))
    return pl.pallas_call(
        functools.partial(fused_kernel, ranks, tp, heads, planes),
        out_shape=jax.ShapeDtypeStruct((piece, model), BF16),
        in_specs=[anywhere] * 17,
        out_specs=pl.BlockSpec(memory_space=pltpu.VMEM),
        scratch_shapes=[
            vmem((piece, model), BF16),
            vmem((1, model), F32),
            vmem((7, model, width), BF16),
            vmem((2, width), F32),
            vmem((2, heads, length), F32),
            vmem((length, LANES), F32),
            vmem((1, LANES), F32),
            vmem((1, heads), F32),
            vmem((1, LANES), F32),
            vmem((2, *out_rec.shape), BF16),
            vmem(table.shape, F32),
            vmem((length, model), BF16),
            vmem((length, LANES), F32),
            vmem((length, LANES), F32),
            vmem((heads, 8, LANES), F32),
            vmem((heads, 8, LANES), F32),
            vmem((4, heads, 2, piece, LANES), BF16),
            vmem((4, heads, 2, piece // 2, LANES), BF16),
            vmem((2, 2, 4, planes, piece, LANES), BF16),
            vmem((4, planes * piece // 2, LANES), BF16),
            vmem((4, length, width), BF16),
            vmem((heads, length, 2 * LANES), BF16),
            vmem((blocks, 2, 8, width), F32),
            vmem((blocks, heads, LANES, 2 * LANES), F32),
            vmem((length, width), F32),
            vmem((2, heads, LANES, LANES), F32),
            vmem((2, heads, 8, LANES), F32),
            vmem((2, heads, LANES + PAD, LANES), BF16),
            vmem((2, heads, LANES + PAD, LANES), BF16),
            vmem((2, LANES + PAD, LANES), BF16),
            vmem((planes, LANES + PAD, LANES), BF16),
            vmem((2, LANES, LANES), F32),
            vmem((2, LANES, LANES), BF16),
            vmem((2, LANES, LANES), BF16),
            vmem((blocks, heads, LANES, 2 * LANES), BF16),
            vmem((length, width), BF16),
            vmem((tp, piece, width), BF16),
            vmem((keys, 2 * piece), F32),
            vmem((keys, 2 * piece), F32),
            vmem((8, 2 * piece), F32),
            vmem((8, 2 * piece), F32),
            vmem((2 * planes, LANES + PAD, 2 * piece), F32),
            vmem((2 * planes, 8, 2 * piece), F32),
            vmem((4 * planes, piece // 2, LANES), BF16),
            vmem((2 * planes, piece, LANES), BF16),
            vmem((piece, model), F32),
            pltpu.SemaphoreType.REGULAR, pltpu.SemaphoreType.REGULAR,
            dma((13,)), dma, dma((2,)), dma, dma((4,)), dma, dma,
            dma, dma((4, planes)), dma, dma((4,)),
            dma, dma((4, planes)), dma, dma((4, 2)),
            dma, dma, dma, dma, dma, dma,
            dma, dma, dma, dma,
        ],
        compiler_params=pltpu.CompilerParams(
            collective_id=2, has_side_effects=True, vmem_limit_bytes=60 * 1024 * 1024
        ),
        cost_estimate=pl.CostEstimate(flops=10**10, bytes_accessed=10**7, transcendentals=10**7),
    )(
        tokens, norm_gain.reshape(1, -1), att_key, att_value, att_query, rec_query, fwd_gate, bwd_gate, rec_value,
        gate_leak, log_decay.transpose(0, 2, 1), rec_gain.reshape(1, LANES), lambdas.reshape(1, heads), att_gain.reshape(1, LANES),
        out_rec, out_att, table,
    )


def solution(mesh):
    placed = (
        P(("sp", "tp"), None), P(), P(None, "tp"), P(None, "tp"), P(None, "tp"), P(None, "tp"),
        P(None, "tp"), P(None, "sp", "tp"), P(), P(None, "tp"), P(None, "tp"), P(None, "tp"),
        P("tp"), P(), P(), P(),
    )
    return jax.shard_map(
        on_device, mesh=mesh, in_specs=placed, out_specs=P(("sp", "tp"), None), check_vma=False
    )
```
